32 devices in a mesh: ep: 8 (over z, x), tp: 4 (over y, core).
Axes of the slice: x: 2, y: 2, z: 4, core: 2. Of those that a mesh axis runs over, the one named last changes fastest.
Arguments:
- mixer_tokens: bfloat16 [1536, 2048], P('ep'), may hold values from -6 to 6
- mixer_gain: float32 [2048], replicated, may hold values from 0.1 to 1.9
- query_weight: bfloat16 [1024, 2048], P('tp'), may hold values from -1 to 1
- key_weight: bfloat16 [1024, 2048], P('tp'), may hold values from -1 to 1
- value_weight: bfloat16 [1024, 2048], P('tp'), may hold values from -0.125 to 0.125
- forget_weight: bfloat16 [2048, 16], P(None, 'tp'), may hold values from -0.125 to 0.125
- forget_bias: float32 [8, 16], P('ep', 'tp'), may hold values from 2.98 to 10.4
- output_weight: bfloat16 [1024, 2048], P(None, 'tp'), may hold values from -0.1875 to 0.1875
- expert_tokens: bfloat16 [1024, 2048], P('ep'), may hold values from -6 to 6
- expert_gain: float32 [2048], replicated, may hold values from 0.1 to 1.9
- routes: int32 [1024, 2], P('ep'), may hold values from 0 to 7, all different within a row; in each aligned block of 128 rows (0 to 127, 128 to 255, ...) at most 64 rows name the same one
- route_weights: float32 [1024, 2], P('ep'), may hold values from 0.2 to 1
- gate_weight: bfloat16 [8, 3584, 2048], P('ep', 'tp'), may hold values from -0.125 to 0.125
- up_weight: bfloat16 [8, 3584, 2048], P('ep', 'tp'), may hold values from -0.125 to 0.125
- down_weight: bfloat16 [8, 3584, 2048], P('ep', 'tp'), may hold values from -0.09375 to 0.09375
Outputs:
- mixer_output: bfloat16 [1536, 2048], P('ep', 'tp')
- expert_output: bfloat16 [1024, 2048], P('ep', 'tp')
The draws below stay inside these ranges and needn't reach their ends.
Inputs may be any that keep to these rules, and one draw needn't show every extreme that they name: `routes`: within the tokens of one index of ep (aligned blocks of 128 rows) no expert is named more than 64 times, a bound that some block reaches; the 2 experts of a token differ.
All inputs are finite; a program needn't handle non-finite values.
Results may differ from the reference program's by a relative error of at most 0.019.
Values may be sent and summed in bfloat16 or wider, within the bound.
A program may use at most 128 MiB of HBM per device.

```python
import math
import jax
import jax.numpy as jnp
import numpy as np
from jax import lax

D = 2048
HEADS = 16
HD = 64
EXPERT_FF = 3584
TOP = 2
TOK_A = 192
TOK_B = 128
EXPERTS = 8
CAP = 64
TOKENS_A = 1536
TOKENS_B = 1024
N_EP = 8
N_TP = 4


def spiked_weight(key, salt):
    base_draw = jax.random.normal(jax.random.fold_in(key, salt), (HEADS * HD, D), jnp.float32)
    base_draw = jnp.clip(base_draw, -6.0, 6.0) * D ** (-0.5)
    return base_draw.astype(jnp.bfloat16)


def draw_query_weight(key, part):
    return spiked_weight(key, 11)


def draw_key_weight(key, part):
    return spiked_weight(key, 12)


def draw_mixer_tokens(key, part):
    values = jnp.clip(jax.random.normal(jax.random.fold_in(key, 201), (TOKENS_A, D), jnp.float32), -6.0, 6.0)
    return values.astype(jnp.bfloat16)


def draw_forget_bias(key, part):
    block_count = TOKENS_A // TOK_A
    chance = 0.5
    slow_heads = jax.random.bernoulli(jax.random.fold_in(key, 301), chance, (HEADS,))
    base_level = jnp.where(slow_heads, 9.7, math.log(40.0)).astype(jnp.float32)
    block_drift = jax.random.uniform(jax.random.fold_in(key, 302), (block_count, HEADS), jnp.float32, -0.7, 0.7)
    return base_level[None, :] + block_drift


def steps_of(rng, shape, split, least, largest):
    factor_of = 1.0
    for axis_at, blocks in split:
        draws = jax.random.uniform(jax.random.fold_in(jax.random.fold_in(rng, 6), axis_at), (blocks,), jnp.float32, least / len(split), largest / len(split))
        factor_of = factor_of * jnp.repeat(jnp.exp(draws), shape[axis_at] // blocks).reshape((-1,) + (1,) * (len(shape) - 1 - axis_at))
    return factor_of


def deal_out(rng, own, number, rows, count, top, limit, lean):
    order = jax.random.permutation(rng, count)
    heavy_load, common = portions_of(count, rows * top, limit, lean, True), portions_of(count, rows * top, limit, lean, False)
    places = jnp.arange(count)

    def named(tallies, offset_by):
        used = int((tallies > 0).sum())
        fixed = max(1, used // 4)
        moved = fixed + (places - fixed + offset_by * (used - fixed)) % max(1, count - fixed)
        return jnp.zeros((count,), jnp.int32).at[order[jnp.where(places < fixed, places, moved)]].set(jnp.asarray(tallies, jnp.int32))

    tallies = jnp.where(number % 4 == 0, named(heavy_load, number // 4), named(common, number - number // 4 - 1))
    mixed = jax.random.permutation(jax.random.fold_in(own, 3), count)
    source_of, sink = mixed[0:count // 2 * 2:2], mixed[1:count // 2 * 2:2]
    margin = jnp.minimum(tallies[source_of] - 1, limit - tallies[sink]) // 2
    margin = jnp.where((source_of == order[0]) | (sink == order[0]) | (tallies[sink] == 0), 0, jnp.maximum(margin, 0))
    moved = jax.random.randint(jax.random.fold_in(own, 4), (count // 2,), 0, 1 << 20) % (margin + 1)
    tallies = tallies.at[source_of].add(-moved).at[sink].add(moved)
    members = jnp.searchsorted(jnp.cumsum(tallies), jnp.arange(rows * top), side="right").astype(jnp.int32)
    listing = members.reshape(top, rows).T
    listing = listing[jax.random.permutation(jax.random.fold_in(own, 1), rows)]
    offset_by = jax.random.randint(jax.random.fold_in(own, 2), (rows, 1), 0, top)
    return jnp.take_along_axis(listing, (jnp.arange(top)[None, :] + offset_by) % top, axis=1)


def portions_of(count, total, most, lean, full):
    loads = [(1 << 20) // math.isqrt(grade ** lean) + 1 for grade in range(1, count + 1)]
    largest = most if full else min(most, max(-(-total // count), total * loads[0] // sum(loads)))
    least = 1 if total - largest >= count - 1 else 0
    given, rest = [largest] + [least] * (count - 1), total - largest - least * (count - 1)
    while rest > 0:
        free = [i for i in range(1, count) if given[i] < largest] or [i for i in range(1, count) if given[i] < most]
        mass, remaining = sum([loads[i] for i in free]), rest
        for i in free:
            extra = min(most - given[i], max(1, remaining * loads[i] // mass), rest)
            given[i] = given[i] + extra
            rest = rest - extra
    return np.array(given)


def centred(rng, dims, width, most, cuts=(), kind=jnp.bfloat16):
    values = jax.random.normal(rng, dims, jnp.float32) * width
    if len(cuts) > 0:
        values = steps_of(rng, dims, cuts, -0.22, 0.18) * values
    return jnp.clip(values, min=-most, max=most).astype(kind)


def setup_inputs(seed: int = 0) -> dict:
    splits = jax.random.split(jax.random.key(seed), 16)
    mixer_tokens = draw_mixer_tokens(jax.random.fold_in(splits[15], 71), 0)
    mixer_gain = jnp.clip(1.0 + 0.18 * jax.random.normal(splits[1], (D,), jnp.float32), 0.1, 1.9)
    query_weight = draw_query_weight(jax.random.fold_in(splits[15], 71), 0)
    key_weight = draw_key_weight(jax.random.fold_in(splits[15], 71), 0)
    value_weight = centred(splits[4], (HEADS * HD, D), D ** -0.5, 0.125, ((0, 4),))
    forget_weight = centred(splits[5], (D, HEADS), D ** -0.5, 0.125, ((1, 4),))
    forget_bias = draw_forget_bias(jax.random.fold_in(splits[15], 71), 0)
    output_weight = centred(splits[7], (HEADS * HD, D), (HEADS * HD) ** -0.5, 0.1875, ((1, 4),))
    expert_tokens = centred(splits[8], (TOKENS_B, D), 1.0, 6.0, ((0, 8),))
    expert_gain = jnp.clip(1.0 + 0.18 * jax.random.normal(splits[9], (D,), jnp.float32), 0.1, 1.9)
    routes_keys = jax.random.split(jax.random.fold_in(splits[10], 1), TOKENS_B // TOK_B)
    routes_turns = jax.random.permutation(jax.random.fold_in(splits[10], 3), TOKENS_B // TOK_B)
    routes = jax.vmap(lambda own, number: deal_out(jax.random.fold_in(splits[10], 2), own, number, TOK_B, EXPERTS, TOP, CAP, 2))(routes_keys, routes_turns).reshape((TOKENS_B, TOP))
    route_weights = jnp.clip(0.2 + 0.8 * jax.random.uniform(splits[11], (TOKENS_B, TOP), jnp.float32) ** steps_of(splits[11], (TOKENS_B, TOP), ((0, 8),), -0.2, 0.2), 0.2, 1.0)
    gate_weight = centred(splits[12], (EXPERTS, EXPERT_FF, D), D ** -0.5, 0.125, ((0, 8), (1, 4)))
    up_weight = centred(splits[13], (EXPERTS, EXPERT_FF, D), D ** -0.5, 0.125, ((0, 8), (1, 4)))
    down_weight = centred(splits[14], (EXPERTS, EXPERT_FF, D), EXPERT_FF ** -0.5, 0.09375, ((0, 8), (1, 4)))
    return {"mixer_tokens": mixer_tokens, "mixer_gain": mixer_gain, "query_weight": query_weight, "key_weight": key_weight, "value_weight": value_weight, "forget_weight": forget_weight, "forget_bias": forget_bias, "output_weight": output_weight, "expert_tokens": expert_tokens, "expert_gain": expert_gain, "routes": routes, "route_weights": route_weights, "gate_weight": gate_weight, "up_weight": up_weight, "down_weight": down_weight}


MEAN_FLOOR = 0.1
HEAD_FLOOR = 1.0

def normed_rows(inputs, gain):
    values = inputs.astype(jnp.float32)
    square = lax.optimization_barrier(jnp.mean(values * values, axis=-1, keepdims=True))
    return (values * lax.rsqrt(jnp.maximum(square, MEAN_FLOOR)) * gain).astype(jnp.bfloat16)

def by_rows(left, weight):
    return lax.dot_general(left, weight, (((1,), (1,)), ((), ())), preferred_element_type=jnp.float32)

def reference(mixer_tokens, mixer_gain, query_weight, key_weight, value_weight, forget_weight, forget_bias, output_weight, expert_tokens, expert_gain, routes, route_weights, gate_weight, up_weight, down_weight):
    sequence = mixer_tokens.shape[0]
    normed = normed_rows(mixer_tokens, mixer_gain)
    queries = by_rows(normed, query_weight).astype(jnp.bfloat16)
    key_rows = by_rows(normed, key_weight).astype(jnp.bfloat16)
    value_rows = by_rows(normed, value_weight).astype(jnp.bfloat16)
    pre_gate = jnp.dot(normed, forget_weight, preferred_element_type=jnp.float32)
    pre_gate = pre_gate + jnp.repeat(forget_bias, TOK_A, axis=0)
    cumulative = jnp.cumsum(jax.nn.log_sigmoid(pre_gate), axis=0)
    head_query = queries.reshape(sequence, HEADS, HD).astype(jnp.float32)
    head_keys = key_rows.reshape(sequence, HEADS, HD).astype(jnp.float32)
    head_values = value_rows.reshape(sequence, HEADS, HD).astype(jnp.float32)
    key_pos = jnp.arange(sequence, dtype=jnp.int32)

    def attend_block(number):
        first_row = (number * TOK_A).astype(jnp.int32)
        block_query = lax.dynamic_slice_in_dim(head_query, first_row, TOK_A, 0)
        block_cum = lax.dynamic_slice_in_dim(cumulative, first_row, TOK_A, 0)
        scores = jnp.einsum('qhd,khd->hqk', block_query, head_keys) * HD ** (-0.5)
        scores = scores + block_cum.T[:, :, None] - cumulative.T[:, None, :]
        query_pos = first_row + jnp.arange(TOK_A, dtype=jnp.int32)
        scores = jnp.where(key_pos[None, None, :] <= query_pos[None, :, None], scores, -jnp.inf)
        row_max = lax.optimization_barrier(jnp.max(scores, axis=-1, keepdims=True))
        weights = lax.optimization_barrier(jnp.exp(scores - row_max).astype(jnp.bfloat16)).astype(jnp.float32)
        attended = jnp.einsum('hqk,khd->qhd', weights, head_values)
        attended = attended * lax.rsqrt(lax.optimization_barrier(jnp.mean(attended * attended, axis=-1, keepdims=True)) + HEAD_FLOOR)
        return attended.reshape(TOK_A, HEADS * HD).astype(jnp.bfloat16)
    head_out = lax.map(attend_block, jnp.arange(N_EP, dtype=jnp.int32)).reshape(sequence, HEADS * HD)
    mixer_output = jnp.dot(head_out, output_weight, preferred_element_type=jnp.float32).astype(jnp.bfloat16)
    expert_normed = normed_rows(expert_tokens, expert_gain).reshape(N_EP, TOK_B, D)
    flat_routes = routes.reshape(N_EP, TOK_B * TOP)
    onehot = (flat_routes[:, :, None] == jnp.arange(EXPERTS, dtype=jnp.int32)[None, None, :]).astype(jnp.int32)
    slot_rank = lax.optimization_barrier(jnp.sum((jnp.cumsum(onehot, axis=1) - 1) * onehot, axis=2)).astype(jnp.int32)
    slot_index = flat_routes * CAP + slot_rank
    token_of = jnp.arange(TOK_B * TOP, dtype=jnp.int32) // TOP
    source = jnp.broadcast_to(jnp.arange(N_EP, dtype=jnp.int32)[:, None], flat_routes.shape)
    outgoing = jnp.zeros((N_EP, EXPERTS * CAP, D), jnp.bfloat16)
    outgoing = outgoing.at[source, slot_index].set(expert_normed[source, token_of[None, :]])
    groups = EXPERT_FF // N_TP

    def run_expert(number):
        slot_rows = lax.dynamic_slice_in_dim(outgoing, (number * CAP).astype(jnp.int32), CAP, 1)
        slot_rows = slot_rows.reshape(N_EP * CAP, D)
        gate_act = by_rows(slot_rows, gate_weight[number])
        up_act = by_rows(slot_rows, up_weight[number])
        hidden = (jax.nn.silu(gate_act) * up_act).astype(jnp.bfloat16)
        partial_value = jnp.einsum('rtf,tfd->trd', hidden.reshape(N_EP * CAP, N_TP, groups).astype(jnp.float32), down_weight[number].reshape(N_TP, groups, D).astype(jnp.float32))
        partial_value = lax.optimization_barrier(partial_value.astype(jnp.bfloat16)).astype(jnp.float32)
        return lax.optimization_barrier(jnp.sum(partial_value, axis=0)).astype(jnp.bfloat16)
    results = lax.map(run_expert, jnp.arange(EXPERTS, dtype=jnp.int32))
    picked = results.reshape(EXPERTS, N_EP, CAP, D)[flat_routes, source, slot_rank]
    weighted = picked.astype(jnp.float32) * route_weights.reshape(N_EP, TOK_B * TOP)[:, :, None]
    expert_output = lax.optimization_barrier(jnp.sum(weighted.reshape(N_EP, TOK_B, TOP, D), axis=2))
    expert_output = expert_output.reshape(N_EP * TOK_B, D).astype(jnp.bfloat16)
    return (mixer_output, expert_output)
```

```python
import functools

import jax
import jax.numpy as jnp
from jax import lax
from jax.experimental import pallas as pl
from jax.experimental.pallas import tpu as pltpu
from jax.sharding import PartitionSpec as P

HD = 64
MEAN_FLOOR = 0.1
HEAD_FLOOR = 1.0
MESH = pl.DeviceIdType.MESH
VM = pl.BlockSpec(memory_space=pltpu.VMEM)
ANY = pl.BlockSpec(memory_space=pl.ANY)
DMA = pltpu.SemaphoreType.DMA
LIMIT = 48 << 20


def normed_rows(inputs, gain):
    values = inputs.astype(jnp.float32)
    square = jnp.mean(values * values, axis=-1, keepdims=True)
    return (values * lax.rsqrt(jnp.maximum(square, MEAN_FLOOR)) * gain).astype(jnp.bfloat16)


def by_rows(left, weight):
    return lax.dot_general(
        left, weight, (((1,), (1,)), ((), ())), preferred_element_type=jnp.float32
    )


class Place:
    def __init__(self, n_ep, n_tp):
        self.n_ep, self.n_tp, self.ny = n_ep, n_tp, n_tp // 2
        self.e = lax.axis_index("ep")
        self.t = lax.axis_index("tp")
        self.y, self.c = self.t // 2, self.t % 2
        self.partner = self.y * 2 + (1 - self.c)

    def ep(self, k):
        return (self.e + k) % self.n_ep

    def y_at(self, off):
        return (self.y + self.ny + off) % self.ny

    def chip(self, off):
        return self.y_at(off) * 2 + self.c

    def barrier(self):
        sem = pltpu.get_barrier_semaphore()
        for k in range(1, self.n_ep):
            pl.semaphore_signal(
                sem, inc=1, device_id={"ep": self.ep(k), "tp": self.t}, device_id_type=MESH
            )
        for off in range(1, self.ny):
            pl.semaphore_signal(
                sem, inc=1, device_id={"ep": self.e, "tp": self.chip(off)}, device_id_type=MESH
            )
        pl.semaphore_signal(
            sem, inc=1, device_id={"ep": self.e, "tp": self.partner}, device_id_type=MESH
        )
        pl.semaphore_wait(sem, self.n_ep - 1 + self.ny - 1 + 1)


def remote(src, dst, send, recv, e, t):
    return pltpu.make_async_remote_copy(
        src_ref=src,
        dst_ref=dst,
        send_sem=send,
        recv_sem=recv,
        device_id={"ep": e, "tp": t},
        device_id_type=MESH,
    )


class Exchange:
    def __init__(self, place, send, land, sems):
        self.p, self.send, self.land = place, send, land
        self.ssem, self.rsem = sems

    def copy(self, k):
        p = self.p
        d = p.ep(k)
        return remote(
            self.send(d), self.land(p.e), self.ssem.at[d], self.rsem.at[p.e], d, p.t
        )

    def arrival(self, k):
        p = self.p
        s = p.ep(k)
        return remote(self.send(s), self.land(s), self.ssem.at[s], self.rsem.at[s], s, p.t)

    def own(self):
        p = self.p
        return pltpu.make_async_copy(self.send(p.e), self.land(p.e), self.rsem.at[p.e])

    def start(self):
        for k in range(1, self.p.n_ep):
            self.copy(k).start()
        self.own().start()

    def wait_arrival(self, k):
        if k == 0:
            self.own().wait()
        else:
            self.arrival(k).wait_recv()

    def wait_sent(self):
        for k in range(1, self.p.n_ep):
            self.copy(k).wait_send()


class Spread:
    def __init__(self, place, land, sems):
        self.p, self.land = place, land
        self.ys, self.yr, self.ps, self.pr = sems

    def y_copy(self, off, s):
        p = self.p
        block = self.land(p.t, s)
        return remote(
            block, block, self.ys.at[off - 1, s], self.yr.at[off - 1, s], p.e, p.chip(off)
        )

    def y_arrival(self, off, s):
        p = self.p
        block = self.land(p.chip(-off), s)
        return remote(
            block, block, self.ys.at[off - 1, s], self.yr.at[off - 1, s], p.e, p.chip(-off)
        )

    def p_copy(self, off, s):
        p = self.p
        block = self.land(p.chip(-off), s)
        return remote(block, block, self.ps.at[off, s], self.pr.at[off, s], p.e, p.partner)

    def p_arrival(self, off, s):
        p = self.p
        block = self.land(p.y_at(-off) * 2 + (1 - p.c), s)
        return remote(block, block, self.ps.at[off, s], self.pr.at[off, s], p.e, p.partner)

    def first(self, s):
        for off in range(1, self.p.ny):
            self.y_copy(off, s).start()
        self.p_copy(0, s).start()

    def relay(self, s):
        for off in range(1, self.p.ny):
            self.y_arrival(off, s).wait_recv()
            self.p_copy(off, s).start()

    def finish(self, s):
        for off in range(self.p.ny):
            self.p_arrival(off, s).wait_recv()
        self.wait_sent(s)

    def wait_sent(self, s):
        for off in range(self.p.ny):
            self.p_copy(off, s).wait_send()
        for off in range(1, self.p.ny):
            self.y_copy(off, s).wait_send()


def spread_sems(n_ep, n_tp):
    ny = n_tp // 2
    far = max(ny - 1, 1)
    return [DMA((far, n_ep)), DMA((far, n_ep)), DMA((ny, n_ep)), DMA((ny, n_ep))]


def outward_kernel(
    n_ep, n_tp, slots, message, gates, gate_weight, up_weight,
    hidden, message_out, gates_out,
    out, gate_held, up_held, gate_act, up_act,
    s0, s1, m0, m1, g0, g1, w, ys, yr, ps, pr,
):
    p = Place(n_ep, n_tp)
    width = slots.shape[2]

    def cols(t):
        return pl.ds(pl.multiple_of(t * width, width), width)

    def land(t, s):
        return out.at[s, :, cols(t)]

    def multiply(t, opening):
        rows = out[:, :, cols(t)].reshape(hidden.shape[0], width)
        for held, total in ((gate_held, gate_act), (up_held, up_act)):
            product = by_rows(rows, held[:, cols(t)])
            total[...] = product if opening else total[...] + product

    loads = [
        pltpu.make_async_copy(gate_weight, gate_held, w.at[0]),
        pltpu.make_async_copy(up_weight, up_held, w.at[1]),
    ]
    for load in loads:
        load.start()
    p.barrier()
    slot_move = Exchange(p, lambda d: slots.at[d], lambda s: land(p.t, s), (s0, s1))
    gate_move = Exchange(p, lambda d: gates.at[d], lambda s: gates_out.at[s], (g0, g1))
    message_move = Exchange(p, lambda d: message.at[d], lambda s: message_out.at[s], (m0, m1))
    spread = Spread(p, land, (ys, yr, ps, pr))
    slot_move.start()
    gate_move.start()
    message_move.start()
    for k in range(n_ep):
        slot_move.wait_arrival(k)
        spread.first(p.ep(k))
    for load in loads:
        load.wait()
    multiply(p.t, True)
    for k in range(n_ep):
        spread.p_arrival(0, p.ep(k)).wait_recv()
    multiply(p.partner, False)
    for k in range(n_ep):
        spread.relay(p.ep(k))
    for off in range(1, p.ny):
        multiply(p.chip(-off), False)
        for k in range(n_ep):
            spread.p_arrival(off, p.ep(k)).wait_recv()
        multiply(p.y_at(-off) * 2 + (1 - p.c), False)
    gate = gate_act[...]
    hidden[...] = (gate * lax.logistic(gate) * up_act[...]).astype(hidden.dtype)
    for k in range(n_ep):
        gate_move.wait_arrival(k)
        message_move.wait_arrival(k)
        spread.wait_sent(p.ep(k))
    slot_move.wait_sent()
    gate_move.wait_sent()
    message_move.wait_sent()


def homeward_kernel(
    n_ep, n_tp, hidden, down_weight, heads, ret, heads_all,
    partial, down_held, pair, mine, out_y, in_y, final,
    w, h0, h1, a0, a1, r0, r1, q0, q1, ys, yr, ps, pr,
):
    p = Place(n_ep, n_tp)
    ny = p.ny
    width = ret.shape[2]

    def cols(t):
        return pl.ds(pl.multiple_of(t * width, width), width)

    def land(t, s):
        return heads_all.at[t, s]

    load = pltpu.make_async_copy(down_weight, down_held, w.at[0])
    load.start()
    p.barrier()
    head_move = Exchange(p, lambda d: heads.at[d], lambda s: land(p.t, s), (h0, h1))
    spread = Spread(p, land, (ys, yr, ps, pr))
    head_move.start()

    def pair_copy(s, off):
        src = partial.at[s, :, cols(p.y_at(off) * 2 + (1 - p.c))]
        return remote(src, pair.at[s, off], r0.at[s, off], r1.at[s, off], p.e, p.partner)

    def y_copy(s, off, to):
        return remote(
            out_y.at[s, off - 1], in_y.at[s, off - 1],
            q0.at[s, off - 1], q1.at[s, off - 1], p.e, p.chip(to),
        )

    def final_copy(k):
        d = p.ep(k)
        return remote(final.at[d], ret.at[p.e], a0.at[d], a1.at[p.e], d, p.t)

    order = list(range(1, n_ep)) + [0]
    capacity = ret.shape[1]

    def multiply(t):
        product = jnp.dot(
            hidden[...], down_held[:, cols(t)], preferred_element_type=jnp.float32
        )
        partial[:, :, cols(t)] = product.astype(jnp.bfloat16).reshape(n_ep, capacity, width)

    load.wait()
    turns = [*range(1, ny), 0]
    for off in turns:
        multiply(p.y_at(off) * 2 + (1 - p.c))
        multiply(p.chip(off))
        for k in order:
            pair_copy(p.ep(k), off).start()
        for k in order:
            s = p.ep(k)
            pair_copy(s, off).wait_recv()
            both = partial[s, :, cols(p.chip(off))].astype(jnp.float32) + pair[s, off].astype(
                jnp.float32
            )
            if off == 0:
                mine[s] = both
            else:
                out_y[s, off - 1] = both.astype(jnp.bfloat16)
                y_copy(s, off, off).start()
    for k in range(n_ep):
        head_move.wait_arrival(k)
        spread.first(p.ep(k))
    for k in order:
        s = p.ep(k)
        total = mine[s]
        for off in range(1, ny):
            y_copy(s, off, -off).wait_recv()
            total = total + in_y[s, off - 1].astype(jnp.float32)
        if k == 0:
            ret[s] = total.astype(jnp.bfloat16)
        else:
            final[s] = total.astype(jnp.bfloat16)
            final_copy(k).start()
    for k in range(n_ep):
        spread.relay(p.ep(k))
    for k in range(n_ep):
        spread.finish(p.ep(k))
    for k in range(n_ep):
        s = p.ep(k)
        for off in range(ny):
            pair_copy(s, off).wait_send()
        for off in range(1, ny):
            y_copy(s, off, off).wait_send()
    for k in range(1, n_ep):
        s = p.ep(k)
        remote(final.at[s], ret.at[s], a0.at[s], a1.at[s], s, p.t).wait_recv()
        final_copy(k).wait_send()
    head_move.wait_sent()


def outward(slots, message, gates, gate_weight, up_weight, n_ep, n_tp):
    _, capacity, width = slots.shape
    rows, units = n_ep * capacity, gate_weight.shape[0]
    scratch = [
        pltpu.VMEM((n_ep, capacity, width * n_tp), slots.dtype),
        pltpu.VMEM(gate_weight.shape, gate_weight.dtype),
        pltpu.VMEM(up_weight.shape, up_weight.dtype),
        pltpu.VMEM((rows, units), jnp.float32),
        pltpu.VMEM((rows, units), jnp.float32),
    ]
    sems = [DMA((n_ep,))] * 6 + [DMA((2,))] + spread_sems(n_ep, n_tp)
    return pl.pallas_call(
        functools.partial(outward_kernel, n_ep, n_tp),
        out_shape=[
            jax.ShapeDtypeStruct((rows, units), slots.dtype),
            jax.ShapeDtypeStruct(message.shape, message.dtype),
            jax.ShapeDtypeStruct(gates.shape, gates.dtype),
        ],
        in_specs=[VM] * 3 + [ANY] * 2,
        out_specs=[VM] * 3,
        scratch_shapes=scratch + sems,
        compiler_params=pltpu.CompilerParams(collective_id=0, has_side_effects=True),
        name="outward",
    )(slots, message, gates, gate_weight, up_weight)


def homeward(hidden, down_weight, heads, n_ep, n_tp):
    capacity, features = hidden.shape[0] // n_ep, down_weight.shape[1]
    width, ny = features // n_tp, n_tp // 2
    far = max(ny - 1, 1)
    scratch = [
        pltpu.VMEM((n_ep, capacity, features), jnp.bfloat16),
        pltpu.VMEM(down_weight.shape, down_weight.dtype),
        pltpu.VMEM((n_ep, ny, capacity, width), jnp.bfloat16),
        pltpu.VMEM((n_ep, capacity, width), jnp.float32),
        pltpu.VMEM((n_ep, far, capacity, width), jnp.bfloat16),
        pltpu.VMEM((n_ep, far, capacity, width), jnp.bfloat16),
        pltpu.VMEM((n_ep, capacity, width), jnp.bfloat16),
    ]
    sems = [DMA((1,))] + [DMA((n_ep,))] * 4 + [DMA((n_ep, ny))] * 2 + [DMA((n_ep, far))] * 2
    return pl.pallas_call(
        functools.partial(homeward_kernel, n_ep, n_tp),
        out_shape=[
            jax.ShapeDtypeStruct((n_ep, capacity, width), jnp.bfloat16),
            jax.ShapeDtypeStruct((n_tp,) + heads.shape, jnp.bfloat16),
        ],
        in_specs=[VM, ANY, VM],
        out_specs=[VM] * 2,
        scratch_shapes=scratch + sems + spread_sems(n_ep, n_tp),
        compiler_params=pltpu.CompilerParams(collective_id=1, has_side_effects=True),
        name="homeward",
    )(hidden, down_weight, heads)


def on_device(
    mixer_tokens,
    mixer_gain,
    query_weight,
    key_weight,
    value_weight,
    forget_weight,
    forget_bias,
    output_weight,
    expert_tokens,
    expert_gain,
    routes,
    route_weights,
    gate_weight,
    up_weight,
    down_weight,
):
    n_ep, n_tp = lax.axis_size("ep"), lax.axis_size("tp")
    rows, features = mixer_tokens.shape
    local_heads = forget_weight.shape[1]
    share = n_ep // local_heads
    part = rows // share
    width = features // n_tp
    bf16, f32 = jnp.bfloat16, jnp.float32

    expert_normed = normed_rows(expert_tokens, expert_gain)
    token_count, top_count = routes.shape
    capacity = 2 * top_count * token_count // n_ep
    pairs = token_count * top_count
    flat_routes = routes.reshape(-1)
    onehot = flat_routes[:, None] == jnp.arange(n_ep, dtype=jnp.int32)[None, :]
    before = jnp.tril(jnp.ones((pairs, pairs), bf16), -1)
    ranks = jnp.dot(before, onehot.astype(bf16), preferred_element_type=f32)
    slot_rank = jnp.sum(jnp.where(onehot, ranks, 0.0), axis=1).astype(jnp.int32)
    slot_index = (flat_routes * capacity + slot_rank).reshape(token_count, top_count)
    slot_ids = jnp.arange(n_ep * capacity, dtype=jnp.int32)
    picks = [(slot_index[:, j][:, None] == slot_ids[None, :]).astype(bf16) for j in range(top_count)]
    column = lax.axis_index("tp") * width
    own_columns = lax.dynamic_slice_in_dim(expert_normed, column, width, 1)
    slots = lax.dot_general(
        sum(picks[1:], picks[0]), own_columns, (((0,), (0,)), ((), ())),
        preferred_element_type=f32,
    ).astype(bf16).reshape(n_ep, capacity, width)

    normed = normed_rows(mixer_tokens, mixer_gain)
    queries = by_rows(normed, query_weight).astype(bf16)
    key_rows = by_rows(normed, key_weight).astype(bf16)
    value_rows = by_rows(normed, value_weight).astype(bf16)
    pre_gate = jnp.dot(normed, forget_weight, preferred_element_type=f32) + forget_bias
    block_cum = jnp.dot(
        jnp.tril(jnp.ones((rows, rows), f32)), jax.nn.log_sigmoid(pre_gate),
        precision=lax.Precision.HIGHEST, preferred_element_type=f32,
    )
    key_value = jnp.concatenate(
        [
            key_rows.reshape(rows, local_heads, HD).transpose(1, 0, 2),
            value_rows.reshape(rows, local_heads, HD).transpose(1, 0, 2),
        ],
        axis=2,
    )
    key_value = jnp.broadcast_to(
        key_value[:, None], (local_heads, share, rows, 2 * HD)
    ).reshape(n_ep, rows, 2 * HD)
    half = part // 2
    query_parts = queries.reshape(share, 2, half, local_heads, HD).transpose(3, 0, 2, 1, 4)
    query_parts = query_parts.reshape(n_ep, half, 2 * HD)
    message = jnp.concatenate([key_value, query_parts], axis=1)
    gates = jnp.broadcast_to(block_cum.T[:, None, None, :], (local_heads, share, 1, rows))
    gates = gates.reshape(n_ep, 1, rows)

    hidden, all_messages, all_gates = outward(
        slots, message, gates, gate_weight[0], up_weight[0], n_ep, n_tp
    )

    positions = n_ep * rows
    all_gates = all_gates.reshape(n_ep, rows)
    totals = all_gates[:, rows - 1]
    lower = jnp.arange(n_ep)[None, :] < jnp.arange(n_ep)[:, None]
    base = jnp.sum(jnp.where(lower, totals[None, :], 0.0), axis=1)
    cumulative = all_gates + base[:, None]
    keys = all_messages[:, :rows, :HD].reshape(positions, HD)
    values = all_messages[:, :rows, HD:].reshape(positions, HD)
    head_query = all_messages[:, rows:].reshape(n_ep, half, 2, HD).transpose(0, 2, 1, 3)
    head_query = head_query.reshape(n_ep * part, HD)
    first = (lax.axis_index("ep") % share) * part
    query_cum = lax.dynamic_slice_in_dim(cumulative, first, part, 1).reshape(-1)
    query_pos = (
        jnp.arange(n_ep, dtype=jnp.int32)[:, None] * rows
        + first
        + jnp.arange(part, dtype=jnp.int32)[None, :]
    ).reshape(-1)
    key_pos = jnp.arange(positions, dtype=jnp.int32)
    scores = by_rows(head_query, keys) * HD ** (-0.5)
    scores = scores + query_cum[:, None] - cumulative.reshape(-1)[None, :]
    scores = jnp.where(key_pos[None, :] <= query_pos[:, None], scores, -jnp.inf)
    weights = jnp.exp(scores - jnp.max(scores, axis=-1, keepdims=True)).astype(bf16)
    attended = jnp.dot(weights, values, preferred_element_type=f32)
    rescale = lax.rsqrt(jnp.mean(attended * attended, axis=-1, keepdims=True) + HEAD_FLOOR)
    head_out = (attended * rescale).astype(bf16).reshape(n_ep, part, HD)

    returned, heads_all = homeward(hidden, down_weight[0], head_out, n_ep, n_tp)

    heads_all = heads_all.reshape(n_tp, local_heads, share, part, HD).transpose(2, 3, 0, 1, 4)
    heads_all = heads_all.reshape(rows, n_tp * local_heads * HD)
    mixer_output = jnp.dot(heads_all, output_weight, preferred_element_type=f32).astype(bf16)
    returned = returned.reshape(n_ep * capacity, width)
    expert_output = 0.0
    for j in range(top_count):
        picked = jnp.dot(picks[j], returned, preferred_element_type=f32)
        expert_output = expert_output + picked * route_weights[:, j][:, None]
    return (mixer_output, expert_output.astype(bf16))


def lanes_of(shape, dim):
    return lax.broadcasted_iota(jnp.int32, shape, dim)


def flipped(place, bits):
    at, weight = place, 1
    while bits:
        if bits % 2:
            at = at + weight * (1 - 2 * (place // weight % 2))
        bits, weight = bits // 2, weight * 2
    return at


def fused_kernel(
    n_ep, n_tp,
    tokens_a, gain_a, w_q, w_k, w_v, w_f, b_f, w_o, tokens_b, gain_b, routes, route_w,
    w_gate, w_up, w_down,
    out_a, out_b,
    a_held, ga_held, q_held, kv_held, f_held, bf_held, o_held, b_held, gb_held, r_held, rw_held,
    gate_held, up_held, down_held,
    slots, land, w_hi, w_lo, kv_send, q_send, g_send, kv_land, q_land, g_land,
    hidden, pair_send, pair_land, own_part, mine, y_send, y_land, final, ret,
    q_all, q_cum, scores, running, row_max, attended, head_send, heads_all, lhs,
    lsem, s0, s1, ys, yr, ps, pr, k0, k1, x0, x1, q0, q1, g0, g1,
    p0, p1, z0, z1, a0, a1, h0, h1, hy0, hy1, hp0, hp1,
):
    p = Place(n_ep, n_tp)
    ny = p.ny
    bf16, f32 = jnp.bfloat16, jnp.float32
    rows, features = a_held.shape
    tokens = b_held.shape[0]
    _, capacity, width = slots.shape
    local_heads = kv_send.shape[0]
    share = n_ep // local_heads
    part = rows // share
    half = part // 2
    units = gate_held.shape[0]
    near, quarter = range(n_ep // 2), n_ep // 4
    third, second = range(n_ep // 2, 3 * quarter), range(3 * quarter, n_ep)
    groups = [near, second, third]
    own_share = p.e % share
    first = own_share * part

    def cols(t):
        return pl.ds(pl.multiple_of(t * width, width), width)

    def peer(j):
        return flipped(p.e, j)

    barrier = pltpu.get_barrier_semaphore()
    for k in range(1, n_ep):
        pl.semaphore_signal(
            barrier, inc=1, device_id={"ep": p.ep(k), "tp": p.t}, device_id_type=MESH
        )
    for off in range(1, ny):
        pl.semaphore_signal(
            barrier, inc=1, device_id={"ep": p.e, "tp": p.chip(off)}, device_id_type=MESH
        )
    pl.semaphore_signal(
        barrier, inc=1, device_id={"ep": p.e, "tp": p.partner}, device_id_type=MESH
    )

    early = [(tokens_b, b_held), (routes, r_held), (gain_b, gb_held)]
    middle = [(tokens_a, a_held), (gain_a, ga_held), (w_f, f_held), (b_f, bf_held)]
    for h in range(local_heads):
        mine_rows = pl.ds(h * HD, HD)
        middle.append((w_k.at[mine_rows], kv_held.at[pl.ds(2 * h * HD, HD)]))
        middle.append((w_v.at[mine_rows], kv_held.at[pl.ds((2 * h + 1) * HD, HD)]))
    middle.append((w_q, q_held))
    late = [
        (w_gate, gate_held), (w_up, up_held), (w_down, down_held), (route_w, rw_held),
        (w_o, o_held),
    ]
    loads, number = [], 0
    for batch in (early, middle, late):
        made = []
        for src, dst in batch:
            made.append(pltpu.make_async_copy(src, dst, lsem.at[number]))
            number += 1
        loads.append(made)
    early, middle, late = loads
    for load in early + middle:
        load.start()

    for load in early:
        load.wait()
    values = b_held[...].astype(f32)
    square = jnp.mean(values * values, axis=-1, keepdims=True)
    scale = lax.rsqrt(jnp.maximum(square, MEAN_FLOOR))
    own_columns = (b_held[:, cols(p.t)].astype(f32) * scale * gb_held[:, cols(p.t)]).astype(bf16)
    named_by = r_held[...]
    top_count = named_by.shape[0]
    place = lanes_of((n_ep, tokens), 0)
    expert_at, weight = place, 1
    while weight < n_ep:
        flip = (p.e // weight) % 2
        expert_at = expert_at + flip * weight * (1 - 2 * ((place // weight) % 2))
        weight *= 2
    chosen = [named_by[c : c + 1, :] == expert_at for c in range(top_count)]
    named = sum([c.astype(f32) for c in chosen[1:]], chosen[0].astype(f32))
    earlier = (lanes_of((tokens, tokens), 0) < lanes_of((tokens, tokens), 1)).astype(bf16)
    ranks = jnp.dot(named.astype(bf16), earlier, preferred_element_type=f32)
    ranks = jnp.where(named > 0, ranks, -1.0).astype(jnp.int32)
    slot_at = lanes_of((capacity, tokens), 0)
    picks = [ranks[j : j + 1, :] == slot_at for j in range(n_ep)]
    for j in range(n_ep):
        block = jnp.dot(
            picks[j].astype(f32).astype(bf16), own_columns, preferred_element_type=f32
        ).astype(bf16)
        if j == 0:
            land[0, :, cols(p.t)] = block
        else:
            slots[j] = block
    pl.semaphore_wait(barrier, n_ep - 1 + ny - 1 + 1)

    def slot_copy(j):
        return remote(
            slots.at[j], land.at[j, :, cols(p.t)], s0.at[j], s1.at[j], peer(j), p.t
        )

    spread = Spread(p, lambda t, j: land.at[j, :, cols(t)], (ys, yr, ps, pr))
    for j in [*near[1:], *second, *third]:
        slot_copy(j).start()
    spread.first(0)

    for load in middle:
        load.wait()
    for load in late:
        load.start()
    values = a_held[...].astype(f32)
    square = jnp.mean(values * values, axis=-1, keepdims=True)
    scale = lax.rsqrt(jnp.maximum(square, MEAN_FLOOR))
    a_held[...] = (values * scale * ga_held[...]).astype(bf16)
    normed = a_held[...]
    eye = lanes_of((local_heads, local_heads), 0) == lanes_of((local_heads, local_heads), 1)
    bias = jnp.sum(jnp.where(eye, bf_held[...], 0.0), axis=1, keepdims=True)
    gate = by_rows(f_held[...], normed) + bias
    log_gate = jnp.minimum(gate, 0.0) - jnp.log1p(jnp.exp(-jnp.abs(gate)))
    upto = (lanes_of((rows, rows), 0) <= lanes_of((rows, rows), 1)).astype(f32)
    block_cum = jnp.dot(
        log_gate, upto, precision=lax.Precision.HIGHEST, preferred_element_type=f32
    )
    for h in range(local_heads):
        g_send[h] = block_cum[h : h + 1, :]

    def kv_copy(h):
        to = h * share + own_share
        return remote(kv_send.at[h], kv_land.at[p.e], k0.at[h], k1.at[p.e], to, p.t)

    def kv_arrival(n):
        s = (p.e // share + n) % local_heads * share + own_share
        return remote(kv_send.at[0], kv_land.at[s], k0.at[0], k1.at[s], p.e, p.t), s

    def sibling(off):
        return p.e // share * share + (own_share + off) % share

    def kv_relay(s, off):
        return remote(
            kv_land.at[s], kv_land.at[s], x0.at[off, s], x1.at[s], sibling(off), p.t
        )

    def q_copy(k):
        d = p.ep(k)
        return remote(q_send.at[d], q_land.at[p.e], q0.at[d], q1.at[p.e], d, p.t)

    def q_arrival(k):
        s = p.ep(k)
        return remote(q_send.at[s], q_land.at[s], q0.at[s], q1.at[s], s, p.t)

    def g_copy(k):
        d = p.ep(k)
        return remote(g_send.at[d // share], g_land.at[p.e], g0.at[d], g1.at[p.e], d, p.t)

    def g_arrival(k):
        s = p.ep(k)
        return remote(g_send.at[0], g_land.at[s], g0.at[s], g1.at[s], s, p.t)

    key_value = by_rows(normed, kv_held[...]).astype(bf16)
    for h in range(local_heads):
        kv_send[h] = key_value[:, 2 * h * HD : 2 * (h + 1) * HD]
    for n in range(1, local_heads):
        kv_copy((p.e // share + n) % local_heads).start()
    own_head = p.e // share
    kv_land[p.e] = kv_send[own_head]
    for off in range(1, share):
        kv_relay(p.e, off).start()
    slot_copy(1).wait_recv()
    spread.first(1)
    queries = by_rows(normed, q_held[...]) * HD ** (-0.5)
    left = lanes_of((half, 2 * HD), 1) < HD
    for pair in range(local_heads // 2):
        there = queries[:, 2 * pair * HD : 2 * (pair + 1) * HD]
        moved = pltpu.roll(there, HD, 1)
        for x in range(share):
            top, bottom = slice(x * part, x * part + half), slice(x * part + half, (x + 1) * part)
            q_send[2 * pair * share + x] = jnp.where(left, there[top], moved[bottom]).astype(bf16)
            q_send[(2 * pair + 1) * share + x] = jnp.where(
                left, moved[top], there[bottom]
            ).astype(bf16)
    for k in range(1, n_ep):
        q_copy(k).start()
        g_copy(k).start()
    q_land[p.e] = q_send[p.e]
    g_land[p.e] = g_send[own_head]

    def arrive(j):
        slot_copy(j).wait_recv()
        spread.first(j)

    def complete(j):
        spread.relay(j)

    def settle(j):
        for off in range(ny):
            spread.p_arrival(off, j).wait_recv()

    cuts = [(at, min(at + 256, units)) for at in range(0, units, 256)]

    def open_up(g, beside):
        low_row, count = groups[g][0], len(groups[g])
        block = land[low_row : low_row + count].reshape(count * capacity, features)
        lines = slice(low_row * capacity, (low_row + count) * capacity)
        for number, (low, high) in enumerate(cuts):
            gated = by_rows(block, gate_held[low:high])
            upped = by_rows(block, up_held[low:high])
            hidden[lines, low:high] = (gated * lax.logistic(gated) * upped).astype(bf16)
            for act in beside[number : number + 1]:
                act()
        for act in beside[len(cuts) :]:
            act()

    def pair_copy(g, off):
        low_row, count = groups[g][0], len(groups[g])
        lines = pl.ds(low_row * capacity, count * capacity)
        return remote(
            pair_send.at[off, lines], pair_land.at[off, lines], p0.at[g, off], p1.at[g, off],
            p.e, p.partner,
        )

    def y_copy(j, off, to):
        return remote(
            y_send.at[j, off - 1], y_land.at[j, off - 1],
            z0.at[j, off - 1], z1.at[j, off - 1], p.e, p.chip(to),
        )

    turns = [*range(1, ny), 0]

    def close_down(g):
        low_row, count = groups[g][0], len(groups[g])
        lines = slice(low_row * capacity, (low_row + count) * capacity)

        def product(t):
            return jnp.dot(hidden[lines], down_held[:, cols(t)], preferred_element_type=f32)

        for off in turns:
            pair_send[off, lines] = product(p.y_at(off) * 2 + (1 - p.c)).astype(bf16)
            pair_copy(g, off).start()
        for off in turns:
            own_part[lines] = product(p.chip(off))
            pair_copy(g, off).wait_recv()
            both = own_part[lines] + pair_land[off, lines].astype(f32)
            both = both.reshape(count, capacity, width)
            for m in range(count):
                j = low_row + m
                if off == 0:
                    mine[j] = both[m]
                else:
                    y_send[j, off - 1] = both[m].astype(bf16)
                    y_copy(j, off, off).start()

    def final_copy(j):
        return remote(final.at[j], ret.at[j], a0.at[j], a1.at[j], peer(j), p.t)

    def finish(j):
        total = mine[j]
        for off in range(1, ny):
            y_copy(j, off, -off).wait_recv()
            total = total + y_land[j, off - 1].astype(f32)
        if j == 0:
            ret[0] = total.astype(bf16)
        else:
            final[j] = total.astype(bf16)
            final_copy(j).start()

    def kv_forward(n):
        copy, s = kv_arrival(n)
        copy.wait_recv()
        for off in range(1, share):
            kv_relay(s, off).start()

    for j in near[2:]:
        arrive(j)
    for j in near:
        complete(j)
    for j in near:
        settle(j)
    late[0].wait()
    late[1].wait()
    open_up(0, [functools.partial(arrive, j) for j in second])
    for j in second:
        complete(j)
    for j in second:
        settle(j)
    open_up(1, [])
    late[2].wait()
    close_down(1)
    for j in third:
        arrive(j)
    close_down(0)
    for j in third:
        complete(j)
    for j in second:
        finish(j)
    for j in third:
        settle(j)
    open_up(2, [functools.partial(kv_forward, n) for n in range(1, local_heads)])
    close_down(2)
    for j in near:
        finish(j)

    late[3].wait()
    for j in range(n_ep):
        weight = 0.0
        for c in range(top_count):
            weight = weight + jnp.where(
                named_by[c : c + 1, :] == peer(j), rw_held[c : c + 1, :], 0.0
            )
        weight = jnp.where(ranks[j : j + 1, :] == slot_at, weight, 0.0)
        high = weight.astype(bf16)
        w_hi[j * capacity : (j + 1) * capacity] = high
        w_lo[j * capacity : (j + 1) * capacity] = (weight - high.astype(f32)).astype(bf16)

    for k in range(1, n_ep):
        g_arrival(k).wait_recv()
        q_arrival(k).wait_recv()
    for off in range(1, share):
        for n in range(local_heads):
            s = (p.e // share + n) % local_heads * share + (own_share + share - off) % share
            remote(kv_send.at[0], kv_land.at[s], k0.at[0], x1.at[s], p.e, p.t).wait_recv()
    positions = lanes_of((part, rows), 1)
    asked = first + lanes_of((part, rows), 0)
    base = jnp.zeros((1, 1), f32)
    key_cum = []
    last = lanes_of((1, rows), 1) == rows - 1
    for b in range(n_ep):
        block = g_land[b]
        key_cum.append(block + base)
        base = base + jnp.sum(jnp.where(last, block, 0.0), axis=1, keepdims=True)
        at = b * part
        q_cum[at : at + part] = jnp.sum(
            jnp.where(positions == asked, key_cum[b], 0.0), axis=1, keepdims=True
        )
        packed = q_land[b].astype(f32)
        q_all[at : at + half] = jnp.where(left, packed, 0.0).astype(bf16)
        q_all[at + half : at + part] = jnp.where(
            left, pltpu.roll(packed, HD, 1), 0.0
        ).astype(bf16)
    for b in range(n_ep):
        at = b * part
        block = by_rows(q_all[at:], kv_land[b]) + q_cum[at:] - key_cum[b]
        seen = jnp.where(positions <= asked, block[:part], -jnp.inf)
        scores[b, at : at + part] = seen
        if b == 0:
            running[:part] = seen
            running[part:] = block[part:]
        else:
            running[at : at + part] = jnp.maximum(running[at : at + part], seen)
        if b + 1 < n_ep:
            scores[b, at + part :] = block[part:]
            if b > 0:
                running[at + part :] = jnp.maximum(running[at + part :], block[part:])
    row_max[...] = jnp.max(running[...], axis=1, keepdims=True)
    for b in range(n_ep):
        at = b * part
        weights = jnp.exp(scores[b, at:] - row_max[at:]).astype(bf16)
        product = jnp.dot(weights, kv_land[b], preferred_element_type=f32)
        if b == 0:
            attended[...] = product
        else:
            attended[at:] = attended[at:] + product
    right = lanes_of((part, 2 * HD), 1) >= HD
    for b in range(n_ep):
        block = jnp.where(right, attended[b * part : (b + 1) * part], 0.0)
        block = block * lax.rsqrt(
            jnp.sum(block * block, axis=1, keepdims=True) * (1.0 / HD) + HEAD_FLOOR
        )
        moved = pltpu.roll(block, HD, 1)
        head_send[b] = jnp.where(left, moved[:half], block[half:]).astype(bf16)

    def head_copy(k):
        d = peer(k)
        return remote(head_send.at[d], heads_all.at[p.t, p.e], h0.at[d], h1.at[p.e], d, p.t)

    def head_arrival(k):
        s = peer(k)
        return remote(head_send.at[s], heads_all.at[p.t, s], h0.at[s], h1.at[s], s, p.t)

    for k in range(1, n_ep):
        head_copy(k).start()
    heads_all[p.t, p.e] = head_send[p.e]

    for j in third:
        finish(j)

    gather = Spread(p, lambda t, s: heads_all.at[t, s], (hy0, hy1, hp0, hp1))
    gather.first(p.e)
    for k in range(1, n_ep):
        head_arrival(k).wait_recv()
        gather.first(peer(k))
    for k in range(n_ep):
        gather.relay(peer(k))
    for k in range(n_ep):
        for off in range(ny):
            gather.p_arrival(off, peer(k)).wait_recv()
    for t in range(n_tp):
        for pair in range(local_heads // 2):
            lanes = slice((t * local_heads + 2 * pair) * HD, (t * local_heads + 2 * pair + 2) * HD)
            for x in range(share):
                one = heads_all[t, 2 * pair * share + x].astype(f32)
                two = heads_all[t, (2 * pair + 1) * share + x].astype(f32)
                at = x * part
                lhs[at : at + half, lanes] = jnp.where(
                    left, one, pltpu.roll(two, HD, 1)
                ).astype(bf16)
                lhs[at + half : at + part, lanes] = jnp.where(
                    left, pltpu.roll(one, HD, 1), two
                ).astype(bf16)
    late[4].wait()
    out_a[...] = jnp.dot(lhs[...], o_held[...], preferred_element_type=f32).astype(bf16)

    for j in range(1, n_ep):
        final_copy(j).wait_recv()
    returned = ret[...].reshape(n_ep * capacity, width)
    over_slots = (((0,), (0,)), ((), ()))
    total = lax.dot_general(w_hi[...], returned, over_slots, preferred_element_type=f32)
    total = total + lax.dot_general(w_lo[...], returned, over_slots, preferred_element_type=f32)
    out_b[...] = total.astype(bf16)

    for j in range(n_ep):
        spread.wait_sent(j)
        gather.wait_sent(peer(j))
        for off in range(1, ny):
            y_copy(j, off, off).wait_send()
    for j in range(1, n_ep):
        slot_copy(j).wait_send()
        final_copy(j).wait_send()
        q_copy(j).wait_send()
        g_copy(j).wait_send()
        head_copy(j).wait_send()
    for n in range(1, local_heads):
        kv_copy((p.e // share + n) % local_heads).wait_send()
    for n in range(local_heads):
        s = (p.e // share + n) % local_heads * share + own_share
        for off in range(1, share):
            kv_relay(s, off).wait_send()
    for g in range(len(groups)):
        for off in range(ny):
            pair_copy(g, off).wait_send()


def fused_on_device(
    mixer_tokens, mixer_gain, query_weight, key_weight, value_weight, forget_weight,
    forget_bias, output_weight, expert_tokens, expert_gain, routes, route_weights,
    gate_weight, up_weight, down_weight,
):
    n_ep, n_tp = lax.axis_size("ep"), lax.axis_size("tp")
    ny = n_tp // 2
    far = max(ny - 1, 1)
    rows, features = mixer_tokens.shape
    tokens, top_count = routes.shape
    local_heads = forget_weight.shape[1]
    share = n_ep // local_heads
    part = rows // share
    half = part // 2
    width = features // n_tp
    capacity = 2 * top_count * tokens // n_ep
    units = gate_weight.shape[1]
    groups = 3
    asked = n_ep * part
    bf16, f32 = jnp.bfloat16, jnp.float32
    operands = [
        mixer_tokens, mixer_gain.reshape(1, features), query_weight, key_weight, value_weight,
        forget_weight.T, forget_bias, output_weight, expert_tokens,
        expert_gain.reshape(1, features), routes.T, route_weights.T,
        gate_weight[0], up_weight[0], down_weight[0],
    ]
    operands = [pltpu.with_memory_space_constraint(x, pltpu.HBM) for x in operands]
    vmem = pltpu.VMEM
    scratch = [
        vmem((rows, features), bf16), vmem((1, features), f32),
        vmem(query_weight.shape, bf16), vmem((2 * local_heads * HD, features), bf16),
        vmem((local_heads, features), bf16), vmem((1, local_heads), f32),
        vmem(output_weight.shape, bf16), vmem((tokens, features), bf16),
        vmem((1, features), f32), vmem((top_count, tokens), jnp.int32),
        vmem((top_count, tokens), f32),
        vmem((units, features), bf16), vmem((units, features), bf16),
        vmem((units, features), bf16),
        vmem((n_ep, capacity, width), bf16), vmem((n_ep, capacity, features), bf16),
        vmem((n_ep * capacity, tokens), bf16), vmem((n_ep * capacity, tokens), bf16),
        vmem((local_heads, rows, 2 * HD), bf16), vmem((n_ep, half, 2 * HD), bf16),
        vmem((local_heads, 1, rows), f32),
        vmem((n_ep, rows, 2 * HD), bf16), vmem((n_ep, half, 2 * HD), bf16),
        vmem((n_ep, 1, rows), f32),
        vmem((n_ep * capacity, units), bf16),
        vmem((ny, n_ep * capacity, width), bf16),
        vmem((ny, n_ep * capacity, width), bf16),
        vmem((n_ep * capacity, width), f32),
        vmem((n_ep, capacity, width), f32),
        vmem((n_ep, far, capacity, width), bf16), vmem((n_ep, far, capacity, width), bf16),
        vmem((n_ep, capacity, width), bf16), vmem((n_ep, capacity, width), bf16),
        vmem((asked, 2 * HD), bf16), vmem((asked, 1), f32),
        vmem((n_ep, asked, rows), f32), vmem((asked, rows), f32), vmem((asked, 1), f32),
        vmem((asked, 2 * HD), f32), vmem((n_ep, half, 2 * HD), bf16),
        vmem((n_tp, n_ep, half, 2 * HD), bf16), vmem((rows, n_tp * local_heads * HD), bf16),
    ]
    sems = [DMA((13 + 2 * local_heads,)), DMA((n_ep,)), DMA((n_ep,))] + spread_sems(n_ep, n_tp)
    sems += [DMA((local_heads,)), DMA((n_ep,)), DMA((share, n_ep)), DMA((n_ep,))]
    sems += [DMA((n_ep,))] * 4 + [DMA((groups, ny))] * 2 + [DMA((n_ep, far))] * 2
    sems += [DMA((n_ep,))] * 4 + spread_sems(n_ep, n_tp)
    return pl.pallas_call(
        functools.partial(fused_kernel, n_ep, n_tp),
        out_shape=[
            jax.ShapeDtypeStruct((rows, width), bf16),
            jax.ShapeDtypeStruct((tokens, width), bf16),
        ],
        in_specs=[ANY] * len(operands),
        out_specs=[VM] * 2,
        scratch_shapes=scratch + sems,
        compiler_params=pltpu.CompilerParams(
            collective_id=2, has_side_effects=True, vmem_limit_bytes=LIMIT
        ),
        name="fused",
    )(*operands)


def deliver_kernel(one, two, one_out, two_out, sem):
    copies = [
        pltpu.make_async_copy(one, one_out, sem.at[0]),
        pltpu.make_async_copy(two, two_out, sem.at[1]),
    ]
    for copy in copies:
        copy.start()
    for copy in copies:
        copy.wait()


def deliver(one, two):
    return pl.pallas_call(
        deliver_kernel,
        out_shape=[
            jax.ShapeDtypeStruct(one.shape, one.dtype),
            jax.ShapeDtypeStruct(two.shape, two.dtype),
        ],
        in_specs=[ANY] * 2,
        out_specs=[ANY] * 2,
        scratch_shapes=[DMA((2,))],
        compiler_params=pltpu.CompilerParams(vmem_limit_bytes=1 << 20),
        name="deliver",
    )(one, two)


def choose(*arguments):
    n_ep = lax.axis_size("ep")
    rows, local_heads = arguments[0].shape[0], arguments[5].shape[1]
    share = n_ep // local_heads
    packed = local_heads % 2 == 0 and n_ep % local_heads == 0
    packed = packed and n_ep >= 8 and n_ep & (n_ep - 1) == 0
    if packed and rows % (32 * share) == 0:
        return tuple(deliver(*fused_on_device(*arguments)))
    return on_device(*arguments)


def solution(mesh):
    in_specs = (
        P("ep", None),
        P(),
        P("tp", None),
        P("tp", None),
        P("tp", None),
        P(None, "tp"),
        P("ep", "tp"),
        P(None, "tp"),
        P("ep", None),
        P(),
        P("ep", None),
        P("ep", None),
        P("ep", "tp", None),
        P("ep", "tp", None),
        P("ep", "tp", None),
    )
    out_specs = (P("ep", "tp"), P("ep", "tp"))
    return jax.shard_map(
        choose, mesh=mesh, in_specs=in_specs, out_specs=out_specs, check_vma=False
    )
```

```python
import functools

import jax
import jax.numpy as jnp
from jax import lax
from jax.experimental import pallas as pl
from jax.experimental.pallas import tpu as pltpu
from jax.sharding import PartitionSpec as P

HD = 64
MEAN_FLOOR = 0.1
HEAD_FLOOR = 1.0
MESH = pl.DeviceIdType.MESH
VM = pl.BlockSpec(memory_space=pltpu.VMEM)
ANY = pl.BlockSpec(memory_space=pl.ANY)
DMA = pltpu.SemaphoreType.DMA
LIMIT = 48 << 20


def normed_rows(inputs, gain):
    values = inputs.astype(jnp.float32)
    square = jnp.mean(values * values, axis=-1, keepdims=True)
    return (values * lax.rsqrt(jnp.maximum(square, MEAN_FLOOR)) * gain).astype(jnp.bfloat16)


def by_rows(left, weight):
    return lax.dot_general(
        left, weight, (((1,), (1,)), ((), ())), preferred_element_type=jnp.float32
    )


class Place:
    def __init__(self, n_ep, n_tp):
        self.n_ep, self.n_tp, self.ny = n_ep, n_tp, n_tp // 2
        self.e = lax.axis_index("ep")
        self.t = lax.axis_index("tp")
        self.y, self.c = self.t // 2, self.t % 2
        self.partner = self.y * 2 + (1 - self.c)

    def ep(self, k):
        return (self.e + k) % self.n_ep

    def y_at(self, off):
        return (self.y + self.ny + off) % self.ny

    def chip(self, off):
        return self.y_at(off) * 2 + self.c

    def barrier(self):
        sem = pltpu.get_barrier_semaphore()
        for k in range(1, self.n_ep):
            pl.semaphore_signal(
                sem, inc=1, device_id={"ep": self.ep(k), "tp": self.t}, device_id_type=MESH
            )
        for off in range(1, self.ny):
            pl.semaphore_signal(
                sem, inc=1, device_id={"ep": self.e, "tp": self.chip(off)}, device_id_type=MESH
            )
        pl.semaphore_signal(
            sem, inc=1, device_id={"ep": self.e, "tp": self.partner}, device_id_type=MESH
        )
        pl.semaphore_wait(sem, self.n_ep - 1 + self.ny - 1 + 1)


def remote(src, dst, send, recv, e, t):
    return pltpu.make_async_remote_copy(
        src_ref=src,
        dst_ref=dst,
        send_sem=send,
        recv_sem=recv,
        device_id={"ep": e, "tp": t},
        device_id_type=MESH,
    )


class Exchange:
    def __init__(self, place, send, land, sems):
        self.p, self.send, self.land = place, send, land
        self.ssem, self.rsem = sems

    def copy(self, k):
        p = self.p
        d = p.ep(k)
        return remote(
            self.send(d), self.land(p.e), self.ssem.at[d], self.rsem.at[p.e], d, p.t
        )

    def arrival(self, k):
        p = self.p
        s = p.ep(k)
        return remote(self.send(s), self.land(s), self.ssem.at[s], self.rsem.at[s], s, p.t)

    def own(self):
        p = self.p
        return pltpu.make_async_copy(self.send(p.e), self.land(p.e), self.rsem.at[p.e])

    def start(self):
        for k in range(1, self.p.n_ep):
            self.copy(k).start()
        self.own().start()

    def wait_arrival(self, k):
        if k == 0:
            self.own().wait()
        else:
            self.arrival(k).wait_recv()

    def wait_sent(self):
        for k in range(1, self.p.n_ep):
            self.copy(k).wait_send()


class Spread:
    def __init__(self, place, land, sems):
        self.p, self.land = place, land
        self.ys, self.yr, self.ps, self.pr = sems

    def y_copy(self, off, s):
        p = self.p
        block = self.land(p.t, s)
        return remote(
            block, block, self.ys.at[off - 1, s], self.yr.at[off - 1, s], p.e, p.chip(off)
        )

    def y_arrival(self, off, s):
        p = self.p
        block = self.land(p.chip(-off), s)
        return remote(
            block, block, self.ys.at[off - 1, s], self.yr.at[off - 1, s], p.e, p.chip(-off)
        )

    def p_copy(self, off, s):
        p = self.p
        block = self.land(p.chip(-off), s)
        return remote(block, block, self.ps.at[off, s], self.pr.at[off, s], p.e, p.partner)

    def p_arrival(self, off, s):
        p = self.p
        block = self.land(p.y_at(-off) * 2 + (1 - p.c), s)
        return remote(block, block, self.ps.at[off, s], self.pr.at[off, s], p.e, p.partner)

    def first(self, s):
        for off in range(1, self.p.ny):
            self.y_copy(off, s).start()
        self.p_copy(0, s).start()

    def relay(self, s):
        for off in range(1, self.p.ny):
            self.y_arrival(off, s).wait_recv()
            self.p_copy(off, s).start()

    def finish(self, s):
        for off in range(self.p.ny):
            self.p_arrival(off, s).wait_recv()
        self.wait_sent(s)

    def wait_sent(self, s):
        for off in range(self.p.ny):
            self.p_copy(off, s).wait_send()
        for off in range(1, self.p.ny):
            self.y_copy(off, s).wait_send()


def spread_sems(n_ep, n_tp):
    ny = n_tp // 2
    far = max(ny - 1, 1)
    return [DMA((far, n_ep)), DMA((far, n_ep)), DMA((ny, n_ep)), DMA((ny, n_ep))]


def outward_kernel(
    n_ep, n_tp, slots, message, gates, gate_weight, up_weight,
    hidden, message_out, gates_out,
    out, gate_held, up_held, gate_act, up_act,
    s0, s1, m0, m1, g0, g1, w, ys, yr, ps, pr,
):
    p = Place(n_ep, n_tp)
    width = slots.shape[2]

    def cols(t):
        return pl.ds(pl.multiple_of(t * width, width), width)

    def land(t, s):
        return out.at[s, :, cols(t)]

    def multiply(t, opening):
        rows = out[:, :, cols(t)].reshape(hidden.shape[0], width)
        for held, total in ((gate_held, gate_act), (up_held, up_act)):
            product = by_rows(rows, held[:, cols(t)])
            total[...] = product if opening else total[...] + product

    loads = [
        pltpu.make_async_copy(gate_weight, gate_held, w.at[0]),
        pltpu.make_async_copy(up_weight, up_held, w.at[1]),
    ]
    for load in loads:
        load.start()
    p.barrier()
    slot_move = Exchange(p, lambda d: slots.at[d], lambda s: land(p.t, s), (s0, s1))
    gate_move = Exchange(p, lambda d: gates.at[d], lambda s: gates_out.at[s], (g0, g1))
    message_move = Exchange(p, lambda d: message.at[d], lambda s: message_out.at[s], (m0, m1))
    spread = Spread(p, land, (ys, yr, ps, pr))
    slot_move.start()
    gate_move.start()
    message_move.start()
    for k in range(n_ep):
        slot_move.wait_arrival(k)
        spread.first(p.ep(k))
    for load in loads:
        load.wait()
    multiply(p.t, True)
    for k in range(n_ep):
        spread.p_arrival(0, p.ep(k)).wait_recv()
    multiply(p.partner, False)
    for k in range(n_ep):
        spread.relay(p.ep(k))
    for off in range(1, p.ny):
        multiply(p.chip(-off), False)
        for k in range(n_ep):
            spread.p_arrival(off, p.ep(k)).wait_recv()
        multiply(p.y_at(-off) * 2 + (1 - p.c), False)
    gate = gate_act[...]
    hidden[...] = (gate * lax.logistic(gate) * up_act[...]).astype(hidden.dtype)
    for k in range(n_ep):
        gate_move.wait_arrival(k)
        message_move.wait_arrival(k)
        spread.wait_sent(p.ep(k))
    slot_move.wait_sent()
    gate_move.wait_sent()
    message_move.wait_sent()


def homeward_kernel(
    n_ep, n_tp, hidden, down_weight, heads, ret, heads_all,
    partial, down_held, pair, mine, out_y, in_y, final,
    w, h0, h1, a0, a1, r0, r1, q0, q1, ys, yr, ps, pr,
):
    p = Place(n_ep, n_tp)
    ny = p.ny
    width = ret.shape[2]

    def cols(t):
        return pl.ds(pl.multiple_of(t * width, width), width)

    def land(t, s):
        return heads_all.at[t, s]

    load = pltpu.make_async_copy(down_weight, down_held, w.at[0])
    load.start()
    p.barrier()
    head_move = Exchange(p, lambda d: heads.at[d], lambda s: land(p.t, s), (h0, h1))
    spread = Spread(p, land, (ys, yr, ps, pr))
    head_move.start()

    def pair_copy(s, off):
        src = partial.at[s, :, cols(p.y_at(off) * 2 + (1 - p.c))]
        return remote(src, pair.at[s, off], r0.at[s, off], r1.at[s, off], p.e, p.partner)

    def y_copy(s, off, to):
        return remote(
            out_y.at[s, off - 1], in_y.at[s, off - 1],
            q0.at[s, off - 1], q1.at[s, off - 1], p.e, p.chip(to),
        )

    def final_copy(k):
        d = p.ep(k)
        return remote(final.at[d], ret.at[p.e], a0.at[d], a1.at[p.e], d, p.t)

    order = list(range(1, n_ep)) + [0]
    capacity = ret.shape[1]

    def multiply(t):
        product = jnp.dot(
            hidden[...], down_held[:, cols(t)], preferred_element_type=jnp.float32
        )
        partial[:, :, cols(t)] = product.astype(jnp.bfloat16).reshape(n_ep, capacity, width)

    load.wait()
    turns = [*range(1, ny), 0]
    for off in turns:
        multiply(p.y_at(off) * 2 + (1 - p.c))
        multiply(p.chip(off))
        for k in order:
            pair_copy(p.ep(k), off).start()
        for k in order:
            s = p.ep(k)
            pair_copy(s, off).wait_recv()
            both = partial[s, :, cols(p.chip(off))].astype(jnp.float32) + pair[s, off].astype(
                jnp.float32
            )
            if off == 0:
                mine[s] = both
            else:
                out_y[s, off - 1] = both.astype(jnp.bfloat16)
                y_copy(s, off, off).start()
    for k in range(n_ep):
        head_move.wait_arrival(k)
        spread.first(p.ep(k))
    for k in order:
        s = p.ep(k)
        total = mine[s]
        for off in range(1, ny):
            y_copy(s, off, -off).wait_recv()
            total = total + in_y[s, off - 1].astype(jnp.float32)
        if k == 0:
            ret[s] = total.astype(jnp.bfloat16)
        else:
            final[s] = total.astype(jnp.bfloat16)
            final_copy(k).start()
    for k in range(n_ep):
        spread.relay(p.ep(k))
    for k in range(n_ep):
        spread.finish(p.ep(k))
    for k in range(n_ep):
        s = p.ep(k)
        for off in range(ny):
            pair_copy(s, off).wait_send()
        for off in range(1, ny):
            y_copy(s, off, off).wait_send()
    for k in range(1, n_ep):
        s = p.ep(k)
        remote(final.at[s], ret.at[s], a0.at[s], a1.at[s], s, p.t).wait_recv()
        final_copy(k).wait_send()
    head_move.wait_sent()


def outward(slots, message, gates, gate_weight, up_weight, n_ep, n_tp):
    _, capacity, width = slots.shape
    rows, units = n_ep * capacity, gate_weight.shape[0]
    scratch = [
        pltpu.VMEM((n_ep, capacity, width * n_tp), slots.dtype),
        pltpu.VMEM(gate_weight.shape, gate_weight.dtype),
        pltpu.VMEM(up_weight.shape, up_weight.dtype),
        pltpu.VMEM((rows, units), jnp.float32),
        pltpu.VMEM((rows, units), jnp.float32),
    ]
    sems = [DMA((n_ep,))] * 6 + [DMA((2,))] + spread_sems(n_ep, n_tp)
    return pl.pallas_call(
        functools.partial(outward_kernel, n_ep, n_tp),
        out_shape=[
            jax.ShapeDtypeStruct((rows, units), slots.dtype),
            jax.ShapeDtypeStruct(message.shape, message.dtype),
            jax.ShapeDtypeStruct(gates.shape, gates.dtype),
        ],
        in_specs=[VM] * 3 + [ANY] * 2,
        out_specs=[VM] * 3,
        scratch_shapes=scratch + sems,
        compiler_params=pltpu.CompilerParams(collective_id=0, has_side_effects=True),
        name="outward",
    )(slots, message, gates, gate_weight, up_weight)


def homeward(hidden, down_weight, heads, n_ep, n_tp):
    capacity, features = hidden.shape[0] // n_ep, down_weight.shape[1]
    width, ny = features // n_tp, n_tp // 2
    far = max(ny - 1, 1)
    scratch = [
        pltpu.VMEM((n_ep, capacity, features), jnp.bfloat16),
        pltpu.VMEM(down_weight.shape, down_weight.dtype),
        pltpu.VMEM((n_ep, ny, capacity, width), jnp.bfloat16),
        pltpu.VMEM((n_ep, capacity, width), jnp.float32),
        pltpu.VMEM((n_ep, far, capacity, width), jnp.bfloat16),
        pltpu.VMEM((n_ep, far, capacity, width), jnp.bfloat16),
        pltpu.VMEM((n_ep, capacity, width), jnp.bfloat16),
    ]
    sems = [DMA((1,))] + [DMA((n_ep,))] * 4 + [DMA((n_ep, ny))] * 2 + [DMA((n_ep, far))] * 2
    return pl.pallas_call(
        functools.partial(homeward_kernel, n_ep, n_tp),
        out_shape=[
            jax.ShapeDtypeStruct((n_ep, capacity, width), jnp.bfloat16),
            jax.ShapeDtypeStruct((n_tp,) + heads.shape, jnp.bfloat16),
        ],
        in_specs=[VM, ANY, VM],
        out_specs=[VM] * 2,
        scratch_shapes=scratch + sems + spread_sems(n_ep, n_tp),
        compiler_params=pltpu.CompilerParams(collective_id=1, has_side_effects=True),
        name="homeward",
    )(hidden, down_weight, heads)


def on_device(
    mixer_tokens,
    mixer_gain,
    query_weight,
    key_weight,
    value_weight,
    forget_weight,
    forget_bias,
    output_weight,
    expert_tokens,
    expert_gain,
    routes,
    route_weights,
    gate_weight,
    up_weight,
    down_weight,
):
    n_ep, n_tp = lax.axis_size("ep"), lax.axis_size("tp")
    rows, features = mixer_tokens.shape
    local_heads = forget_weight.shape[1]
    share = n_ep // local_heads
    part = rows // share
    width = features // n_tp
    bf16, f32 = jnp.bfloat16, jnp.float32

    expert_normed = normed_rows(expert_tokens, expert_gain)
    token_count, top_count = routes.shape
    capacity = 2 * top_count * token_count // n_ep
    pairs = token_count * top_count
    flat_routes = routes.reshape(-1)
    onehot = flat_routes[:, None] == jnp.arange(n_ep, dtype=jnp.int32)[None, :]
    before = jnp.tril(jnp.ones((pairs, pairs), bf16), -1)
    ranks = jnp.dot(before, onehot.astype(bf16), preferred_element_type=f32)
    slot_rank = jnp.sum(jnp.where(onehot, ranks, 0.0), axis=1).astype(jnp.int32)
    slot_index = (flat_routes * capacity + slot_rank).reshape(token_count, top_count)
    slot_ids = jnp.arange(n_ep * capacity, dtype=jnp.int32)
    picks = [(slot_index[:, j][:, None] == slot_ids[None, :]).astype(bf16) for j in range(top_count)]
    column = lax.axis_index("tp") * width
    own_columns = lax.dynamic_slice_in_dim(expert_normed, column, width, 1)
    slots = lax.dot_general(
        sum(picks[1:], picks[0]), own_columns, (((0,), (0,)), ((), ())),
        preferred_element_type=f32,
    ).astype(bf16).reshape(n_ep, capacity, width)

    normed = normed_rows(mixer_tokens, mixer_gain)
    queries = by_rows(normed, query_weight).astype(bf16)
    key_rows = by_rows(normed, key_weight).astype(bf16)
    value_rows = by_rows(normed, value_weight).astype(bf16)
    pre_gate = jnp.dot(normed, forget_weight, preferred_element_type=f32) + forget_bias
    block_cum = jnp.dot(
        jnp.tril(jnp.ones((rows, rows), f32)), jax.nn.log_sigmoid(pre_gate),
        precision=lax.Precision.HIGHEST, preferred_element_type=f32,
    )
    key_value = jnp.concatenate(
        [
            key_rows.reshape(rows, local_heads, HD).transpose(1, 0, 2),
            value_rows.reshape(rows, local_heads, HD).transpose(1, 0, 2),
        ],
        axis=2,
    )
    key_value = jnp.broadcast_to(
        key_value[:, None], (local_heads, share, rows, 2 * HD)
    ).reshape(n_ep, rows, 2 * HD)
    half = part // 2
    query_parts = queries.reshape(share, 2, half, local_heads, HD).transpose(3, 0, 2, 1, 4)
    query_parts = query_parts.reshape(n_ep, half, 2 * HD)
    message = jnp.concatenate([key_value, query_parts], axis=1)
    gates = jnp.broadcast_to(block_cum.T[:, None, None, :], (local_heads, share, 1, rows))
    gates = gates.reshape(n_ep, 1, rows)

    hidden, all_messages, all_gates = outward(
        slots, message, gates, gate_weight[0], up_weight[0], n_ep, n_tp
    )

    positions = n_ep * rows
    all_gates = all_gates.reshape(n_ep, rows)
    totals = all_gates[:, rows - 1]
    lower = jnp.arange(n_ep)[None, :] < jnp.arange(n_ep)[:, None]
    base = jnp.sum(jnp.where(lower, totals[None, :], 0.0), axis=1)
    cumulative = all_gates + base[:, None]
    keys = all_messages[:, :rows, :HD].reshape(positions, HD)
    values = all_messages[:, :rows, HD:].reshape(positions, HD)
    head_query = all_messages[:, rows:].reshape(n_ep, half, 2, HD).transpose(0, 2, 1, 3)
    head_query = head_query.reshape(n_ep * part, HD)
    first = (lax.axis_index("ep") % share) * part
    query_cum = lax.dynamic_slice_in_dim(cumulative, first, part, 1).reshape(-1)
    query_pos = (
        jnp.arange(n_ep, dtype=jnp.int32)[:, None] * rows
        + first
        + jnp.arange(part, dtype=jnp.int32)[None, :]
    ).reshape(-1)
    key_pos = jnp.arange(positions, dtype=jnp.int32)
    scores = by_rows(head_query, keys) * HD ** (-0.5)
    scores = scores + query_cum[:, None] - cumulative.reshape(-1)[None, :]
    scores = jnp.where(key_pos[None, :] <= query_pos[:, None], scores, -jnp.inf)
    weights = jnp.exp(scores - jnp.max(scores, axis=-1, keepdims=True)).astype(bf16)
    attended = jnp.dot(weights, values, preferred_element_type=f32)
    rescale = lax.rsqrt(jnp.mean(attended * attended, axis=-1, keepdims=True) + HEAD_FLOOR)
    head_out = (attended * rescale).astype(bf16).reshape(n_ep, part, HD)

    returned, heads_all = homeward(hidden, down_weight[0], head_out, n_ep, n_tp)

    heads_all = heads_all.reshape(n_tp, local_heads, share, part, HD).transpose(2, 3, 0, 1, 4)
    heads_all = heads_all.reshape(rows, n_tp * local_heads * HD)
    mixer_output = jnp.dot(heads_all, output_weight, preferred_element_type=f32).astype(bf16)
    returned = returned.reshape(n_ep * capacity, width)
    expert_output = 0.0
    for j in range(top_count):
        picked = jnp.dot(picks[j], returned, preferred_element_type=f32)
        expert_output = expert_output + picked * route_weights[:, j][:, None]
    return (mixer_output, expert_output.astype(bf16))


def lanes_of(shape, dim):
    return lax.broadcasted_iota(jnp.int32, shape, dim)


def flipped(place, bits):
    at, weight = place, 1
    while bits:
        if bits % 2:
            at = at + weight * (1 - 2 * (place // weight % 2))
        bits, weight = bits // 2, weight * 2
    return at


def fused_kernel(
    n_ep, n_tp,
    tokens_a, gain_a, w_q, w_k, w_v, w_f, b_f, w_o, tokens_b, gain_b, routes, route_w,
    w_gate, w_up, w_down,
    out_a, out_b,
    a_held, ga_held, q_held, kv_held, f_held, bf_held, o_held, b_held, gb_held, r_held, rw_held,
    gate_held, up_held, down_held,
    slots, land, w_hi, w_lo, kv_send, q_send, g_send, kv_land, q_land, g_land,
    hidden, pair_send, pair_land, own_part, mine, y_send, y_land, final, ret,
    q_all, q_cum, scores, running, row_max, attended, head_send, heads_all, lhs,
    lsem, s0, s1, ys, yr, ps, pr, k0, k1, x0, x1, q0, q1, g0, g1,
    p0, p1, z0, z1, a0, a1, h0, h1, hy0, hy1, hp0, hp1,
):
    p = Place(n_ep, n_tp)
    ny = p.ny
    bf16, f32 = jnp.bfloat16, jnp.float32
    rows, features = a_held.shape
    tokens = b_held.shape[0]
    _, capacity, width = slots.shape
    local_heads = kv_send.shape[0]
    share = n_ep // local_heads
    part = rows // share
    half = part // 2
    units = gate_held.shape[0]
    near, quarter = range(n_ep // 2), n_ep // 4
    third, second = range(n_ep // 2, 3 * quarter), range(3 * quarter, n_ep)
    groups = [near, second, third]
    own_share = p.e % share
    first = own_share * part

    def cols(t):
        return pl.ds(pl.multiple_of(t * width, width), width)

    def peer(j):
        return flipped(p.e, j)

    barrier = pltpu.get_barrier_semaphore()
    for k in range(1, n_ep):
        pl.semaphore_signal(
            barrier, inc=1, device_id={"ep": p.ep(k), "tp": p.t}, device_id_type=MESH
        )
    for off in range(1, ny):
        pl.semaphore_signal(
            barrier, inc=1, device_id={"ep": p.e, "tp": p.chip(off)}, device_id_type=MESH
        )
    pl.semaphore_signal(
        barrier, inc=1, device_id={"ep": p.e, "tp": p.partner}, device_id_type=MESH
    )

    early = [(tokens_b, b_held), (routes, r_held), (gain_b, gb_held)]
    middle = [(tokens_a, a_held), (gain_a, ga_held), (w_f, f_held), (b_f, bf_held)]
    for h in range(local_heads):
        mine_rows = pl.ds(h * HD, HD)
        middle.append((w_k.at[mine_rows], kv_held.at[pl.ds(2 * h * HD, HD)]))
        middle.append((w_v.at[mine_rows], kv_held.at[pl.ds((2 * h + 1) * HD, HD)]))
    middle.append((w_q, q_held))
    late = [
        (w_gate, gate_held), (w_up, up_held), (w_down, down_held), (route_w, rw_held),
        (w_o, o_held),
    ]
    loads, number = [], 0
    for batch in (early, middle, late):
        made = []
        for src, dst in batch:
            made.append(pltpu.make_async_copy(src, dst, lsem.at[number]))
            number += 1
        loads.append(made)
    early, middle, late = loads
    for load in early + middle:
        load.start()

    for load in early:
        load.wait()
    values = b_held[...].astype(f32)
    square = jnp.mean(values * values, axis=-1, keepdims=True)
    scale = lax.rsqrt(jnp.maximum(square, MEAN_FLOOR))
    own_columns = (b_held[:, cols(p.t)].astype(f32) * scale * gb_held[:, cols(p.t)]).astype(bf16)
    named_by = r_held[...]
    top_count = named_by.shape[0]
    place = lanes_of((n_ep, tokens), 0)
    expert_at, weight = place, 1
    while weight < n_ep:
        flip = (p.e // weight) % 2
        expert_at = expert_at + flip * weight * (1 - 2 * ((place // weight) % 2))
        weight *= 2
    chosen = [named_by[c : c + 1, :] == expert_at for c in range(top_count)]
    named = sum([c.astype(f32) for c in chosen[1:]], chosen[0].astype(f32))
    earlier = (lanes_of((tokens, tokens), 0) < lanes_of((tokens, tokens), 1)).astype(bf16)
    ranks = jnp.dot(named.astype(bf16), earlier, preferred_element_type=f32)
    ranks = jnp.where(named > 0, ranks, -1.0).astype(jnp.int32)
    slot_at = lanes_of((capacity, tokens), 0)
    picks = [ranks[j : j + 1, :] == slot_at for j in range(n_ep)]
    for j in range(n_ep):
        block = jnp.dot(
            picks[j].astype(f32).astype(bf16), own_columns, preferred_element_type=f32
        ).astype(bf16)
        if j == 0:
            land[0, :, cols(p.t)] = block
        else:
            slots[j] = block
    pl.semaphore_wait(barrier, n_ep - 1 + ny - 1 + 1)

    def slot_copy(j):
        return remote(
            slots.at[j], land.at[j, :, cols(p.t)], s0.at[j], s1.at[j], peer(j), p.t
        )

    spread = Spread(p, lambda t, j: land.at[j, :, cols(t)], (ys, yr, ps, pr))
    for j in [*near[1:], *second, *third]:
        slot_copy(j).start()
    spread.first(0)

    for load in middle:
        load.wait()
    for load in late:
        load.start()
    values = a_held[...].astype(f32)
    square = jnp.mean(values * values, axis=-1, keepdims=True)
    scale = lax.rsqrt(jnp.maximum(square, MEAN_FLOOR))
    a_held[...] = (values * scale * ga_held[...]).astype(bf16)
    normed = a_held[...]
    eye = lanes_of((local_heads, local_heads), 0) == lanes_of((local_heads, local_heads), 1)
    bias = jnp.sum(jnp.where(eye, bf_held[...], 0.0), axis=1, keepdims=True)
    gate = by_rows(f_held[...], normed) + bias
    log_gate = jnp.minimum(gate, 0.0) - jnp.log1p(jnp.exp(-jnp.abs(gate)))
    upto = (lanes_of((rows, rows), 0) <= lanes_of((rows, rows), 1)).astype(f32)
    block_cum = jnp.dot(
        log_gate, upto, precision=lax.Precision.HIGHEST, preferred_element_type=f32
    )
    for h in range(local_heads):
        g_send[h] = block_cum[h : h + 1, :]

    def kv_copy(h):
        to = h * share + own_share
        return remote(kv_send.at[h], kv_land.at[p.e], k0.at[h], k1.at[p.e], to, p.t)

    def kv_arrival(n):
        s = (p.e // share + n) % local_heads * share + own_share
        return remote(kv_send.at[0], kv_land.at[s], k0.at[0], k1.at[s], p.e, p.t), s

    def sibling(off):
        return p.e // share * share + (own_share + off) % share

    def kv_relay(s, off):
        return remote(
            kv_land.at[s], kv_land.at[s], x0.at[off, s], x1.at[s], sibling(off), p.t
        )

    def q_copy(k):
        d = p.ep(k)
        return remote(q_send.at[d], q_land.at[p.e], q0.at[d], q1.at[p.e], d, p.t)

    def q_arrival(k):
        s = p.ep(k)
        return remote(q_send.at[s], q_land.at[s], q0.at[s], q1.at[s], s, p.t)

    def g_copy(k):
        d = p.ep(k)
        return remote(g_send.at[d // share], g_land.at[p.e], g0.at[d], g1.at[p.e], d, p.t)

    def g_arrival(k):
        s = p.ep(k)
        return remote(g_send.at[0], g_land.at[s], g0.at[s], g1.at[s], s, p.t)

    key_value = by_rows(normed, kv_held[...]).astype(bf16)
    for h in range(local_heads):
        kv_send[h] = key_value[:, 2 * h * HD : 2 * (h + 1) * HD]
    for n in range(1, local_heads):
        kv_copy((p.e // share + n) % local_heads).start()
    own_head = p.e // share
    kv_land[p.e] = kv_send[own_head]
    for off in range(1, share):
        kv_relay(p.e, off).start()
    slot_copy(1).wait_recv()
    spread.first(1)
    queries = by_rows(normed, q_held[...]) * HD ** (-0.5)
    left = lanes_of((half, 2 * HD), 1) < HD
    for pair in range(local_heads // 2):
        there = queries[:, 2 * pair * HD : 2 * (pair + 1) * HD]
        moved = pltpu.roll(there, HD, 1)
        for x in range(share):
            top, bottom = slice(x * part, x * part + half), slice(x * part + half, (x + 1) * part)
            q_send[2 * pair * share + x] = jnp.where(left, there[top], moved[bottom]).astype(bf16)
            q_send[(2 * pair + 1) * share + x] = jnp.where(
                left, moved[top], there[bottom]
            ).astype(bf16)
    for k in range(1, n_ep):
        q_copy(k).start()
        g_copy(k).start()
    q_land[p.e] = q_send[p.e]
    g_land[p.e] = g_send[own_head]

    def arrive(j):
        slot_copy(j).wait_recv()
        spread.first(j)

    def complete(j):
        spread.relay(j)

    def settle(j):
        for off in range(ny):
            spread.p_arrival(off, j).wait_recv()

    cuts = [(at, min(at + 256, units)) for at in range(0, units, 256)]

    def serve(beside, number, count):
        for act, *given in beside[len(beside) * number // count : len(beside) * (number + 1) // count]:
            act(*given)

    def open_up(g, beside):
        low_row, count = groups[g][0], len(groups[g])
        block = land[low_row : low_row + count].reshape(count * capacity, features)
        lines = slice(low_row * capacity, (low_row + count) * capacity)
        for number, (low, high) in enumerate(cuts):
            gated = by_rows(block, gate_held[low:high])
            upped = by_rows(block, up_held[low:high])
            hidden[lines, low:high] = (gated * lax.logistic(gated) * upped).astype(bf16)
            serve(beside, number, len(cuts))

    def pair_copy(g, off):
        low_row, count = groups[g][0], len(groups[g])
        lines = pl.ds(low_row * capacity, count * capacity)
        return remote(
            pair_send.at[off, lines], pair_land.at[off, lines], p0.at[g, off], p1.at[g, off],
            p.e, p.partner,
        )

    def y_copy(j, off, to):
        return remote(
            y_send.at[j, off - 1], y_land.at[j, off - 1],
            z0.at[j, off - 1], z1.at[j, off - 1], p.e, p.chip(to),
        )

    turns = [*range(1, ny), 0]

    def close_down(g, beside):
        low_row, count = groups[g][0], len(groups[g])
        lines = slice(low_row * capacity, (low_row + count) * capacity)

        def product(t):
            return jnp.dot(hidden[lines], down_held[:, cols(t)], preferred_element_type=f32)

        for number, off in enumerate(turns):
            pair_send[off, lines] = product(p.y_at(off) * 2 + (1 - p.c)).astype(bf16)
            pair_copy(g, off).start()
            serve(beside, number, 2 * ny)
        for number, off in enumerate(turns):
            own_part[lines] = product(p.chip(off))
            serve(beside, ny + number, 2 * ny)
            pair_copy(g, off).wait_recv()
            both = own_part[lines] + pair_land[off, lines].astype(f32)
            both = both.reshape(count, capacity, width)
            for m in range(count):
                j = low_row + m
                if off == 0:
                    mine[j] = both[m]
                else:
                    y_send[j, off - 1] = both[m].astype(bf16)
                    y_copy(j, off, off).start()

    def final_copy(j):
        return remote(final.at[j], ret.at[j], a0.at[j], a1.at[j], peer(j), p.t)

    def finish(j):
        total = mine[j]
        for off in range(1, ny):
            y_copy(j, off, -off).wait_recv()
            total = total + y_land[j, off - 1].astype(f32)
        if j == 0:
            ret[0] = total.astype(bf16)
        else:
            final[j] = total.astype(bf16)
            final_copy(j).start()

    def kv_forward(n):
        copy, s = kv_arrival(n)
        copy.wait_recv()
        for off in range(1, share):
            kv_relay(s, off).start()

    half_near, some = len(near) // 2, len(second) // 2
    for j in near[2 : half_near + 1]:
        arrive(j)
    complete(0)
    for j in near[half_near + 1 :]:
        arrive(j)
    for j in near[1:-1]:
        complete(j)
    for j in second[:some]:
        arrive(j)
    complete(near[-1])
    for j in second[some:]:
        arrive(j)
    for j in near:
        settle(j)
    late[0].wait()
    late[1].wait()
    open_up(
        0,
        [(arrive, j) for j in third[:some]]
        + [(complete, j) for j in second]
        + [(arrive, j) for j in third[some:]],
    )
    for j in second:
        settle(j)
    open_up(1, [(complete, j) for j in third])
    late[2].wait()
    close_down(1, [])
    for j in third:
        settle(j)
    open_up(2, [(kv_forward, n) for n in range(1, local_heads)])
    close_down(2, [(finish, j) for j in second])
    close_down(0, [])

    late[3].wait()
    for j in range(n_ep):
        weight = 0.0
        for c in range(top_count):
            weight = weight + jnp.where(
                named_by[c : c + 1, :] == peer(j), rw_held[c : c + 1, :], 0.0
            )
        weight = jnp.where(ranks[j : j + 1, :] == slot_at, weight, 0.0)
        high = weight.astype(bf16)
        w_hi[j * capacity : (j + 1) * capacity] = high
        w_lo[j * capacity : (j + 1) * capacity] = (weight - high.astype(f32)).astype(bf16)

    for k in range(1, n_ep):
        g_arrival(k).wait_recv()
        q_arrival(k).wait_recv()
    for off in range(1, share):
        for n in range(local_heads):
            s = (p.e // share + n) % local_heads * share + (own_share + share - off) % share
            remote(kv_send.at[0], kv_land.at[s], k0.at[0], x1.at[s], p.e, p.t).wait_recv()
    positions = lanes_of((part, rows), 1)
    asked = first + lanes_of((part, rows), 0)
    base = jnp.zeros((1, 1), f32)
    key_cum = []
    last = lanes_of((1, rows), 1) == rows - 1
    for b in range(n_ep):
        block = g_land[b]
        key_cum.append(block + base)
        base = base + jnp.sum(jnp.where(last, block, 0.0), axis=1, keepdims=True)
        at = b * part
        q_cum[at : at + part] = jnp.sum(
            jnp.where(positions == asked, key_cum[b], 0.0), axis=1, keepdims=True
        )
        packed = q_land[b].astype(f32)
        q_all[at : at + half] = jnp.where(left, packed, 0.0).astype(bf16)
        q_all[at + half : at + part] = jnp.where(
            left, pltpu.roll(packed, HD, 1), 0.0
        ).astype(bf16)
    for b in range(n_ep):
        at = b * part
        block = by_rows(q_all[at:], kv_land[b]) + q_cum[at:] - key_cum[b]
        seen = jnp.where(positions <= asked, block[:part], -jnp.inf)
        scores[b, at : at + part] = seen
        if b == 0:
            running[:part] = seen
            running[part:] = block[part:]
        else:
            running[at : at + part] = jnp.maximum(running[at : at + part], seen)
        if b + 1 < n_ep:
            scores[b, at + part :] = block[part:]
            if b > 0:
                running[at + part :] = jnp.maximum(running[at + part :], block[part:])
    for j in third:
        finish(j)
    row_max[...] = jnp.max(running[...], axis=1, keepdims=True)
    for b in range(n_ep):
        at = b * part
        weights = jnp.exp(scores[b, at:] - row_max[at:]).astype(bf16)
        product = jnp.dot(weights, kv_land[b], preferred_element_type=f32)
        if b == 0:
            attended[...] = product
        else:
            attended[at:] = attended[at:] + product
    right = lanes_of((part, 2 * HD), 1) >= HD
    for b in range(n_ep):
        block = jnp.where(right, attended[b * part : (b + 1) * part], 0.0)
        block = block * lax.rsqrt(
            jnp.sum(block * block, axis=1, keepdims=True) * (1.0 / HD) + HEAD_FLOOR
        )
        moved = pltpu.roll(block, HD, 1)
        head_send[b] = jnp.where(left, moved[:half], block[half:]).astype(bf16)

    def head_copy(k):
        d = peer(k)
        return remote(head_send.at[d], heads_all.at[p.t, p.e], h0.at[d], h1.at[p.e], d, p.t)

    def head_arrival(k):
        s = peer(k)
        return remote(head_send.at[s], heads_all.at[p.t, s], h0.at[s], h1.at[s], s, p.t)

    for k in range(1, n_ep):
        head_copy(k).start()
    heads_all[p.t, p.e] = head_send[p.e]

    for j in near:
        finish(j)

    gather = Spread(p, lambda t, s: heads_all.at[t, s], (hy0, hy1, hp0, hp1))
    gather.first(p.e)
    for k in range(1, n_ep):
        head_arrival(k).wait_recv()
        gather.first(peer(k))
    for k in range(n_ep):
        gather.relay(peer(k))
    for k in range(n_ep):
        for off in range(ny):
            gather.p_arrival(off, peer(k)).wait_recv()
    for t in range(n_tp):
        for pair in range(local_heads // 2):
            lanes = slice((t * local_heads + 2 * pair) * HD, (t * local_heads + 2 * pair + 2) * HD)
            for x in range(share):
                one = heads_all[t, 2 * pair * share + x].astype(f32)
                two = heads_all[t, (2 * pair + 1) * share + x].astype(f32)
                at = x * part
                lhs[at : at + half, lanes] = jnp.where(
                    left, one, pltpu.roll(two, HD, 1)
                ).astype(bf16)
                lhs[at + half : at + part, lanes] = jnp.where(
                    left, pltpu.roll(one, HD, 1), two
                ).astype(bf16)
    late[4].wait()
    out_a[...] = jnp.dot(lhs[...], o_held[...], preferred_element_type=f32).astype(bf16)

    for j in range(1, n_ep):
        final_copy(j).wait_recv()
    returned = ret[...].reshape(n_ep * capacity, width)
    over_slots = (((0,), (0,)), ((), ()))
    total = lax.dot_general(w_hi[...], returned, over_slots, preferred_element_type=f32)
    total = total + lax.dot_general(w_lo[...], returned, over_slots, preferred_element_type=f32)
    out_b[...] = total.astype(bf16)

    for j in range(n_ep):
        spread.wait_sent(j)
        gather.wait_sent(peer(j))
        for off in range(1, ny):
            y_copy(j, off, off).wait_send()
    for j in range(1, n_ep):
        slot_copy(j).wait_send()
        final_copy(j).wait_send()
        q_copy(j).wait_send()
        g_copy(j).wait_send()
        head_copy(j).wait_send()
    for n in range(1, local_heads):
        kv_copy((p.e // share + n) % local_heads).wait_send()
    for n in range(local_heads):
        s = (p.e // share + n) % local_heads * share + own_share
        for off in range(1, share):
            kv_relay(s, off).wait_send()
    for g in range(len(groups)):
        for off in range(ny):
            pair_copy(g, off).wait_send()


def fused_on_device(
    mixer_tokens, mixer_gain, query_weight, key_weight, value_weight, forget_weight,
    forget_bias, output_weight, expert_tokens, expert_gain, routes, route_weights,
    gate_weight, up_weight, down_weight,
):
    n_ep, n_tp = lax.axis_size("ep"), lax.axis_size("tp")
    ny = n_tp // 2
    far = max(ny - 1, 1)
    rows, features = mixer_tokens.shape
    tokens, top_count = routes.shape
    local_heads = forget_weight.shape[1]
    share = n_ep // local_heads
    part = rows // share
    half = part // 2
    width = features // n_tp
    capacity = 2 * top_count * tokens // n_ep
    units = gate_weight.shape[1]
    groups = 3
    asked = n_ep * part
    bf16, f32 = jnp.bfloat16, jnp.float32
    operands = [
        mixer_tokens, mixer_gain.reshape(1, features), query_weight, key_weight, value_weight,
        forget_weight.T, forget_bias, output_weight, expert_tokens,
        expert_gain.reshape(1, features), routes.T, route_weights.T,
        gate_weight[0], up_weight[0], down_weight[0],
    ]
    operands = [pltpu.with_memory_space_constraint(x, pltpu.HBM) for x in operands]
    vmem = pltpu.VMEM
    scratch = [
        vmem((rows, features), bf16), vmem((1, features), f32),
        vmem(query_weight.shape, bf16), vmem((2 * local_heads * HD, features), bf16),
        vmem((local_heads, features), bf16), vmem((1, local_heads), f32),
        vmem(output_weight.shape, bf16), vmem((tokens, features), bf16),
        vmem((1, features), f32), vmem((top_count, tokens), jnp.int32),
        vmem((top_count, tokens), f32),
        vmem((units, features), bf16), vmem((units, features), bf16),
        vmem((units, features), bf16),
        vmem((n_ep, capacity, width), bf16), vmem((n_ep, capacity, features), bf16),
        vmem((n_ep * capacity, tokens), bf16), vmem((n_ep * capacity, tokens), bf16),
        vmem((local_heads, rows, 2 * HD), bf16), vmem((n_ep, half, 2 * HD), bf16),
        vmem((local_heads, 1, rows), f32),
        vmem((n_ep, rows, 2 * HD), bf16), vmem((n_ep, half, 2 * HD), bf16),
        vmem((n_ep, 1, rows), f32),
        vmem((n_ep * capacity, units), bf16),
        vmem((ny, n_ep * capacity, width), bf16),
        vmem((ny, n_ep * capacity, width), bf16),
        vmem((n_ep * capacity, width), f32),
        vmem((n_ep, capacity, width), f32),
        vmem((n_ep, far, capacity, width), bf16), vmem((n_ep, far, capacity, width), bf16),
        vmem((n_ep, capacity, width), bf16), vmem((n_ep, capacity, width), bf16),
        vmem((asked, 2 * HD), bf16), vmem((asked, 1), f32),
        vmem((n_ep, asked, rows), f32), vmem((asked, rows), f32), vmem((asked, 1), f32),
        vmem((asked, 2 * HD), f32), vmem((n_ep, half, 2 * HD), bf16),
        vmem((n_tp, n_ep, half, 2 * HD), bf16), vmem((rows, n_tp * local_heads * HD), bf16),
    ]
    sems = [DMA((13 + 2 * local_heads,)), DMA((n_ep,)), DMA((n_ep,))] + spread_sems(n_ep, n_tp)
    sems += [DMA((local_heads,)), DMA((n_ep,)), DMA((share, n_ep)), DMA((n_ep,))]
    sems += [DMA((n_ep,))] * 4 + [DMA((groups, ny))] * 2 + [DMA((n_ep, far))] * 2
    sems += [DMA((n_ep,))] * 4 + spread_sems(n_ep, n_tp)
    return pl.pallas_call(
        functools.partial(fused_kernel, n_ep, n_tp),
        out_shape=[
            jax.ShapeDtypeStruct((rows, width), bf16),
            jax.ShapeDtypeStruct((tokens, width), bf16),
        ],
        in_specs=[ANY] * len(operands),
        out_specs=[VM] * 2,
        scratch_shapes=scratch + sems,
        compiler_params=pltpu.CompilerParams(
            collective_id=2, has_side_effects=True, vmem_limit_bytes=LIMIT
        ),
        name="fused",
    )(*operands)


def deliver_kernel(one, two, one_out, two_out, sem):
    copies = [
        pltpu.make_async_copy(one, one_out, sem.at[0]),
        pltpu.make_async_copy(two, two_out, sem.at[1]),
    ]
    for copy in copies:
        copy.start()
    for copy in copies:
        copy.wait()


def deliver(one, two):
    return pl.pallas_call(
        deliver_kernel,
        out_shape=[
            jax.ShapeDtypeStruct(one.shape, one.dtype),
            jax.ShapeDtypeStruct(two.shape, two.dtype),
        ],
        in_specs=[ANY] * 2,
        out_specs=[ANY] * 2,
        scratch_shapes=[DMA((2,))],
        compiler_params=pltpu.CompilerParams(vmem_limit_bytes=1 << 20),
        name="deliver",
    )(one, two)


def choose(*arguments):
    n_ep = lax.axis_size("ep")
    rows, local_heads = arguments[0].shape[0], arguments[5].shape[1]
    share = n_ep // local_heads
    packed = local_heads % 2 == 0 and n_ep % local_heads == 0
    packed = packed and n_ep >= 8 and n_ep & (n_ep - 1) == 0
    if packed and rows % (32 * share) == 0:
        return tuple(deliver(*fused_on_device(*arguments)))
    return on_device(*arguments)


def solution(mesh):
    in_specs = (
        P("ep", None),
        P(),
        P("tp", None),
        P("tp", None),
        P("tp", None),
        P(None, "tp"),
        P("ep", "tp"),
        P(None, "tp"),
        P("ep", None),
        P(),
        P("ep", None),
        P("ep", None),
        P("ep", "tp", None),
        P("ep", "tp", None),
        P("ep", "tp", None),
    )
    out_specs = (P("ep", "tp"), P("ep", "tp"))
    return jax.shard_map(
        choose, mesh=mesh, in_specs=in_specs, out_specs=out_specs, check_vma=False
    )
```

```python
import functools

import jax
import jax.numpy as jnp
from jax import lax
from jax.experimental import pallas as pl
from jax.experimental.pallas import tpu as pltpu
from jax.sharding import PartitionSpec as P

HD = 64
MEAN_FLOOR = 0.1
HEAD_FLOOR = 1.0
MESH = pl.DeviceIdType.MESH
VM = pl.BlockSpec(memory_space=pltpu.VMEM)
ANY = pl.BlockSpec(memory_space=pl.ANY)
DMA = pltpu.SemaphoreType.DMA
LIMIT = 48 << 20


def normed_rows(inputs, gain):
    values = inputs.astype(jnp.float32)
    square = jnp.mean(values * values, axis=-1, keepdims=True)
    return (values * lax.rsqrt(jnp.maximum(square, MEAN_FLOOR)) * gain).astype(jnp.bfloat16)


def by_rows(left, weight):
    return lax.dot_general(
        left, weight, (((1,), (1,)), ((), ())), preferred_element_type=jnp.float32
    )


class Place:
    def __init__(self, n_ep, n_tp):
        self.n_ep, self.n_tp, self.ny = n_ep, n_tp, n_tp // 2
        self.e = lax.axis_index("ep")
        self.t = lax.axis_index("tp")
        self.y, self.c = self.t // 2, self.t % 2
        self.partner = self.y * 2 + (1 - self.c)

    def ep(self, k):
        return (self.e + k) % self.n_ep

    def y_at(self, off):
        return (self.y + self.ny + off) % self.ny

    def chip(self, off):
        return self.y_at(off) * 2 + self.c

    def barrier(self):
        sem = pltpu.get_barrier_semaphore()
        for k in range(1, self.n_ep):
            pl.semaphore_signal(
                sem, inc=1, device_id={"ep": self.ep(k), "tp": self.t}, device_id_type=MESH
            )
        for off in range(1, self.ny):
            pl.semaphore_signal(
                sem, inc=1, device_id={"ep": self.e, "tp": self.chip(off)}, device_id_type=MESH
            )
        pl.semaphore_signal(
            sem, inc=1, device_id={"ep": self.e, "tp": self.partner}, device_id_type=MESH
        )
        pl.semaphore_wait(sem, self.n_ep - 1 + self.ny - 1 + 1)


def remote(src, dst, send, recv, e, t):
    return pltpu.make_async_remote_copy(
        src_ref=src,
        dst_ref=dst,
        send_sem=send,
        recv_sem=recv,
        device_id={"ep": e, "tp": t},
        device_id_type=MESH,
    )


class Exchange:
    def __init__(self, place, send, land, sems):
        self.p, self.send, self.land = place, send, land
        self.ssem, self.rsem = sems

    def copy(self, k):
        p = self.p
        d = p.ep(k)
        return remote(
            self.send(d), self.land(p.e), self.ssem.at[d], self.rsem.at[p.e], d, p.t
        )

    def arrival(self, k):
        p = self.p
        s = p.ep(k)
        return remote(self.send(s), self.land(s), self.ssem.at[s], self.rsem.at[s], s, p.t)

    def own(self):
        p = self.p
        return pltpu.make_async_copy(self.send(p.e), self.land(p.e), self.rsem.at[p.e])

    def start(self):
        for k in range(1, self.p.n_ep):
            self.copy(k).start()
        self.own().start()

    def wait_arrival(self, k):
        if k == 0:
            self.own().wait()
        else:
            self.arrival(k).wait_recv()

    def wait_sent(self):
        for k in range(1, self.p.n_ep):
            self.copy(k).wait_send()


class Spread:
    def __init__(self, place, land, sems):
        self.p, self.land = place, land
        self.ys, self.yr, self.ps, self.pr = sems

    def y_copy(self, off, s):
        p = self.p
        block = self.land(p.t, s)
        return remote(
            block, block, self.ys.at[off - 1, s], self.yr.at[off - 1, s], p.e, p.chip(off)
        )

    def y_arrival(self, off, s):
        p = self.p
        block = self.land(p.chip(-off), s)
        return remote(
            block, block, self.ys.at[off - 1, s], self.yr.at[off - 1, s], p.e, p.chip(-off)
        )

    def p_copy(self, off, s):
        p = self.p
        block = self.land(p.chip(-off), s)
        return remote(block, block, self.ps.at[off, s], self.pr.at[off, s], p.e, p.partner)

    def p_arrival(self, off, s):
        p = self.p
        block = self.land(p.y_at(-off) * 2 + (1 - p.c), s)
        return remote(block, block, self.ps.at[off, s], self.pr.at[off, s], p.e, p.partner)

    def first(self, s):
        for off in range(1, self.p.ny):
            self.y_copy(off, s).start()
        self.p_copy(0, s).start()

    def relay(self, s):
        for off in range(1, self.p.ny):
            self.y_arrival(off, s).wait_recv()
            self.p_copy(off, s).start()

    def finish(self, s):
        for off in range(self.p.ny):
            self.p_arrival(off, s).wait_recv()
        self.wait_sent(s)

    def wait_sent(self, s):
        for off in range(self.p.ny):
            self.p_copy(off, s).wait_send()
        for off in range(1, self.p.ny):
            self.y_copy(off, s).wait_send()


def spread_sems(n_ep, n_tp):
    ny = n_tp // 2
    far = max(ny - 1, 1)
    return [DMA((far, n_ep)), DMA((far, n_ep)), DMA((ny, n_ep)), DMA((ny, n_ep))]


def outward_kernel(
    n_ep, n_tp, slots, message, gates, gate_weight, up_weight,
    hidden, message_out, gates_out,
    out, gate_held, up_held, gate_act, up_act,
    s0, s1, m0, m1, g0, g1, w, ys, yr, ps, pr,
):
    p = Place(n_ep, n_tp)
    width = slots.shape[2]

    def cols(t):
        return pl.ds(pl.multiple_of(t * width, width), width)

    def land(t, s):
        return out.at[s, :, cols(t)]

    def multiply(t, opening):
        rows = out[:, :, cols(t)].reshape(hidden.shape[0], width)
        for held, total in ((gate_held, gate_act), (up_held, up_act)):
            product = by_rows(rows, held[:, cols(t)])
            total[...] = product if opening else total[...] + product

    loads = [
        pltpu.make_async_copy(gate_weight, gate_held, w.at[0]),
        pltpu.make_async_copy(up_weight, up_held, w.at[1]),
    ]
    for load in loads:
        load.start()
    p.barrier()
    slot_move = Exchange(p, lambda d: slots.at[d], lambda s: land(p.t, s), (s0, s1))
    gate_move = Exchange(p, lambda d: gates.at[d], lambda s: gates_out.at[s], (g0, g1))
    message_move = Exchange(p, lambda d: message.at[d], lambda s: message_out.at[s], (m0, m1))
    spread = Spread(p, land, (ys, yr, ps, pr))
    slot_move.start()
    gate_move.start()
    message_move.start()
    for k in range(n_ep):
        slot_move.wait_arrival(k)
        spread.first(p.ep(k))
    for load in loads:
        load.wait()
    multiply(p.t, True)
    for k in range(n_ep):
        spread.p_arrival(0, p.ep(k)).wait_recv()
    multiply(p.partner, False)
    for k in range(n_ep):
        spread.relay(p.ep(k))
    for off in range(1, p.ny):
        multiply(p.chip(-off), False)
        for k in range(n_ep):
            spread.p_arrival(off, p.ep(k)).wait_recv()
        multiply(p.y_at(-off) * 2 + (1 - p.c), False)
    gate = gate_act[...]
    hidden[...] = (gate * lax.logistic(gate) * up_act[...]).astype(hidden.dtype)
    for k in range(n_ep):
        gate_move.wait_arrival(k)
        message_move.wait_arrival(k)
        spread.wait_sent(p.ep(k))
    slot_move.wait_sent()
    gate_move.wait_sent()
    message_move.wait_sent()


def homeward_kernel(
    n_ep, n_tp, hidden, down_weight, heads, ret, heads_all,
    partial, down_held, pair, mine, out_y, in_y, final,
    w, h0, h1, a0, a1, r0, r1, q0, q1, ys, yr, ps, pr,
):
    p = Place(n_ep, n_tp)
    ny = p.ny
    width = ret.shape[2]

    def cols(t):
        return pl.ds(pl.multiple_of(t * width, width), width)

    def land(t, s):
        return heads_all.at[t, s]

    load = pltpu.make_async_copy(down_weight, down_held, w.at[0])
    load.start()
    p.barrier()
    head_move = Exchange(p, lambda d: heads.at[d], lambda s: land(p.t, s), (h0, h1))
    spread = Spread(p, land, (ys, yr, ps, pr))
    head_move.start()

    def pair_copy(s, off):
        src = partial.at[s, :, cols(p.y_at(off) * 2 + (1 - p.c))]
        return remote(src, pair.at[s, off], r0.at[s, off], r1.at[s, off], p.e, p.partner)

    def y_copy(s, off, to):
        return remote(
            out_y.at[s, off - 1], in_y.at[s, off - 1],
            q0.at[s, off - 1], q1.at[s, off - 1], p.e, p.chip(to),
        )

    def final_copy(k):
        d = p.ep(k)
        return remote(final.at[d], ret.at[p.e], a0.at[d], a1.at[p.e], d, p.t)

    order = list(range(1, n_ep)) + [0]
    capacity = ret.shape[1]

    def multiply(t):
        product = jnp.dot(
            hidden[...], down_held[:, cols(t)], preferred_element_type=jnp.float32
        )
        partial[:, :, cols(t)] = product.astype(jnp.bfloat16).reshape(n_ep, capacity, width)

    load.wait()
    turns = [*range(1, ny), 0]
    for off in turns:
        multiply(p.y_at(off) * 2 + (1 - p.c))
        multiply(p.chip(off))
        for k in order:
            pair_copy(p.ep(k), off).start()
        for k in order:
            s = p.ep(k)
            pair_copy(s, off).wait_recv()
            both = partial[s, :, cols(p.chip(off))].astype(jnp.float32) + pair[s, off].astype(
                jnp.float32
            )
            if off == 0:
                mine[s] = both
            else:
                out_y[s, off - 1] = both.astype(jnp.bfloat16)
                y_copy(s, off, off).start()
    for k in range(n_ep):
        head_move.wait_arrival(k)
        spread.first(p.ep(k))
    for k in order:
        s = p.ep(k)
        total = mine[s]
        for off in range(1, ny):
            y_copy(s, off, -off).wait_recv()
            total = total + in_y[s, off - 1].astype(jnp.float32)
        if k == 0:
            ret[s] = total.astype(jnp.bfloat16)
        else:
            final[s] = total.astype(jnp.bfloat16)
            final_copy(k).start()
    for k in range(n_ep):
        spread.relay(p.ep(k))
    for k in range(n_ep):
        spread.finish(p.ep(k))
    for k in range(n_ep):
        s = p.ep(k)
        for off in range(ny):
            pair_copy(s, off).wait_send()
        for off in range(1, ny):
            y_copy(s, off, off).wait_send()
    for k in range(1, n_ep):
        s = p.ep(k)
        remote(final.at[s], ret.at[s], a0.at[s], a1.at[s], s, p.t).wait_recv()
        final_copy(k).wait_send()
    head_move.wait_sent()


def outward(slots, message, gates, gate_weight, up_weight, n_ep, n_tp):
    _, capacity, width = slots.shape
    rows, units = n_ep * capacity, gate_weight.shape[0]
    scratch = [
        pltpu.VMEM((n_ep, capacity, width * n_tp), slots.dtype),
        pltpu.VMEM(gate_weight.shape, gate_weight.dtype),
        pltpu.VMEM(up_weight.shape, up_weight.dtype),
        pltpu.VMEM((rows, units), jnp.float32),
        pltpu.VMEM((rows, units), jnp.float32),
    ]
    sems = [DMA((n_ep,))] * 6 + [DMA((2,))] + spread_sems(n_ep, n_tp)
    return pl.pallas_call(
        functools.partial(outward_kernel, n_ep, n_tp),
        out_shape=[
            jax.ShapeDtypeStruct((rows, units), slots.dtype),
            jax.ShapeDtypeStruct(message.shape, message.dtype),
            jax.ShapeDtypeStruct(gates.shape, gates.dtype),
        ],
        in_specs=[VM] * 3 + [ANY] * 2,
        out_specs=[VM] * 3,
        scratch_shapes=scratch + sems,
        compiler_params=pltpu.CompilerParams(collective_id=0, has_side_effects=True),
        name="outward",
    )(slots, message, gates, gate_weight, up_weight)


def homeward(hidden, down_weight, heads, n_ep, n_tp):
    capacity, features = hidden.shape[0] // n_ep, down_weight.shape[1]
    width, ny = features // n_tp, n_tp // 2
    far = max(ny - 1, 1)
    scratch = [
        pltpu.VMEM((n_ep, capacity, features), jnp.bfloat16),
        pltpu.VMEM(down_weight.shape, down_weight.dtype),
        pltpu.VMEM((n_ep, ny, capacity, width), jnp.bfloat16),
        pltpu.VMEM((n_ep, capacity, width), jnp.float32),
        pltpu.VMEM((n_ep, far, capacity, width), jnp.bfloat16),
        pltpu.VMEM((n_ep, far, capacity, width), jnp.bfloat16),
        pltpu.VMEM((n_ep, capacity, width), jnp.bfloat16),
    ]
    sems = [DMA((1,))] + [DMA((n_ep,))] * 4 + [DMA((n_ep, ny))] * 2 + [DMA((n_ep, far))] * 2
    return pl.pallas_call(
        functools.partial(homeward_kernel, n_ep, n_tp),
        out_shape=[
            jax.ShapeDtypeStruct((n_ep, capacity, width), jnp.bfloat16),
            jax.ShapeDtypeStruct((n_tp,) + heads.shape, jnp.bfloat16),
        ],
        in_specs=[VM, ANY, VM],
        out_specs=[VM] * 2,
        scratch_shapes=scratch + sems + spread_sems(n_ep, n_tp),
        compiler_params=pltpu.CompilerParams(collective_id=1, has_side_effects=True),
        name="homeward",
    )(hidden, down_weight, heads)


def on_device(
    mixer_tokens,
    mixer_gain,
    query_weight,
    key_weight,
    value_weight,
    forget_weight,
    forget_bias,
    output_weight,
    expert_tokens,
    expert_gain,
    routes,
    route_weights,
    gate_weight,
    up_weight,
    down_weight,
):
    n_ep, n_tp = lax.axis_size("ep"), lax.axis_size("tp")
    rows, features = mixer_tokens.shape
    local_heads = forget_weight.shape[1]
    share = n_ep // local_heads
    part = rows // share
    width = features // n_tp
    bf16, f32 = jnp.bfloat16, jnp.float32

    expert_normed = normed_rows(expert_tokens, expert_gain)
    token_count, top_count = routes.shape
    capacity = 2 * top_count * token_count // n_ep
    pairs = token_count * top_count
    flat_routes = routes.reshape(-1)
    onehot = flat_routes[:, None] == jnp.arange(n_ep, dtype=jnp.int32)[None, :]
    before = jnp.tril(jnp.ones((pairs, pairs), bf16), -1)
    ranks = jnp.dot(before, onehot.astype(bf16), preferred_element_type=f32)
    slot_rank = jnp.sum(jnp.where(onehot, ranks, 0.0), axis=1).astype(jnp.int32)
    slot_index = (flat_routes * capacity + slot_rank).reshape(token_count, top_count)
    slot_ids = jnp.arange(n_ep * capacity, dtype=jnp.int32)
    picks = [(slot_index[:, j][:, None] == slot_ids[None, :]).astype(bf16) for j in range(top_count)]
    column = lax.axis_index("tp") * width
    own_columns = lax.dynamic_slice_in_dim(expert_normed, column, width, 1)
    slots = lax.dot_general(
        sum(picks[1:], picks[0]), own_columns, (((0,), (0,)), ((), ())),
        preferred_element_type=f32,
    ).astype(bf16).reshape(n_ep, capacity, width)

    normed = normed_rows(mixer_tokens, mixer_gain)
    queries = by_rows(normed, query_weight).astype(bf16)
    key_rows = by_rows(normed, key_weight).astype(bf16)
    value_rows = by_rows(normed, value_weight).astype(bf16)
    pre_gate = jnp.dot(normed, forget_weight, preferred_element_type=f32) + forget_bias
    block_cum = jnp.dot(
        jnp.tril(jnp.ones((rows, rows), f32)), jax.nn.log_sigmoid(pre_gate),
        precision=lax.Precision.HIGHEST, preferred_element_type=f32,
    )
    key_value = jnp.concatenate(
        [
            key_rows.reshape(rows, local_heads, HD).transpose(1, 0, 2),
            value_rows.reshape(rows, local_heads, HD).transpose(1, 0, 2),
        ],
        axis=2,
    )
    key_value = jnp.broadcast_to(
        key_value[:, None], (local_heads, share, rows, 2 * HD)
    ).reshape(n_ep, rows, 2 * HD)
    half = part // 2
    query_parts = queries.reshape(share, 2, half, local_heads, HD).transpose(3, 0, 2, 1, 4)
    query_parts = query_parts.reshape(n_ep, half, 2 * HD)
    message = jnp.concatenate([key_value, query_parts], axis=1)
    gates = jnp.broadcast_to(block_cum.T[:, None, None, :], (local_heads, share, 1, rows))
    gates = gates.reshape(n_ep, 1, rows)

    hidden, all_messages, all_gates = outward(
        slots, message, gates, gate_weight[0], up_weight[0], n_ep, n_tp
    )

    positions = n_ep * rows
    all_gates = all_gates.reshape(n_ep, rows)
    totals = all_gates[:, rows - 1]
    lower = jnp.arange(n_ep)[None, :] < jnp.arange(n_ep)[:, None]
    base = jnp.sum(jnp.where(lower, totals[None, :], 0.0), axis=1)
    cumulative = all_gates + base[:, None]
    keys = all_messages[:, :rows, :HD].reshape(positions, HD)
    values = all_messages[:, :rows, HD:].reshape(positions, HD)
    head_query = all_messages[:, rows:].reshape(n_ep, half, 2, HD).transpose(0, 2, 1, 3)
    head_query = head_query.reshape(n_ep * part, HD)
    first = (lax.axis_index("ep") % share) * part
    query_cum = lax.dynamic_slice_in_dim(cumulative, first, part, 1).reshape(-1)
    query_pos = (
        jnp.arange(n_ep, dtype=jnp.int32)[:, None] * rows
        + first
        + jnp.arange(part, dtype=jnp.int32)[None, :]
    ).reshape(-1)
    key_pos = jnp.arange(positions, dtype=jnp.int32)
    scores = by_rows(head_query, keys) * HD ** (-0.5)
    scores = scores + query_cum[:, None] - cumulative.reshape(-1)[None, :]
    scores = jnp.where(key_pos[None, :] <= query_pos[:, None], scores, -jnp.inf)
    weights = jnp.exp(scores - jnp.max(scores, axis=-1, keepdims=True)).astype(bf16)
    attended = jnp.dot(weights, values, preferred_element_type=f32)
    rescale = lax.rsqrt(jnp.mean(attended * attended, axis=-1, keepdims=True) + HEAD_FLOOR)
    head_out = (attended * rescale).astype(bf16).reshape(n_ep, part, HD)

    returned, heads_all = homeward(hidden, down_weight[0], head_out, n_ep, n_tp)

    heads_all = heads_all.reshape(n_tp, local_heads, share, part, HD).transpose(2, 3, 0, 1, 4)
    heads_all = heads_all.reshape(rows, n_tp * local_heads * HD)
    mixer_output = jnp.dot(heads_all, output_weight, preferred_element_type=f32).astype(bf16)
    returned = returned.reshape(n_ep * capacity, width)
    expert_output = 0.0
    for j in range(top_count):
        picked = jnp.dot(picks[j], returned, preferred_element_type=f32)
        expert_output = expert_output + picked * route_weights[:, j][:, None]
    return (mixer_output, expert_output.astype(bf16))


def lanes_of(shape, dim):
    return lax.broadcasted_iota(jnp.int32, shape, dim)


class Relay:
    def __init__(self, place, land, sems, batch):
        self.p, self.land, self.batch = place, land, batch
        self.ys, self.yr, self.ps, self.pr = sems

    def y_copy(self, off, s, t, to):
        block = self.land(t, s)
        return remote(block, block, self.ys.at[0], self.yr.at[off - 1, s], self.p.e, to)

    def p_copy(self, off, s, t):
        block, p = self.land(t, s), self.p
        return remote(block, block, self.ps.at[0], self.pr.at[self.batch(s)], p.e, p.partner)

    def first(self, s):
        p = self.p
        for off in range(1, p.ny):
            self.y_copy(off, s, p.t, p.chip(off)).start()
        self.p_copy(0, s, p.t).start()

    def relay(self, s):
        p = self.p
        for off in range(1, p.ny):
            self.y_copy(off, s, p.chip(-off), p.chip(-off)).wait_recv()
            self.p_copy(off, s, p.chip(-off)).start()

    def settle(self, batch, blocks):
        p = self.p
        remote(blocks, blocks, self.ps.at[0], self.pr.at[batch], p.e, p.partner).wait_recv()

    def sent(self, y_blocks, p_blocks):
        p = self.p
        remote(y_blocks, y_blocks, self.ys.at[0], self.yr.at[0, 0], p.e, p.partner).wait_send()
        remote(p_blocks, p_blocks, self.ps.at[0], self.pr.at[0], p.e, p.partner).wait_send()


def flipped(place, bits):
    at, weight = place, 1
    while bits:
        if bits % 2:
            at = at + weight * (1 - 2 * (place // weight % 2))
        bits, weight = bits // 2, weight * 2
    return at


def fused_kernel(
    n_ep, n_tp,
    tokens_a, gain_a, w_q, w_k, w_v, w_f, b_f, w_o, tokens_b, gain_b, routes, route_w,
    w_gate, w_up, w_down,
    out_a, out_b,
    a_held, ga_held, q_held, kv_held, f_held, bf_held, o_held, b_held, gb_held, r_held, rw_held,
    gate_held, up_held, down_held,
    slots, land, w_hi, w_lo, kv_send, q_send, g_send, kv_land, q_land, g_land,
    hidden, pair_send, pair_land, own_part, mine, y_send, y_land, final, ret,
    q_all, q_cum, scores, running, row_max, attended, head_send, heads_all, lhs,
    lsem, s0, s1, ys, yr, ps, pr, k0, k1, x0, x1, q0, q1, g0, g1,
    p0, p1, z0, z1, a0, a1, h0, h1, hy0, hy1, hp0, hp1,
):
    p = Place(n_ep, n_tp)
    ny = p.ny
    bf16, f32 = jnp.bfloat16, jnp.float32
    rows, features = a_held.shape
    tokens = b_held.shape[0]
    _, capacity, width = slots.shape
    local_heads = kv_send.shape[0]
    share = n_ep // local_heads
    part = rows // share
    half = part // 2
    units = gate_held.shape[0]
    quarter = n_ep // 4
    near, second, third = range(2 * quarter), range(2 * quarter, 3 * quarter), range(3 * quarter, n_ep)
    groups = [near[:quarter], range(quarter, 3 * quarter), third]
    own_share = p.e % share
    first = own_share * part

    def cols(t):
        return pl.ds(pl.multiple_of(t * width, width), width)

    def peer(j):
        return flipped(p.e, j + quarter if j in second else j - quarter if j in third else j)

    barrier = pltpu.get_barrier_semaphore()
    for k in range(1, n_ep):
        pl.semaphore_signal(
            barrier, inc=1, device_id={"ep": p.ep(k), "tp": p.t}, device_id_type=MESH
        )
    for off in range(1, ny):
        pl.semaphore_signal(
            barrier, inc=1, device_id={"ep": p.e, "tp": p.chip(off)}, device_id_type=MESH
        )
    pl.semaphore_signal(
        barrier, inc=1, device_id={"ep": p.e, "tp": p.partner}, device_id_type=MESH
    )

    early = [(tokens_b, b_held), (routes, r_held), (gain_b, gb_held)]
    middle = [(tokens_a, a_held), (gain_a, ga_held), (w_f, f_held), (b_f, bf_held), (w_q, q_held)]
    late = [
        (w_gate, gate_held), (w_up, up_held), (w_down, down_held), (route_w, rw_held),
        (w_o, o_held),
    ]
    loads, number = [], 0
    for batch in (early, middle, late):
        made = []
        for src, dst in batch:
            made.append(pltpu.make_async_copy(src, dst, lsem.at[number]))
            number += 1
        loads.append(made)
    pieces = []
    for h in range(local_heads):
        mine_rows = pl.ds(h * HD, HD)
        for at, src in ((2 * h, w_k), (2 * h + 1, w_v)):
            there = kv_held.at[pl.ds(at * HD, HD)]
            pieces.append(pltpu.make_async_copy(src.at[mine_rows], there, lsem.at[number]))
    all_pieces = pltpu.make_async_copy(kv_held, kv_held, lsem.at[number])
    early, middle, late = loads
    for load in early + middle + pieces:
        load.start()

    for load in early:
        load.wait()
    values = b_held[...].astype(f32)
    square = jnp.mean(values * values, axis=-1, keepdims=True)
    scale = lax.rsqrt(jnp.maximum(square, MEAN_FLOOR))
    own_columns = (b_held[:, cols(p.t)].astype(f32) * scale * gb_held[:, cols(p.t)]).astype(bf16)
    named_by = r_held[...]
    top_count = named_by.shape[0]
    place = lanes_of((n_ep, tokens), 0)
    place = place + jnp.where(place < 2 * quarter, 0, jnp.where(place < 3 * quarter, 1, -1)) * quarter
    expert_at, weight = place, 1
    while weight < n_ep:
        flip = (p.e // weight) % 2
        expert_at = expert_at + flip * weight * (1 - 2 * ((place // weight) % 2))
        weight *= 2
    chosen = [named_by[c : c + 1, :] == expert_at for c in range(top_count)]
    named = sum([c.astype(f32) for c in chosen[1:]], chosen[0].astype(f32))
    earlier = (lanes_of((tokens, tokens), 0) < lanes_of((tokens, tokens), 1)).astype(bf16)
    ranks = jnp.dot(named.astype(bf16), earlier, preferred_element_type=f32)
    ranks = jnp.where(named > 0, ranks, -1.0).astype(jnp.int32)
    slot_at = lanes_of((capacity, tokens), 0)
    picks = [ranks[j : j + 1, :] == slot_at for j in range(n_ep)]
    for j in range(n_ep):
        block = jnp.dot(
            picks[j].astype(f32).astype(bf16), own_columns, preferred_element_type=f32
        ).astype(bf16)
        if j == 0:
            land[0, :, cols(p.t)] = block
        else:
            slots[j] = block
    pl.semaphore_wait(barrier, n_ep - 1 + ny - 1 + 1)

    def slot_copy(j):
        return remote(
            slots.at[j], land.at[j, :, cols(p.t)], s0.at[0], s1.at[j], peer(j), p.t
        )

    spread = Relay(
        p,
        lambda t, j: land.at[j, :, cols(t)],
        (ys, yr, ps, pr),
        lambda j: [j in group for group in groups].index(True),
    )
    for j in [*near[1:], *second, *third]:
        slot_copy(j).start()
    spread.first(0)

    for load in middle + [all_pieces]:
        load.wait()
    for load in late:
        load.start()
    values = a_held[...].astype(f32)
    square = jnp.mean(values * values, axis=-1, keepdims=True)
    scale = lax.rsqrt(jnp.maximum(square, MEAN_FLOOR))
    a_held[...] = (values * scale * ga_held[...]).astype(bf16)
    normed = a_held[...]
    eye = lanes_of((local_heads, local_heads), 0) == lanes_of((local_heads, local_heads), 1)
    bias = jnp.sum(jnp.where(eye, bf_held[...], 0.0), axis=1, keepdims=True)
    gate = by_rows(f_held[...], normed) + bias
    log_gate = jnp.minimum(gate, 0.0) - jnp.log1p(jnp.exp(-jnp.abs(gate)))
    upto = (lanes_of((rows, rows), 0) <= lanes_of((rows, rows), 1)).astype(f32)
    block_cum = jnp.dot(
        log_gate, upto, precision=lax.Precision.HIGHEST, preferred_element_type=f32
    )
    for h in range(local_heads):
        g_send[h] = block_cum[h : h + 1, :]

    def kv_copy(h):
        to = h * share + own_share
        return remote(kv_send.at[h], kv_land.at[p.e], k0.at[0], k1.at[p.e // share], to, p.t)

    def kv_arrival(n):
        s = (p.e // share + n) % local_heads * share + own_share
        return remote(kv_send.at[0], kv_land.at[s], k0.at[0], k1.at[s // share], p.e, p.t), s

    def sibling(off):
        return p.e // share * share + (own_share + off) % share

    def kv_relay(s, off):
        return remote(
            kv_land.at[s], kv_land.at[s], x0.at[0], x1.at[0], sibling(off), p.t
        )

    def q_copy(k):
        d = p.ep(k)
        return remote(q_send.at[d], q_land.at[p.e], q0.at[0], q1.at[0], d, p.t)

    def g_copy(k):
        d = p.ep(k)
        return remote(g_send.at[d // share], g_land.at[p.e], g0.at[0], g1.at[0], d, p.t)

    def others(ref):
        return ref.at[pl.ds(0, n_ep - 1)]

    def batch_of(ref, send, recv):
        return remote(ref, ref, send.at[0], recv.at[0], p.e, p.partner)

    key_value = by_rows(normed, kv_held[...]).astype(bf16)
    for h in range(local_heads):
        kv_send[h] = key_value[:, 2 * h * HD : 2 * (h + 1) * HD]
    for n in range(1, local_heads):
        kv_copy((p.e // share + n) % local_heads).start()
    own_head = p.e // share
    kv_land[p.e] = kv_send[own_head]
    for off in range(1, share):
        kv_relay(p.e, off).start()
    slot_copy(1).wait_recv()
    spread.first(1)
    queries = by_rows(normed, q_held[...]) * HD ** (-0.5)
    left = lanes_of((half, 2 * HD), 1) < HD
    for pair in range(local_heads // 2):
        there = queries[:, 2 * pair * HD : 2 * (pair + 1) * HD]
        moved = pltpu.roll(there, HD, 1)
        for x in range(share):
            top, bottom = slice(x * part, x * part + half), slice(x * part + half, (x + 1) * part)
            q_send[2 * pair * share + x] = jnp.where(left, there[top], moved[bottom]).astype(bf16)
            q_send[(2 * pair + 1) * share + x] = jnp.where(
                left, moved[top], there[bottom]
            ).astype(bf16)
    for k in range(1, n_ep):
        q_copy(k).start()
        g_copy(k).start()
    q_land[p.e] = q_send[p.e]
    g_land[p.e] = g_send[own_head]

    def arrive(j):
        slot_copy(j).wait_recv()
        spread.first(j)

    def complete(j):
        spread.relay(j)

    def settle(g):
        low_row, count = groups[g][0], len(groups[g])
        spread.settle(g, land.at[pl.ds(low_row, count), :, pl.ds(0, ny * width)])

    cuts = [(at, min(at + 512, units)) for at in range(0, units, 512)]

    def serve(beside, number, count):
        for act, *given in beside[len(beside) * number // count : len(beside) * (number + 1) // count]:
            act(*given)

    def open_up(g, beside):
        low_row, count = groups[g][0], len(groups[g])
        block = land[low_row : low_row + count].reshape(count * capacity, features)
        lines = slice(low_row * capacity, (low_row + count) * capacity)
        for number, (low, high) in enumerate(cuts):
            gated = by_rows(gate_held[low:high], block)
            upped = by_rows(up_held[low:high], block)
            hidden[lines, low:high] = (gated * lax.logistic(gated) * upped).astype(bf16).T
            serve(beside, number, len(cuts))

    def pair_copy(g, off):
        low_row, count = groups[g][0], len(groups[g])
        lines = pl.ds(low_row * capacity, count * capacity)
        return remote(
            pair_send.at[off, lines], pair_land.at[off, lines], p0.at[0], p1.at[g, off],
            p.e, p.partner,
        )

    def y_copy(j, off, to):
        return remote(
            y_send.at[j, off - 1], y_land.at[j, off - 1],
            z0.at[0], z1.at[j, off - 1], p.e, p.chip(to),
        )

    turns = [*range(1, ny), 0]

    def close_down(g, beside, held=()):
        low_row, count = groups[g][0], len(groups[g])
        lines = slice(low_row * capacity, (low_row + count) * capacity)

        def product(t):
            return jnp.dot(hidden[lines], down_held[:, cols(t)], preferred_element_type=f32)

        for number, off in enumerate(turns):
            pair_send[off, lines] = product(p.y_at(off) * 2 + (1 - p.c)).astype(bf16)
            pair_copy(g, off).start()
            serve(beside, number, 2 * ny)
        for number, off in enumerate(turns):
            own_part[lines] = product(p.chip(off))
            serve(beside, ny + number, 2 * ny)
            pair_copy(g, off).wait_recv()
            both = own_part[lines] + pair_land[off, lines].astype(f32)
            both = both.reshape(count, capacity, width)
            for m in range(count):
                j = low_row + m
                if off == 0:
                    mine[j] = both[m]
                else:
                    y_send[j, off - 1] = both[m].astype(bf16)
                    if j not in held:
                        y_copy(j, off, off).start()

    def final_copy(j):
        return remote(final.at[j], ret.at[j], a0.at[0], a1.at[0], peer(j), p.t)

    def finish(j):
        total = mine[j]
        for off in range(1, ny):
            y_copy(j, off, -off).wait_recv()
            total = total + y_land[j, off - 1].astype(f32)
        if j == 0:
            ret[0] = total.astype(bf16)
        else:
            final[j] = total.astype(bf16)
            final_copy(j).start()

    def kv_forward(n):
        copy, s = kv_arrival(n)
        copy.wait_recv()
        for off in range(1, share):
            kv_relay(s, off).start()

    some = len(third) // 2
    for j in near[2 : quarter + 1]:
        arrive(j)
    complete(0)
    for j in near[quarter + 1 :]:
        arrive(j)
    for j in near[1:-1]:
        complete(j)
    for j in second:
        arrive(j)
    settle(0)
    late[0].wait()
    late[1].wait()
    open_up(0, [])
    complete(near[-1])
    for j in second:
        complete(j)
    settle(1)
    open_up(1, [(arrive, j) for j in third])
    late[2].wait()
    close_down(1, [], near)
    for j in near[quarter:]:
        for off in range(1, ny):
            y_copy(j, off, off).start()
    close_down(0, [(complete, j) for j in third], near)
    for n in range(1, local_heads):
        kv_forward(n)
    settle(2)
    open_up(2, [(finish, j) for j in second])
    close_down(2, [])
    behind = near[:quarter]
    for j in behind:
        for off in range(1, ny):
            y_copy(j, off, off).start()

    late[3].wait()
    for j in range(n_ep):
        weight = 0.0
        for c in range(top_count):
            weight = weight + jnp.where(
                named_by[c : c + 1, :] == peer(j), rw_held[c : c + 1, :], 0.0
            )
        weight = jnp.where(ranks[j : j + 1, :] == slot_at, weight, 0.0)
        high = weight.astype(bf16)
        w_hi[j * capacity : (j + 1) * capacity] = high
        w_lo[j * capacity : (j + 1) * capacity] = (weight - high.astype(f32)).astype(bf16)

    batch_of(others(g_land), g0, g1).wait_recv()
    batch_of(others(q_land), q0, q1).wait_recv()
    relayed = kv_land.at[pl.ds(0, local_heads * (share - 1))]
    batch_of(relayed, x0, x1).wait_recv()
    positions = lanes_of((part, rows), 1)
    asked = first + lanes_of((part, rows), 0)
    base = jnp.zeros((1, 1), f32)
    key_cum = []
    last = lanes_of((1, rows), 1) == rows - 1
    for b in range(n_ep):
        block = g_land[b]
        key_cum.append(block + base)
        base = base + jnp.sum(jnp.where(last, block, 0.0), axis=1, keepdims=True)
        at = b * part
        q_cum[at : at + part] = jnp.sum(
            jnp.where(positions == asked, key_cum[b], 0.0), axis=1, keepdims=True
        )
        packed = q_land[b].astype(f32)
        q_all[at : at + half] = jnp.where(left, packed, 0.0).astype(bf16)
        q_all[at + half : at + part] = jnp.where(
            left, pltpu.roll(packed, HD, 1), 0.0
        ).astype(bf16)
    for b in range(n_ep):
        at = b * part
        block = by_rows(q_all[at:], kv_land[b]) + q_cum[at:] - key_cum[b]
        seen = jnp.where(positions <= asked, block[:part], -jnp.inf)
        scores[b, at : at + part] = seen
        if b == 0:
            running[:part] = seen
            running[part:] = block[part:]
        else:
            running[at : at + part] = jnp.maximum(running[at : at + part], seen)
        if b + 1 < n_ep:
            scores[b, at + part :] = block[part:]
            if b > 0:
                running[at + part :] = jnp.maximum(running[at + part :], block[part:])
    row_max[...] = jnp.max(running[...], axis=1, keepdims=True)
    for b in range(n_ep):
        at = b * part
        weights = jnp.exp(scores[b, at:] - row_max[at:]).astype(bf16)
        product = jnp.dot(weights, kv_land[b], preferred_element_type=f32)
        if b == 0:
            attended[...] = product
        else:
            attended[at:] = attended[at:] + product
    right = lanes_of((part, 2 * HD), 1) >= HD
    for b in range(n_ep):
        block = jnp.where(right, attended[b * part : (b + 1) * part], 0.0)
        block = block * lax.rsqrt(
            jnp.sum(block * block, axis=1, keepdims=True) * (1.0 / HD) + HEAD_FLOOR
        )
        moved = pltpu.roll(block, HD, 1)
        head_send[b] = jnp.where(left, moved[:half], block[half:]).astype(bf16)

    def head_copy(k):
        d = peer(k)
        return remote(head_send.at[d], heads_all.at[p.t, p.e], h0.at[0], h1.at[p.e], d, p.t)

    def head_arrival(k):
        s = peer(k)
        return remote(head_send.at[s], heads_all.at[p.t, s], h0.at[0], h1.at[s], s, p.t)

    for k in range(1, n_ep):
        head_copy(k).start()
    heads_all[p.t, p.e] = head_send[p.e]

    for j in near[quarter:]:
        finish(j)
    for j in third:
        finish(j)

    gather = Relay(p, lambda t, s: heads_all.at[t, s], (hy0, hy1, hp0, hp1), lambda s: 0)
    gather.first(p.e)
    for k in near[1:]:
        head_arrival(k).wait_recv()
        gather.first(peer(k))
    for j in behind:
        finish(j)
    for k in [*second, *third]:
        head_arrival(k).wait_recv()
        gather.first(peer(k))
    for k in range(n_ep):
        gather.relay(peer(k))
    gather.settle(0, heads_all.at[pl.ds(0, ny)])
    for t in range(n_tp):
        for pair in range(local_heads // 2):
            lanes = slice((t * local_heads + 2 * pair) * HD, (t * local_heads + 2 * pair + 2) * HD)
            for x in range(share):
                one = heads_all[t, 2 * pair * share + x].astype(f32)
                two = heads_all[t, (2 * pair + 1) * share + x].astype(f32)
                at = x * part
                lhs[at : at + half, lanes] = jnp.where(
                    left, one, pltpu.roll(two, HD, 1)
                ).astype(bf16)
                lhs[at + half : at + part, lanes] = jnp.where(
                    left, pltpu.roll(one, HD, 1), two
                ).astype(bf16)
    late[4].wait()
    out_a[...] = jnp.dot(lhs[...], o_held[...], preferred_element_type=f32).astype(bf16)

    batch_of(others(ret), a0, a1).wait_recv()
    returned = ret[...].reshape(n_ep * capacity, width)
    over_slots = (((0,), (0,)), ((), ()))
    total = lax.dot_general(w_hi[...], returned, over_slots, preferred_element_type=f32)
    total = total + lax.dot_general(w_lo[...], returned, over_slots, preferred_element_type=f32)
    out_b[...] = total.astype(bf16)

    spread.sent(
        land.at[:, :, pl.ds(0, (ny - 1) * width)], land.at[:, :, pl.ds(0, ny * width)]
    )
    gather.sent(heads_all.at[pl.ds(0, ny - 1)], heads_all.at[pl.ds(0, ny)])
    for ref, send, recv in (
        (others(slots), s0, s1), (others(q_send), q0, q1), (others(final), a0, a1),
        (others(head_send), h0, h1), (pair_send, p0, a1), (y_send, z0, a1),
        (others(g_land), g0, g1), (kv_send.at[pl.ds(0, local_heads - 1)], k0, k1),
        (relayed, x0, x1),
    ):
        batch_of(ref, send, recv).wait_send()


def fused_on_device(
    mixer_tokens, mixer_gain, query_weight, key_weight, value_weight, forget_weight,
    forget_bias, output_weight, expert_tokens, expert_gain, routes, route_weights,
    gate_weight, up_weight, down_weight,
):
    n_ep, n_tp = lax.axis_size("ep"), lax.axis_size("tp")
    ny = n_tp // 2
    far = max(ny - 1, 1)
    rows, features = mixer_tokens.shape
    tokens, top_count = routes.shape
    local_heads = forget_weight.shape[1]
    share = n_ep // local_heads
    part = rows // share
    half = part // 2
    width = features // n_tp
    capacity = 2 * top_count * tokens // n_ep
    units = gate_weight.shape[1]
    groups = 3
    asked = n_ep * part
    bf16, f32 = jnp.bfloat16, jnp.float32
    operands = [
        mixer_tokens, mixer_gain.reshape(1, features), query_weight, key_weight, value_weight,
        forget_weight.T, forget_bias, output_weight, expert_tokens,
        expert_gain.reshape(1, features), routes.T, route_weights.T,
        gate_weight[0], up_weight[0], down_weight[0],
    ]
    operands = [pltpu.with_memory_space_constraint(x, pltpu.HBM) for x in operands]
    vmem = pltpu.VMEM
    scratch = [
        vmem((rows, features), bf16), vmem((1, features), f32),
        vmem(query_weight.shape, bf16), vmem((2 * local_heads * HD, features), bf16),
        vmem((local_heads, features), bf16), vmem((1, local_heads), f32),
        vmem(output_weight.shape, bf16), vmem((tokens, features), bf16),
        vmem((1, features), f32), vmem((top_count, tokens), jnp.int32),
        vmem((top_count, tokens), f32),
        vmem((units, features), bf16), vmem((units, features), bf16),
        vmem((units, features), bf16),
        vmem((n_ep, capacity, width), bf16), vmem((n_ep, capacity, features), bf16),
        vmem((n_ep * capacity, tokens), bf16), vmem((n_ep * capacity, tokens), bf16),
        vmem((local_heads, rows, 2 * HD), bf16), vmem((n_ep, half, 2 * HD), bf16),
        vmem((local_heads, 1, rows), f32),
        vmem((n_ep, rows, 2 * HD), bf16), vmem((n_ep, half, 2 * HD), bf16),
        vmem((n_ep, 1, rows), f32),
        vmem((n_ep * capacity, units), bf16),
        vmem((ny, n_ep * capacity, width), bf16),
        vmem((ny, n_ep * capacity, width), bf16),
        vmem((n_ep * capacity, width), f32),
        vmem((n_ep, capacity, width), f32),
        vmem((n_ep, far, capacity, width), bf16), vmem((n_ep, far, capacity, width), bf16),
        vmem((n_ep, capacity, width), bf16), vmem((n_ep, capacity, width), bf16),
        vmem((asked, 2 * HD), bf16), vmem((asked, 1), f32),
        vmem((n_ep, asked, rows), f32), vmem((asked, rows), f32), vmem((asked, 1), f32),
        vmem((asked, 2 * HD), f32), vmem((n_ep, half, 2 * HD), bf16),
        vmem((n_tp, n_ep, half, 2 * HD), bf16), vmem((rows, n_tp * local_heads * HD), bf16),
    ]
    one = DMA((1,))
    sems = [DMA((14,)), one, DMA((n_ep,)), one, DMA((far, n_ep)), one, DMA((groups,))]
    sems += [one, DMA((local_heads,))] + [one] * 6
    sems += [one, DMA((groups, ny)), one, DMA((n_ep, far)), one, one, one, DMA((n_ep,))]
    sems += [one, DMA((far, n_ep)), one, one]
    return pl.pallas_call(
        functools.partial(fused_kernel, n_ep, n_tp),
        out_shape=[
            jax.ShapeDtypeStruct((rows, width), bf16),
            jax.ShapeDtypeStruct((tokens, width), bf16),
        ],
        in_specs=[ANY] * len(operands),
        out_specs=[VM] * 2,
        scratch_shapes=scratch + sems,
        compiler_params=pltpu.CompilerParams(
            collective_id=2, has_side_effects=True, vmem_limit_bytes=LIMIT
        ),
        name="fused",
    )(*operands)


def deliver_kernel(one, two, one_out, two_out, sem):
    copies = [
        pltpu.make_async_copy(one, one_out, sem.at[0]),
        pltpu.make_async_copy(two, two_out, sem.at[1]),
    ]
    for copy in copies:
        copy.start()
    for copy in copies:
        copy.wait()


def deliver(one, two):
    return pl.pallas_call(
        deliver_kernel,
        out_shape=[
            jax.ShapeDtypeStruct(one.shape, one.dtype),
            jax.ShapeDtypeStruct(two.shape, two.dtype),
        ],
        in_specs=[ANY] * 2,
        out_specs=[ANY] * 2,
        scratch_shapes=[DMA((2,))],
        compiler_params=pltpu.CompilerParams(vmem_limit_bytes=1 << 20),
        name="deliver",
    )(one, two)


def choose(*arguments):
    n_ep = lax.axis_size("ep")
    rows, local_heads = arguments[0].shape[0], arguments[5].shape[1]
    share = n_ep // local_heads
    packed = local_heads % 2 == 0 and n_ep % local_heads == 0
    packed = packed and n_ep >= 8 and n_ep & (n_ep - 1) == 0 and lax.axis_size("tp") >= 4
    if packed and rows % (32 * share) == 0:
        return tuple(deliver(*fused_on_device(*arguments)))
    return on_device(*arguments)


def solution(mesh):
    in_specs = (
        P("ep", None),
        P(),
        P("tp", None),
        P("tp", None),
        P("tp", None),
        P(None, "tp"),
        P("ep", "tp"),
        P(None, "tp"),
        P("ep", None),
        P(),
        P("ep", None),
        P("ep", None),
        P("ep", "tp", None),
        P("ep", "tp", None),
        P("ep", "tp", None),
    )
    out_specs = (P("ep", "tp"), P("ep", "tp"))
    return jax.shard_map(
        choose, mesh=mesh, in_specs=in_specs, out_specs=out_specs, check_vma=False
    )
```

```python
import functools

import jax
import jax.numpy as jnp
from jax import lax
from jax.experimental import pallas as pl
from jax.experimental.pallas import tpu as pltpu
from jax.sharding import PartitionSpec as P

HD = 64
MEAN_FLOOR = 0.1
HEAD_FLOOR = 1.0
MESH = pl.DeviceIdType.MESH
VM = pl.BlockSpec(memory_space=pltpu.VMEM)
ANY = pl.BlockSpec(memory_space=pl.ANY)
DMA = pltpu.SemaphoreType.DMA
LIMIT = 48 << 20


def normed_rows(inputs, gain):
    values = inputs.astype(jnp.float32)
    square = jnp.mean(values * values, axis=-1, keepdims=True)
    return (values * lax.rsqrt(jnp.maximum(square, MEAN_FLOOR)) * gain).astype(jnp.bfloat16)


def by_rows(left, weight):
    return lax.dot_general(
        left, weight, (((1,), (1,)), ((), ())), preferred_element_type=jnp.float32
    )


class Place:
    def __init__(self, n_ep, n_tp):
        self.n_ep, self.n_tp, self.ny = n_ep, n_tp, n_tp // 2
        self.e = lax.axis_index("ep")
        self.t = lax.axis_index("tp")
        self.y, self.c = self.t // 2, self.t % 2
        self.partner = self.y * 2 + (1 - self.c)

    def ep(self, k):
        return (self.e + k) % self.n_ep

    def y_at(self, off):
        return (self.y + self.ny + off) % self.ny

    def chip(self, off):
        return self.y_at(off) * 2 + self.c

    def barrier(self):
        sem = pltpu.get_barrier_semaphore()
        for k in range(1, self.n_ep):
            pl.semaphore_signal(
                sem, inc=1, device_id={"ep": self.ep(k), "tp": self.t}, device_id_type=MESH
            )
        for off in range(1, self.ny):
            pl.semaphore_signal(
                sem, inc=1, device_id={"ep": self.e, "tp": self.chip(off)}, device_id_type=MESH
            )
        pl.semaphore_signal(
            sem, inc=1, device_id={"ep": self.e, "tp": self.partner}, device_id_type=MESH
        )
        pl.semaphore_wait(sem, self.n_ep - 1 + self.ny - 1 + 1)


def remote(src, dst, send, recv, e, t):
    return pltpu.make_async_remote_copy(
        src_ref=src,
        dst_ref=dst,
        send_sem=send,
        recv_sem=recv,
        device_id={"ep": e, "tp": t},
        device_id_type=MESH,
    )


class Exchange:
    def __init__(self, place, send, land, sems):
        self.p, self.send, self.land = place, send, land
        self.ssem, self.rsem = sems

    def copy(self, k):
        p = self.p
        d = p.ep(k)
        return remote(
            self.send(d), self.land(p.e), self.ssem.at[d], self.rsem.at[p.e], d, p.t
        )

    def arrival(self, k):
        p = self.p
        s = p.ep(k)
        return remote(self.send(s), self.land(s), self.ssem.at[s], self.rsem.at[s], s, p.t)

    def own(self):
        p = self.p
        return pltpu.make_async_copy(self.send(p.e), self.land(p.e), self.rsem.at[p.e])

    def start(self):
        for k in range(1, self.p.n_ep):
            self.copy(k).start()
        self.own().start()

    def wait_arrival(self, k):
        if k == 0:
            self.own().wait()
        else:
            self.arrival(k).wait_recv()

    def wait_sent(self):
        for k in range(1, self.p.n_ep):
            self.copy(k).wait_send()


class Spread:
    def __init__(self, place, land, sems):
        self.p, self.land = place, land
        self.ys, self.yr, self.ps, self.pr = sems

    def y_copy(self, off, s):
        p = self.p
        block = self.land(p.t, s)
        return remote(
            block, block, self.ys.at[off - 1, s], self.yr.at[off - 1, s], p.e, p.chip(off)
        )

    def y_arrival(self, off, s):
        p = self.p
        block = self.land(p.chip(-off), s)
        return remote(
            block, block, self.ys.at[off - 1, s], self.yr.at[off - 1, s], p.e, p.chip(-off)
        )

    def p_copy(self, off, s):
        p = self.p
        block = self.land(p.chip(-off), s)
        return remote(block, block, self.ps.at[off, s], self.pr.at[off, s], p.e, p.partner)

    def p_arrival(self, off, s):
        p = self.p
        block = self.land(p.y_at(-off) * 2 + (1 - p.c), s)
        return remote(block, block, self.ps.at[off, s], self.pr.at[off, s], p.e, p.partner)

    def first(self, s):
        for off in range(1, self.p.ny):
            self.y_copy(off, s).start()
        self.p_copy(0, s).start()

    def relay(self, s):
        for off in range(1, self.p.ny):
            self.y_arrival(off, s).wait_recv()
            self.p_copy(off, s).start()

    def finish(self, s):
        for off in range(self.p.ny):
            self.p_arrival(off, s).wait_recv()
        self.wait_sent(s)

    def wait_sent(self, s):
        for off in range(self.p.ny):
            self.p_copy(off, s).wait_send()
        for off in range(1, self.p.ny):
            self.y_copy(off, s).wait_send()


def spread_sems(n_ep, n_tp):
    ny = n_tp // 2
    far = max(ny - 1, 1)
    return [DMA((far, n_ep)), DMA((far, n_ep)), DMA((ny, n_ep)), DMA((ny, n_ep))]


def outward_kernel(
    n_ep, n_tp, slots, message, gates, gate_weight, up_weight,
    hidden, message_out, gates_out,
    out, gate_held, up_held, gate_act, up_act,
    s0, s1, m0, m1, g0, g1, w, ys, yr, ps, pr,
):
    p = Place(n_ep, n_tp)
    width = slots.shape[2]

    def cols(t):
        return pl.ds(pl.multiple_of(t * width, width), width)

    def land(t, s):
        return out.at[s, :, cols(t)]

    def multiply(t, opening):
        rows = out[:, :, cols(t)].reshape(hidden.shape[0], width)
        for held, total in ((gate_held, gate_act), (up_held, up_act)):
            product = by_rows(rows, held[:, cols(t)])
            total[...] = product if opening else total[...] + product

    loads = [
        pltpu.make_async_copy(gate_weight, gate_held, w.at[0]),
        pltpu.make_async_copy(up_weight, up_held, w.at[1]),
    ]
    for load in loads:
        load.start()
    p.barrier()
    slot_move = Exchange(p, lambda d: slots.at[d], lambda s: land(p.t, s), (s0, s1))
    gate_move = Exchange(p, lambda d: gates.at[d], lambda s: gates_out.at[s], (g0, g1))
    message_move = Exchange(p, lambda d: message.at[d], lambda s: message_out.at[s], (m0, m1))
    spread = Spread(p, land, (ys, yr, ps, pr))
    slot_move.start()
    gate_move.start()
    message_move.start()
    for k in range(n_ep):
        slot_move.wait_arrival(k)
        spread.first(p.ep(k))
    for load in loads:
        load.wait()
    multiply(p.t, True)
    for k in range(n_ep):
        spread.p_arrival(0, p.ep(k)).wait_recv()
    multiply(p.partner, False)
    for k in range(n_ep):
        spread.relay(p.ep(k))
    for off in range(1, p.ny):
        multiply(p.chip(-off), False)
        for k in range(n_ep):
            spread.p_arrival(off, p.ep(k)).wait_recv()
        multiply(p.y_at(-off) * 2 + (1 - p.c), False)
    gate = gate_act[...]
    hidden[...] = (gate * lax.logistic(gate) * up_act[...]).astype(hidden.dtype)
    for k in range(n_ep):
        gate_move.wait_arrival(k)
        message_move.wait_arrival(k)
        spread.wait_sent(p.ep(k))
    slot_move.wait_sent()
    gate_move.wait_sent()
    message_move.wait_sent()


def homeward_kernel(
    n_ep, n_tp, hidden, down_weight, heads, ret, heads_all,
    partial, down_held, pair, mine, out_y, in_y, final,
    w, h0, h1, a0, a1, r0, r1, q0, q1, ys, yr, ps, pr,
):
    p = Place(n_ep, n_tp)
    ny = p.ny
    width = ret.shape[2]

    def cols(t):
        return pl.ds(pl.multiple_of(t * width, width), width)

    def land(t, s):
        return heads_all.at[t, s]

    load = pltpu.make_async_copy(down_weight, down_held, w.at[0])
    load.start()
    p.barrier()
    head_move = Exchange(p, lambda d: heads.at[d], lambda s: land(p.t, s), (h0, h1))
    spread = Spread(p, land, (ys, yr, ps, pr))
    head_move.start()

    def pair_copy(s, off):
        src = partial.at[s, :, cols(p.y_at(off) * 2 + (1 - p.c))]
        return remote(src, pair.at[s, off], r0.at[s, off], r1.at[s, off], p.e, p.partner)

    def y_copy(s, off, to):
        return remote(
            out_y.at[s, off - 1], in_y.at[s, off - 1],
            q0.at[s, off - 1], q1.at[s, off - 1], p.e, p.chip(to),
        )

    def final_copy(k):
        d = p.ep(k)
        return remote(final.at[d], ret.at[p.e], a0.at[d], a1.at[p.e], d, p.t)

    order = list(range(1, n_ep)) + [0]
    capacity = ret.shape[1]

    def multiply(t):
        product = jnp.dot(
            hidden[...], down_held[:, cols(t)], preferred_element_type=jnp.float32
        )
        partial[:, :, cols(t)] = product.astype(jnp.bfloat16).reshape(n_ep, capacity, width)

    load.wait()
    turns = [*range(1, ny), 0]
    for off in turns:
        multiply(p.y_at(off) * 2 + (1 - p.c))
        multiply(p.chip(off))
        for k in order:
            pair_copy(p.ep(k), off).start()
        for k in order:
            s = p.ep(k)
            pair_copy(s, off).wait_recv()
            both = partial[s, :, cols(p.chip(off))].astype(jnp.float32) + pair[s, off].astype(
                jnp.float32
            )
            if off == 0:
                mine[s] = both
            else:
                out_y[s, off - 1] = both.astype(jnp.bfloat16)
                y_copy(s, off, off).start()
    for k in range(n_ep):
        head_move.wait_arrival(k)
        spread.first(p.ep(k))
    for k in order:
        s = p.ep(k)
        total = mine[s]
        for off in range(1, ny):
            y_copy(s, off, -off).wait_recv()
            total = total + in_y[s, off - 1].astype(jnp.float32)
        if k == 0:
            ret[s] = total.astype(jnp.bfloat16)
        else:
            final[s] = total.astype(jnp.bfloat16)
            final_copy(k).start()
    for k in range(n_ep):
        spread.relay(p.ep(k))
    for k in range(n_ep):
        spread.finish(p.ep(k))
    for k in range(n_ep):
        s = p.ep(k)
        for off in range(ny):
            pair_copy(s, off).wait_send()
        for off in range(1, ny):
            y_copy(s, off, off).wait_send()
    for k in range(1, n_ep):
        s = p.ep(k)
        remote(final.at[s], ret.at[s], a0.at[s], a1.at[s], s, p.t).wait_recv()
        final_copy(k).wait_send()
    head_move.wait_sent()


def outward(slots, message, gates, gate_weight, up_weight, n_ep, n_tp):
    _, capacity, width = slots.shape
    rows, units = n_ep * capacity, gate_weight.shape[0]
    scratch = [
        pltpu.VMEM((n_ep, capacity, width * n_tp), slots.dtype),
        pltpu.VMEM(gate_weight.shape, gate_weight.dtype),
        pltpu.VMEM(up_weight.shape, up_weight.dtype),
        pltpu.VMEM((rows, units), jnp.float32),
        pltpu.VMEM((rows, units), jnp.float32),
    ]
    sems = [DMA((n_ep,))] * 6 + [DMA((2,))] + spread_sems(n_ep, n_tp)
    return pl.pallas_call(
        functools.partial(outward_kernel, n_ep, n_tp),
        out_shape=[
            jax.ShapeDtypeStruct((rows, units), slots.dtype),
            jax.ShapeDtypeStruct(message.shape, message.dtype),
            jax.ShapeDtypeStruct(gates.shape, gates.dtype),
        ],
        in_specs=[VM] * 3 + [ANY] * 2,
        out_specs=[VM] * 3,
        scratch_shapes=scratch + sems,
        compiler_params=pltpu.CompilerParams(collective_id=0, has_side_effects=True),
        name="outward",
    )(slots, message, gates, gate_weight, up_weight)


def homeward(hidden, down_weight, heads, n_ep, n_tp):
    capacity, features = hidden.shape[0] // n_ep, down_weight.shape[1]
    width, ny = features // n_tp, n_tp // 2
    far = max(ny - 1, 1)
    scratch = [
        pltpu.VMEM((n_ep, capacity, features), jnp.bfloat16),
        pltpu.VMEM(down_weight.shape, down_weight.dtype),
        pltpu.VMEM((n_ep, ny, capacity, width), jnp.bfloat16),
        pltpu.VMEM((n_ep, capacity, width), jnp.float32),
        pltpu.VMEM((n_ep, far, capacity, width), jnp.bfloat16),
        pltpu.VMEM((n_ep, far, capacity, width), jnp.bfloat16),
        pltpu.VMEM((n_ep, capacity, width), jnp.bfloat16),
    ]
    sems = [DMA((1,))] + [DMA((n_ep,))] * 4 + [DMA((n_ep, ny))] * 2 + [DMA((n_ep, far))] * 2
    return pl.pallas_call(
        functools.partial(homeward_kernel, n_ep, n_tp),
        out_shape=[
            jax.ShapeDtypeStruct((n_ep, capacity, width), jnp.bfloat16),
            jax.ShapeDtypeStruct((n_tp,) + heads.shape, jnp.bfloat16),
        ],
        in_specs=[VM, ANY, VM],
        out_specs=[VM] * 2,
        scratch_shapes=scratch + sems + spread_sems(n_ep, n_tp),
        compiler_params=pltpu.CompilerParams(collective_id=1, has_side_effects=True),
        name="homeward",
    )(hidden, down_weight, heads)


def on_device(
    mixer_tokens,
    mixer_gain,
    query_weight,
    key_weight,
    value_weight,
    forget_weight,
    forget_bias,
    output_weight,
    expert_tokens,
    expert_gain,
    routes,
    route_weights,
    gate_weight,
    up_weight,
    down_weight,
):
    n_ep, n_tp = lax.axis_size("ep"), lax.axis_size("tp")
    rows, features = mixer_tokens.shape
    local_heads = forget_weight.shape[1]
    share = n_ep // local_heads
    part = rows // share
    width = features // n_tp
    bf16, f32 = jnp.bfloat16, jnp.float32

    expert_normed = normed_rows(expert_tokens, expert_gain)
    token_count, top_count = routes.shape
    capacity = 2 * top_count * token_count // n_ep
    pairs = token_count * top_count
    flat_routes = routes.reshape(-1)
    onehot = flat_routes[:, None] == jnp.arange(n_ep, dtype=jnp.int32)[None, :]
    before = jnp.tril(jnp.ones((pairs, pairs), bf16), -1)
    ranks = jnp.dot(before, onehot.astype(bf16), preferred_element_type=f32)
    slot_rank = jnp.sum(jnp.where(onehot, ranks, 0.0), axis=1).astype(jnp.int32)
    slot_index = (flat_routes * capacity + slot_rank).reshape(token_count, top_count)
    slot_ids = jnp.arange(n_ep * capacity, dtype=jnp.int32)
    picks = [(slot_index[:, j][:, None] == slot_ids[None, :]).astype(bf16) for j in range(top_count)]
    column = lax.axis_index("tp") * width
    own_columns = lax.dynamic_slice_in_dim(expert_normed, column, width, 1)
    slots = lax.dot_general(
        sum(picks[1:], picks[0]), own_columns, (((0,), (0,)), ((), ())),
        preferred_element_type=f32,
    ).astype(bf16).reshape(n_ep, capacity, width)

    normed = normed_rows(mixer_tokens, mixer_gain)
    queries = by_rows(normed, query_weight).astype(bf16)
    key_rows = by_rows(normed, key_weight).astype(bf16)
    value_rows = by_rows(normed, value_weight).astype(bf16)
    pre_gate = jnp.dot(normed, forget_weight, preferred_element_type=f32) + forget_bias
    block_cum = jnp.dot(
        jnp.tril(jnp.ones((rows, rows), f32)), jax.nn.log_sigmoid(pre_gate),
        precision=lax.Precision.HIGHEST, preferred_element_type=f32,
    )
    key_value = jnp.concatenate(
        [
            key_rows.reshape(rows, local_heads, HD).transpose(1, 0, 2),
            value_rows.reshape(rows, local_heads, HD).transpose(1, 0, 2),
        ],
        axis=2,
    )
    key_value = jnp.broadcast_to(
        key_value[:, None], (local_heads, share, rows, 2 * HD)
    ).reshape(n_ep, rows, 2 * HD)
    half = part // 2
    query_parts = queries.reshape(share, 2, half, local_heads, HD).transpose(3, 0, 2, 1, 4)
    query_parts = query_parts.reshape(n_ep, half, 2 * HD)
    message = jnp.concatenate([key_value, query_parts], axis=1)
    gates = jnp.broadcast_to(block_cum.T[:, None, None, :], (local_heads, share, 1, rows))
    gates = gates.reshape(n_ep, 1, rows)

    hidden, all_messages, all_gates = outward(
        slots, message, gates, gate_weight[0], up_weight[0], n_ep, n_tp
    )

    positions = n_ep * rows
    all_gates = all_gates.reshape(n_ep, rows)
    totals = all_gates[:, rows - 1]
    lower = jnp.arange(n_ep)[None, :] < jnp.arange(n_ep)[:, None]
    base = jnp.sum(jnp.where(lower, totals[None, :], 0.0), axis=1)
    cumulative = all_gates + base[:, None]
    keys = all_messages[:, :rows, :HD].reshape(positions, HD)
    values = all_messages[:, :rows, HD:].reshape(positions, HD)
    head_query = all_messages[:, rows:].reshape(n_ep, half, 2, HD).transpose(0, 2, 1, 3)
    head_query = head_query.reshape(n_ep * part, HD)
    first = (lax.axis_index("ep") % share) * part
    query_cum = lax.dynamic_slice_in_dim(cumulative, first, part, 1).reshape(-1)
    query_pos = (
        jnp.arange(n_ep, dtype=jnp.int32)[:, None] * rows
        + first
        + jnp.arange(part, dtype=jnp.int32)[None, :]
    ).reshape(-1)
    key_pos = jnp.arange(positions, dtype=jnp.int32)
    scores = by_rows(head_query, keys) * HD ** (-0.5)
    scores = scores + query_cum[:, None] - cumulative.reshape(-1)[None, :]
    scores = jnp.where(key_pos[None, :] <= query_pos[:, None], scores, -jnp.inf)
    weights = jnp.exp(scores - jnp.max(scores, axis=-1, keepdims=True)).astype(bf16)
    attended = jnp.dot(weights, values, preferred_element_type=f32)
    rescale = lax.rsqrt(jnp.mean(attended * attended, axis=-1, keepdims=True) + HEAD_FLOOR)
    head_out = (attended * rescale).astype(bf16).reshape(n_ep, part, HD)

    returned, heads_all = homeward(hidden, down_weight[0], head_out, n_ep, n_tp)

    heads_all = heads_all.reshape(n_tp, local_heads, share, part, HD).transpose(2, 3, 0, 1, 4)
    heads_all = heads_all.reshape(rows, n_tp * local_heads * HD)
    mixer_output = jnp.dot(heads_all, output_weight, preferred_element_type=f32).astype(bf16)
    returned = returned.reshape(n_ep * capacity, width)
    expert_output = 0.0
    for j in range(top_count):
        picked = jnp.dot(picks[j], returned, preferred_element_type=f32)
        expert_output = expert_output + picked * route_weights[:, j][:, None]
    return (mixer_output, expert_output.astype(bf16))


def lanes_of(shape, dim):
    return lax.broadcasted_iota(jnp.int32, shape, dim)


class Relay:
    def __init__(self, place, land, sems, batch):
        self.p, self.land, self.batch = place, land, batch
        self.ys, self.yr, self.ps, self.pr = sems

    def y_copy(self, off, s, t, to):
        block = self.land(t, s)
        return remote(block, block, self.ys.at[0], self.yr.at[off - 1, s], self.p.e, to)

    def p_copy(self, off, s, t):
        block, p = self.land(t, s), self.p
        return remote(block, block, self.ps.at[0], self.pr.at[self.batch(s)], p.e, p.partner)

    def first(self, s):
        p = self.p
        for off in range(1, p.ny):
            self.y_copy(off, s, p.t, p.chip(off)).start()
        self.p_copy(0, s, p.t).start()

    def relay(self, s):
        p = self.p
        for off in range(1, p.ny):
            self.y_copy(off, s, p.chip(-off), p.chip(-off)).wait_recv()
            self.p_copy(off, s, p.chip(-off)).start()

    def settle(self, batch, blocks):
        p = self.p
        remote(blocks, blocks, self.ps.at[0], self.pr.at[batch], p.e, p.partner).wait_recv()

    def sent(self, y_blocks, p_blocks):
        p = self.p
        remote(y_blocks, y_blocks, self.ys.at[0], self.yr.at[0, 0], p.e, p.partner).wait_send()
        remote(p_blocks, p_blocks, self.ps.at[0], self.pr.at[0], p.e, p.partner).wait_send()


def flipped(place, bits):
    at, weight = place, 1
    while bits:
        if bits % 2:
            at = at + weight * (1 - 2 * (place // weight % 2))
        bits, weight = bits // 2, weight * 2
    return at


def fused_kernel(
    n_ep, n_tp,
    tokens_a, gain_a, w_q, w_k, w_v, w_f, b_f, w_o, tokens_b, gain_b, routes, route_w,
    w_gate, w_up, w_down,
    out_a, out_b,
    a_held, ga_held, q_held, kv_held, f_held, bf_held, o_held, b_held, gb_held, r_held, rw_held,
    gate_held, up_held, down_held,
    slots, slots_more, land, w_hi, w_lo, kv_send, q_send, g_send, kv_land, q_land, g_land,
    hidden, pair_send, pair_land, own_part, mine, y_send, y_land, final, ret,
    q_all, q_cum, scores, running, row_max, attended, head_send, heads_all, lhs, mixed,
    lsem, s0, s1, m0, m1, ys, yr, ps, pr, k0, k1, x0, x1, q0, q1, g0, g1,
    p0, p1, z0, z1, a0, a1, h0, h1, hy0, hy1, hp0, hp1,
):
    p = Place(n_ep, n_tp)
    ny = p.ny
    bf16, f32 = jnp.bfloat16, jnp.float32
    rows, features = a_held.shape
    tokens = b_held.shape[0]
    _, capacity, width = slots.shape
    local_heads = kv_send.shape[0]
    share = n_ep // local_heads
    part = rows // share
    half = part // 2
    units = gate_held.shape[0]
    quarter = n_ep // 4
    near, second, third = range(2 * quarter), range(2 * quarter, 3 * quarter), range(3 * quarter, n_ep)
    groups = [near[:quarter], range(quarter, 3 * quarter), third]
    own_share = p.e % share
    first = own_share * part

    def cols(t):
        return pl.ds(pl.multiple_of(t * width, width), width)

    def peer(j):
        return flipped(p.e, j + quarter if j in second else j - quarter if j in third else j)

    barrier = pltpu.get_barrier_semaphore()
    for k in range(1, n_ep):
        pl.semaphore_signal(
            barrier, inc=1, device_id={"ep": p.ep(k), "tp": p.t}, device_id_type=MESH
        )
    for off in range(1, ny):
        pl.semaphore_signal(
            barrier, inc=1, device_id={"ep": p.e, "tp": p.chip(off)}, device_id_type=MESH
        )
    pl.semaphore_signal(
        barrier, inc=1, device_id={"ep": p.e, "tp": p.partner}, device_id_type=MESH
    )

    early = [(tokens_b, b_held), (routes, r_held), (gain_b, gb_held)]
    middle = [(tokens_a, a_held), (gain_a, ga_held), (w_f, f_held), (b_f, bf_held), (w_q, q_held)]
    late = [
        (w_gate, gate_held), (w_up, up_held), (w_down, down_held), (route_w, rw_held),
        (w_o, o_held),
    ]
    loads, number = [], 0
    for batch in (early, middle, late):
        made = []
        for src, dst in batch:
            made.append(pltpu.make_async_copy(src, dst, lsem.at[number]))
            number += 1
        loads.append(made)
    pieces = []
    for h in range(local_heads):
        mine_rows = pl.ds(h * HD, HD)
        for at, src in ((2 * h, w_k), (2 * h + 1, w_v)):
            there = kv_held.at[pl.ds(at * HD, HD)]
            pieces.append(pltpu.make_async_copy(src.at[mine_rows], there, lsem.at[number]))
    all_pieces = pltpu.make_async_copy(kv_held, kv_held, lsem.at[number])
    early, middle, late = loads
    for load in early + middle + pieces:
        load.start()

    for load in early:
        load.wait()
    values = b_held[...].astype(f32)
    square = jnp.mean(values * values, axis=-1, keepdims=True)
    scale = lax.rsqrt(jnp.maximum(square, MEAN_FLOOR))
    b_held[...] = (values * scale * gb_held[...]).astype(bf16)
    named_by = r_held[...]
    top_count = named_by.shape[0]
    place = lanes_of((n_ep, tokens), 0)
    place = place + jnp.where(place < 2 * quarter, 0, jnp.where(place < 3 * quarter, 1, -1)) * quarter
    expert_at, weight = place, 1
    while weight < n_ep:
        flip = (p.e // weight) % 2
        expert_at = expert_at + flip * weight * (1 - 2 * ((place // weight) % 2))
        weight *= 2
    chosen = [named_by[c : c + 1, :] == expert_at for c in range(top_count)]
    named = sum([c.astype(f32) for c in chosen[1:]], chosen[0].astype(f32))
    earlier = (lanes_of((tokens, tokens), 0) < lanes_of((tokens, tokens), 1)).astype(bf16)
    ranks = jnp.dot(named.astype(bf16), earlier, preferred_element_type=f32)
    ranks = jnp.where(named > 0, ranks, -1.0).astype(jnp.int32)
    slot_at = lanes_of((capacity, tokens), 0)
    picks = [ranks[j : j + 1, :] == slot_at for j in range(n_ep)]
    picks = [pick.astype(f32).astype(bf16) for pick in picks]

    def picked(j, lanes):
        return jnp.dot(picks[j], b_held[:, lanes], preferred_element_type=f32).astype(bf16)

    for j in range(1, n_ep):
        slots[j] = picked(j, cols(p.t))
    for j in near[1:]:
        for off in range(1, ny):
            slots_more[j, off - 1] = picked(j, cols(p.chip(-off)))
    pl.semaphore_wait(barrier, n_ep - 1 + ny - 1 + 1)

    def slot_copy(j):
        return remote(
            slots.at[j], land.at[j, :, cols(p.t)], s0.at[0], s1.at[j], peer(j), p.t
        )

    def more_copy(j, off):
        return remote(
            slots_more.at[j, off - 1], land.at[j, :, cols(p.chip(-off))],
            m0.at[0], m1.at[j, off - 1], peer(j), p.t,
        )

    def send(j):
        slot_copy(j).start()
        if j in near:
            for off in range(1, ny):
                more_copy(j, off).start()

    spread = Relay(
        p,
        lambda t, j: land.at[j, :, cols(t)],
        (ys, yr, ps, pr),
        lambda j: [j in group for group in groups].index(True),
    )
    for j in [*near[1:quarter], *second, *near[quarter:], *third]:
        send(j)
    land[0] = picked(0, slice(None))

    for load in middle + [all_pieces]:
        load.wait()
    for load in late:
        load.start()
    values = a_held[...].astype(f32)
    square = jnp.mean(values * values, axis=-1, keepdims=True)
    scale = lax.rsqrt(jnp.maximum(square, MEAN_FLOOR))
    a_held[...] = (values * scale * ga_held[...]).astype(bf16)
    normed = a_held[...]
    eye = lanes_of((local_heads, local_heads), 0) == lanes_of((local_heads, local_heads), 1)
    bias = jnp.sum(jnp.where(eye, bf_held[...], 0.0), axis=1, keepdims=True)
    gate = by_rows(f_held[...], normed) + bias
    log_gate = jnp.minimum(gate, 0.0) - jnp.log1p(jnp.exp(-jnp.abs(gate)))
    upto = (lanes_of((rows, rows), 0) <= lanes_of((rows, rows), 1)).astype(f32)
    block_cum = jnp.dot(
        log_gate, upto, precision=lax.Precision.HIGHEST, preferred_element_type=f32
    )
    for h in range(local_heads):
        g_send[h] = block_cum[h : h + 1, :]

    def kv_copy(h):
        to = h * share + own_share
        return remote(kv_send.at[h], kv_land.at[p.e], k0.at[0], k1.at[p.e // share], to, p.t)

    def kv_arrival(n):
        s = (p.e // share + n) % local_heads * share + own_share
        return remote(kv_send.at[0], kv_land.at[s], k0.at[0], k1.at[s // share], p.e, p.t), s

    def sibling(off):
        return p.e // share * share + (own_share + off) % share

    def kv_relay(s, off):
        return remote(
            kv_land.at[s], kv_land.at[s], x0.at[0], x1.at[0], sibling(off), p.t
        )

    def q_copy(k):
        d = p.ep(k)
        return remote(q_send.at[d], q_land.at[p.e], q0.at[0], q1.at[0], d, p.t)

    def g_copy(k):
        d = p.ep(k)
        return remote(g_send.at[d // share], g_land.at[p.e], g0.at[0], g1.at[0], d, p.t)

    def others(ref):
        return ref.at[pl.ds(0, n_ep - 1)]

    def batch_of(ref, send, recv):
        return remote(ref, ref, send.at[0], recv.at[0], p.e, p.partner)

    key_value = by_rows(normed, kv_held[...]).astype(bf16)
    for h in range(local_heads):
        kv_send[h] = key_value[:, 2 * h * HD : 2 * (h + 1) * HD]
    for n in range(1, local_heads):
        kv_copy((p.e // share + n) % local_heads).start()
    own_head = p.e // share
    kv_land[p.e] = kv_send[own_head]
    for off in range(1, share):
        kv_relay(p.e, off).start()
    queries = by_rows(normed, q_held[...]) * HD ** (-0.5)
    left = lanes_of((half, 2 * HD), 1) < HD
    for pair in range(local_heads // 2):
        there = queries[:, 2 * pair * HD : 2 * (pair + 1) * HD]
        moved = pltpu.roll(there, HD, 1)
        for x in range(share):
            top, bottom = slice(x * part, x * part + half), slice(x * part + half, (x + 1) * part)
            q_send[2 * pair * share + x] = jnp.where(left, there[top], moved[bottom]).astype(bf16)
            q_send[(2 * pair + 1) * share + x] = jnp.where(
                left, moved[top], there[bottom]
            ).astype(bf16)
    for k in range(1, n_ep):
        q_copy(k).start()
        g_copy(k).start()
    q_land[p.e] = q_send[p.e]
    g_land[p.e] = g_send[own_head]

    def arrive(j):
        slot_copy(j).wait_recv()
        if j in near:
            spread.p_copy(0, j, p.t).start()
            for off in range(1, ny):
                more_copy(j, off).wait_recv()
                spread.p_copy(off, j, p.chip(-off)).start()
        else:
            spread.first(j)

    def complete(j):
        spread.relay(j)

    def settle(g):
        count = len(groups[g]) - (0 in groups[g])
        spread.settle(g, land.at[pl.ds(0, count), :, pl.ds(0, ny * width)])

    cuts = [(at, min(at + 512, units)) for at in range(0, units, 512)]

    def serve(beside, number, count):
        for act, *given in beside[len(beside) * number // count : len(beside) * (number + 1) // count]:
            act(*given)

    def open_up(g, beside):
        low_row, count = groups[g][0], len(groups[g])
        block = land[low_row : low_row + count].reshape(count * capacity, features)
        lines = slice(low_row * capacity, (low_row + count) * capacity)
        for number, (low, high) in enumerate(cuts):
            gated = by_rows(gate_held[low:high], block)
            upped = by_rows(up_held[low:high], block)
            hidden[lines, low:high] = (gated * lax.logistic(gated) * upped).astype(bf16).T
            serve(beside, number, len(cuts))

    def pair_copy(g, off):
        low_row, count = groups[g][0], len(groups[g])
        lines = pl.ds(low_row * capacity, count * capacity)
        return remote(
            pair_send.at[off, lines], pair_land.at[off, lines], p0.at[0], p1.at[g, off],
            p.e, p.partner,
        )

    def y_copy(j, off, to):
        return remote(
            y_send.at[j, off - 1], y_land.at[j, off - 1],
            z0.at[0], z1.at[j, off - 1], p.e, p.chip(to),
        )

    turns = [*range(1, ny), 0]

    def close_down(g, beside, held=()):
        low_row, count = groups[g][0], len(groups[g])
        lines = slice(low_row * capacity, (low_row + count) * capacity)

        def product(t):
            return jnp.dot(hidden[lines], down_held[:, cols(t)], preferred_element_type=f32)

        for number, off in enumerate(turns):
            pair_send[off, lines] = product(p.y_at(off) * 2 + (1 - p.c)).astype(bf16)
            pair_copy(g, off).start()
            serve(beside, number, 2 * ny)
        for number, off in enumerate(turns):
            own_part[lines] = product(p.chip(off))
            serve(beside, ny + number, 2 * ny)
            pair_copy(g, off).wait_recv()
            both = own_part[lines] + pair_land[off, lines].astype(f32)
            both = both.reshape(count, capacity, width)
            for m in range(count):
                j = low_row + m
                if off == 0:
                    mine[j] = both[m]
                else:
                    y_send[j, off - 1] = both[m].astype(bf16)
                    if j not in held:
                        y_copy(j, off, off).start()

    def final_copy(j):
        return remote(final.at[j], ret.at[j], a0.at[0], a1.at[0], peer(j), p.t)

    def finish(j):
        total = mine[j]
        for off in range(1, ny):
            y_copy(j, off, -off).wait_recv()
            total = total + y_land[j, off - 1].astype(f32)
        if j == 0:
            ret[0] = total.astype(bf16)
        else:
            final[j] = total.astype(bf16)
            final_copy(j).start()

    def kv_forward(n):
        copy, s = kv_arrival(n)
        copy.wait_recv()
        for off in range(1, share):
            kv_relay(s, off).start()

    some = len(second) // 2
    for j in [*near[1:quarter], *second[:some]]:
        arrive(j)
    settle(0)
    late[0].wait()
    late[1].wait()
    open_up(0, [(arrive, j) for j in [*second[some:], *near[quarter : quarter + quarter // 2]]])
    late[2].wait()
    close_down(
        0,
        [(arrive, j) for j in near[quarter + quarter // 2 :]] + [(complete, j) for j in second],
        near,
    )
    settle(1)
    open_up(1, [(arrive, j) for j in third])
    close_down(1, [], near)
    for j in near[quarter:]:
        for off in range(1, ny):
            y_copy(j, off, off).start()
    complete(third[0])
    for n in range(1, local_heads):
        kv_forward(n)
    for j in third[1:]:
        complete(j)
    settle(2)
    open_up(2, [(finish, j) for j in second])
    close_down(2, [])
    behind = near[:quarter]
    for j in behind:
        for off in range(1, ny):
            y_copy(j, off, off).start()

    late[3].wait()
    for j in range(n_ep):
        weight = 0.0
        for c in range(top_count):
            weight = weight + jnp.where(
                named_by[c : c + 1, :] == peer(j), rw_held[c : c + 1, :], 0.0
            )
        weight = jnp.where(ranks[j : j + 1, :] == slot_at, weight, 0.0)
        high = weight.astype(bf16)
        w_hi[j * capacity : (j + 1) * capacity] = high
        w_lo[j * capacity : (j + 1) * capacity] = (weight - high.astype(f32)).astype(bf16)

    batch_of(others(g_land), g0, g1).wait_recv()
    batch_of(others(q_land), q0, q1).wait_recv()
    relayed = kv_land.at[pl.ds(0, local_heads * (share - 1))]
    batch_of(relayed, x0, x1).wait_recv()
    positions = lanes_of((part, rows), 1)
    asked = first + lanes_of((part, rows), 0)
    base = jnp.zeros((1, 1), f32)
    key_cum = []
    last = lanes_of((1, rows), 1) == rows - 1
    for b in range(n_ep):
        block = g_land[b]
        key_cum.append(block + base)
        base = base + jnp.sum(jnp.where(last, block, 0.0), axis=1, keepdims=True)
        at = b * part
        q_cum[at : at + part] = jnp.sum(
            jnp.where(positions == asked, key_cum[b], 0.0), axis=1, keepdims=True
        )
        packed = q_land[b].astype(f32)
        q_all[at : at + half] = jnp.where(left, packed, 0.0).astype(bf16)
        q_all[at + half : at + part] = jnp.where(
            left, pltpu.roll(packed, HD, 1), 0.0
        ).astype(bf16)
    for b in range(n_ep):
        at = b * part
        block = by_rows(q_all[at:], kv_land[b]) + q_cum[at:] - key_cum[b]
        seen = jnp.where(positions <= asked, block[:part], -jnp.inf)
        scores[b, at : at + part] = seen
        if b == 0:
            running[:part] = seen
            running[part:] = block[part:]
        else:
            running[at : at + part] = jnp.maximum(running[at : at + part], seen)
        if b + 1 < n_ep:
            scores[b, at + part :] = block[part:]
            if b > 0:
                running[at + part :] = jnp.maximum(running[at + part :], block[part:])
    row_max[...] = jnp.max(running[...], axis=1, keepdims=True)
    for b in range(n_ep):
        at = b * part
        weights = jnp.exp(scores[b, at:] - row_max[at:]).astype(bf16)
        product = jnp.dot(weights, kv_land[b], preferred_element_type=f32)
        if b == 0:
            attended[...] = product
        else:
            attended[at:] = attended[at:] + product
    right = lanes_of((part, 2 * HD), 1) >= HD
    for b in range(n_ep):
        block = jnp.where(right, attended[b * part : (b + 1) * part], 0.0)
        block = block * lax.rsqrt(
            jnp.sum(block * block, axis=1, keepdims=True) * (1.0 / HD) + HEAD_FLOOR
        )
        moved = pltpu.roll(block, HD, 1)
        head_send[b] = jnp.where(left, moved[:half], block[half:]).astype(bf16)

    def head_copy(k):
        d = peer(k)
        return remote(head_send.at[d], heads_all.at[p.t, p.e], h0.at[0], h1.at[p.e], d, p.t)

    def head_arrival(k):
        s = peer(k)
        return remote(head_send.at[s], heads_all.at[p.t, s], h0.at[0], h1.at[s], s, p.t)

    for k in [*second, *third, *near[1:]]:
        head_copy(k).start()
    heads_all[p.t, p.e] = head_send[p.e]

    for j in near[quarter:]:
        finish(j)
    for j in third:
        finish(j)

    gather = Relay(p, lambda t, s: heads_all.at[t, s], (hy0, hy1, hp0, hp1), lambda s: 0)
    gather.first(p.e)
    for k in near[1:]:
        head_arrival(k).wait_recv()
        gather.first(peer(k))
    for j in behind:
        finish(j)
    for k in [*second, *third]:
        head_arrival(k).wait_recv()
        gather.first(peer(k))
    for k in range(n_ep):
        gather.relay(peer(k))
    late[4].wait()

    def project(t):
        for pair in range(local_heads // 2):
            lanes = slice(2 * pair * HD, 2 * (pair + 1) * HD)
            for x in range(share):
                one = heads_all[t, 2 * pair * share + x].astype(f32)
                two = heads_all[t, (2 * pair + 1) * share + x].astype(f32)
                at = x * part
                lhs[at : at + half, lanes] = jnp.where(
                    left, one, pltpu.roll(two, HD, 1)
                ).astype(bf16)
                lhs[at + half : at + part, lanes] = jnp.where(
                    left, pltpu.roll(one, HD, 1), two
                ).astype(bf16)
        deep = local_heads * HD
        here = o_held[pl.ds(pl.multiple_of(t * deep, deep), deep), :]
        return jnp.dot(lhs[...], here, preferred_element_type=f32)

    mixed[...] = project(p.t)
    for off in range(1, ny):
        mixed[...] = mixed[...] + project(p.chip(-off))
    gather.settle(0, heads_all.at[pl.ds(0, ny)])
    for off in range(ny - 1):
        mixed[...] = mixed[...] + project(p.y_at(-off) * 2 + (1 - p.c))
    last_part = project(p.y_at(-(ny - 1)) * 2 + (1 - p.c))
    out_a[...] = (mixed[...] + last_part).astype(bf16)

    batch_of(others(ret), a0, a1).wait_recv()
    returned = ret[...].reshape(n_ep * capacity, width)
    over_slots = (((0,), (0,)), ((), ()))
    total = lax.dot_general(w_hi[...], returned, over_slots, preferred_element_type=f32)
    total = total + lax.dot_general(w_lo[...], returned, over_slots, preferred_element_type=f32)
    out_b[...] = total.astype(bf16)

    spread.sent(
        land.at[pl.ds(0, n_ep - len(near)), :, pl.ds(0, (ny - 1) * width)],
        land.at[pl.ds(0, n_ep - 1), :, pl.ds(0, ny * width)],
    )
    gather.sent(heads_all.at[pl.ds(0, ny - 1)], heads_all.at[pl.ds(0, ny)])
    for ref, send, recv in (
        (others(slots), s0, s1), (slots_more.at[pl.ds(0, len(near) - 1)], m0, s1), (others(q_send), q0, q1), (others(final), a0, a1),
        (others(head_send), h0, h1), (pair_send, p0, a1), (y_send, z0, a1),
        (others(g_land), g0, g1), (kv_send.at[pl.ds(0, local_heads - 1)], k0, k1),
        (relayed, x0, x1),
    ):
        batch_of(ref, send, recv).wait_send()


def fused_on_device(
    mixer_tokens, mixer_gain, query_weight, key_weight, value_weight, forget_weight,
    forget_bias, output_weight, expert_tokens, expert_gain, routes, route_weights,
    gate_weight, up_weight, down_weight,
):
    n_ep, n_tp = lax.axis_size("ep"), lax.axis_size("tp")
    ny = n_tp // 2
    far = max(ny - 1, 1)
    rows, features = mixer_tokens.shape
    tokens, top_count = routes.shape
    local_heads = forget_weight.shape[1]
    share = n_ep // local_heads
    part = rows // share
    half = part // 2
    width = features // n_tp
    capacity = 2 * top_count * tokens // n_ep
    units = gate_weight.shape[1]
    groups = 3
    asked = n_ep * part
    bf16, f32 = jnp.bfloat16, jnp.float32
    operands = [
        mixer_tokens, mixer_gain.reshape(1, features), query_weight, key_weight, value_weight,
        forget_weight.T, forget_bias, output_weight, expert_tokens,
        expert_gain.reshape(1, features), routes.T, route_weights.T,
        gate_weight[0], up_weight[0], down_weight[0],
    ]
    operands = [pltpu.with_memory_space_constraint(x, pltpu.HBM) for x in operands]
    vmem = pltpu.VMEM
    scratch = [
        vmem((rows, features), bf16), vmem((1, features), f32),
        vmem(query_weight.shape, bf16), vmem((2 * local_heads * HD, features), bf16),
        vmem((local_heads, features), bf16), vmem((1, local_heads), f32),
        vmem(output_weight.shape, bf16), vmem((tokens, features), bf16),
        vmem((1, features), f32), vmem((top_count, tokens), jnp.int32),
        vmem((top_count, tokens), f32),
        vmem((units, features), bf16), vmem((units, features), bf16),
        vmem((units, features), bf16),
        vmem((n_ep, capacity, width), bf16), vmem((n_ep // 2, far, capacity, width), bf16),
        vmem((n_ep, capacity, features), bf16),
        vmem((n_ep * capacity, tokens), bf16), vmem((n_ep * capacity, tokens), bf16),
        vmem((local_heads, rows, 2 * HD), bf16), vmem((n_ep, half, 2 * HD), bf16),
        vmem((local_heads, 1, rows), f32),
        vmem((n_ep, rows, 2 * HD), bf16), vmem((n_ep, half, 2 * HD), bf16),
        vmem((n_ep, 1, rows), f32),
        vmem((n_ep * capacity, units), bf16),
        vmem((ny, n_ep * capacity, width), bf16),
        vmem((ny, n_ep * capacity, width), bf16),
        vmem((n_ep * capacity, width), f32),
        vmem((n_ep, capacity, width), f32),
        vmem((n_ep, far, capacity, width), bf16), vmem((n_ep, far, capacity, width), bf16),
        vmem((n_ep, capacity, width), bf16), vmem((n_ep, capacity, width), bf16),
        vmem((asked, 2 * HD), bf16), vmem((asked, 1), f32),
        vmem((n_ep, asked, rows), f32), vmem((asked, rows), f32), vmem((asked, 1), f32),
        vmem((asked, 2 * HD), f32), vmem((n_ep, half, 2 * HD), bf16),
        vmem((n_tp, n_ep, half, 2 * HD), bf16), vmem((rows, local_heads * HD), bf16), vmem((rows, width), f32),
    ]
    one = DMA((1,))
    sems = [DMA((14,)), one, DMA((n_ep,)), one, DMA((n_ep // 2, far)), one, DMA((far, n_ep)), one, DMA((groups,))]
    sems += [one, DMA((local_heads,))] + [one] * 6
    sems += [one, DMA((groups, ny)), one, DMA((n_ep, far)), one, one, one, DMA((n_ep,))]
    sems += [one, DMA((far, n_ep)), one, one]
    return pl.pallas_call(
        functools.partial(fused_kernel, n_ep, n_tp),
        out_shape=[
            jax.ShapeDtypeStruct((rows, width), bf16),
            jax.ShapeDtypeStruct((tokens, width), bf16),
        ],
        in_specs=[ANY] * len(operands),
        out_specs=[VM] * 2,
        scratch_shapes=scratch + sems,
        compiler_params=pltpu.CompilerParams(
            collective_id=2, has_side_effects=True, vmem_limit_bytes=LIMIT
        ),
        name="fused",
    )(*operands)


def deliver_kernel(one, two, one_out, two_out, sem):
    copies = [
        pltpu.make_async_copy(one, one_out, sem.at[0]),
        pltpu.make_async_copy(two, two_out, sem.at[1]),
    ]
    for copy in copies:
        copy.start()
    for copy in copies:
        copy.wait()


def deliver(one, two):
    return pl.pallas_call(
        deliver_kernel,
        out_shape=[
            jax.ShapeDtypeStruct(one.shape, one.dtype),
            jax.ShapeDtypeStruct(two.shape, two.dtype),
        ],
        in_specs=[ANY] * 2,
        out_specs=[ANY] * 2,
        scratch_shapes=[DMA((2,))],
        compiler_params=pltpu.CompilerParams(vmem_limit_bytes=1 << 20),
        name="deliver",
    )(one, two)


def choose(*arguments):
    n_ep = lax.axis_size("ep")
    rows, local_heads = arguments[0].shape[0], arguments[5].shape[1]
    share = n_ep // local_heads
    packed = local_heads % 2 == 0 and n_ep % local_heads == 0
    packed = packed and n_ep >= 8 and n_ep & (n_ep - 1) == 0 and lax.axis_size("tp") >= 4
    if packed and rows % (32 * share) == 0:
        return tuple(deliver(*fused_on_device(*arguments)))
    return on_device(*arguments)


def solution(mesh):
    in_specs = (
        P("ep", None),
        P(),
        P("tp", None),
        P("tp", None),
        P("tp", None),
        P(None, "tp"),
        P("ep", "tp"),
        P(None, "tp"),
        P("ep", None),
        P(),
        P("ep", None),
        P("ep", None),
        P("ep", "tp", None),
        P("ep", "tp", None),
        P("ep", "tp", None),
    )
    out_specs = (P("ep", "tp"), P("ep", "tp"))
    return jax.shard_map(
        choose, mesh=mesh, in_specs=in_specs, out_specs=out_specs, check_vma=False
    )
```

```python
import functools

import jax
import jax.numpy as jnp
from jax import lax
from jax.experimental import pallas as pl
from jax.experimental.pallas import tpu as pltpu
from jax.sharding import PartitionSpec as P

HD = 64
MEAN_FLOOR = 0.1
HEAD_FLOOR = 1.0
MESH = pl.DeviceIdType.MESH
VM = pl.BlockSpec(memory_space=pltpu.VMEM)
ANY = pl.BlockSpec(memory_space=pl.ANY)
DMA = pltpu.SemaphoreType.DMA
LIMIT = 48 << 20


def normed_rows(inputs, gain):
    values = inputs.astype(jnp.float32)
    square = jnp.mean(values * values, axis=-1, keepdims=True)
    return (values * lax.rsqrt(jnp.maximum(square, MEAN_FLOOR)) * gain).astype(jnp.bfloat16)


def by_rows(left, weight):
    return lax.dot_general(
        left, weight, (((1,), (1,)), ((), ())), preferred_element_type=jnp.float32
    )


class Place:
    def __init__(self, n_ep, n_tp):
        self.n_ep, self.n_tp, self.ny = n_ep, n_tp, n_tp // 2
        self.e = lax.axis_index("ep")
        self.t = lax.axis_index("tp")
        self.y, self.c = self.t // 2, self.t % 2
        self.partner = self.y * 2 + (1 - self.c)

    def ep(self, k):
        return (self.e + k) % self.n_ep

    def y_at(self, off):
        return (self.y + self.ny + off) % self.ny

    def chip(self, off):
        return self.y_at(off) * 2 + self.c

    def barrier(self):
        sem = pltpu.get_barrier_semaphore()
        for k in range(1, self.n_ep):
            pl.semaphore_signal(
                sem, inc=1, device_id={"ep": self.ep(k), "tp": self.t}, device_id_type=MESH
            )
        for off in range(1, self.ny):
            pl.semaphore_signal(
                sem, inc=1, device_id={"ep": self.e, "tp": self.chip(off)}, device_id_type=MESH
            )
        pl.semaphore_signal(
            sem, inc=1, device_id={"ep": self.e, "tp": self.partner}, device_id_type=MESH
        )
        pl.semaphore_wait(sem, self.n_ep - 1 + self.ny - 1 + 1)


def remote(src, dst, send, recv, e, t):
    return pltpu.make_async_remote_copy(
        src_ref=src,
        dst_ref=dst,
        send_sem=send,
        recv_sem=recv,
        device_id={"ep": e, "tp": t},
        device_id_type=MESH,
    )


class Exchange:
    def __init__(self, place, send, land, sems):
        self.p, self.send, self.land = place, send, land
        self.ssem, self.rsem = sems

    def copy(self, k):
        p = self.p
        d = p.ep(k)
        return remote(
            self.send(d), self.land(p.e), self.ssem.at[d], self.rsem.at[p.e], d, p.t
        )

    def arrival(self, k):
        p = self.p
        s = p.ep(k)
        return remote(self.send(s), self.land(s), self.ssem.at[s], self.rsem.at[s], s, p.t)

    def own(self):
        p = self.p
        return pltpu.make_async_copy(self.send(p.e), self.land(p.e), self.rsem.at[p.e])

    def start(self):
        for k in range(1, self.p.n_ep):
            self.copy(k).start()
        self.own().start()

    def wait_arrival(self, k):
        if k == 0:
            self.own().wait()
        else:
            self.arrival(k).wait_recv()

    def wait_sent(self):
        for k in range(1, self.p.n_ep):
            self.copy(k).wait_send()


class Spread:
    def __init__(self, place, land, sems):
        self.p, self.land = place, land
        self.ys, self.yr, self.ps, self.pr = sems

    def y_copy(self, off, s):
        p = self.p
        block = self.land(p.t, s)
        return remote(
            block, block, self.ys.at[off - 1, s], self.yr.at[off - 1, s], p.e, p.chip(off)
        )

    def y_arrival(self, off, s):
        p = self.p
        block = self.land(p.chip(-off), s)
        return remote(
            block, block, self.ys.at[off - 1, s], self.yr.at[off - 1, s], p.e, p.chip(-off)
        )

    def p_copy(self, off, s):
        p = self.p
        block = self.land(p.chip(-off), s)
        return remote(block, block, self.ps.at[off, s], self.pr.at[off, s], p.e, p.partner)

    def p_arrival(self, off, s):
        p = self.p
        block = self.land(p.y_at(-off) * 2 + (1 - p.c), s)
        return remote(block, block, self.ps.at[off, s], self.pr.at[off, s], p.e, p.partner)

    def first(self, s):
        for off in range(1, self.p.ny):
            self.y_copy(off, s).start()
        self.p_copy(0, s).start()

    def relay(self, s):
        for off in range(1, self.p.ny):
            self.y_arrival(off, s).wait_recv()
            self.p_copy(off, s).start()

    def finish(self, s):
        for off in range(self.p.ny):
            self.p_arrival(off, s).wait_recv()
        self.wait_sent(s)

    def wait_sent(self, s):
        for off in range(self.p.ny):
            self.p_copy(off, s).wait_send()
        for off in range(1, self.p.ny):
            self.y_copy(off, s).wait_send()


def spread_sems(n_ep, n_tp):
    ny = n_tp // 2
    far = max(ny - 1, 1)
    return [DMA((far, n_ep)), DMA((far, n_ep)), DMA((ny, n_ep)), DMA((ny, n_ep))]


def outward_kernel(
    n_ep, n_tp, slots, message, gates, gate_weight, up_weight,
    hidden, message_out, gates_out,
    out, gate_held, up_held, gate_act, up_act,
    s0, s1, m0, m1, g0, g1, w, ys, yr, ps, pr,
):
    p = Place(n_ep, n_tp)
    width = slots.shape[2]

    def cols(t):
        return pl.ds(pl.multiple_of(t * width, width), width)

    def land(t, s):
        return out.at[s, :, cols(t)]

    def multiply(t, opening):
        rows = out[:, :, cols(t)].reshape(hidden.shape[0], width)
        for held, total in ((gate_held, gate_act), (up_held, up_act)):
            product = by_rows(rows, held[:, cols(t)])
            total[...] = product if opening else total[...] + product

    loads = [
        pltpu.make_async_copy(gate_weight, gate_held, w.at[0]),
        pltpu.make_async_copy(up_weight, up_held, w.at[1]),
    ]
    for load in loads:
        load.start()
    p.barrier()
    slot_move = Exchange(p, lambda d: slots.at[d], lambda s: land(p.t, s), (s0, s1))
    gate_move = Exchange(p, lambda d: gates.at[d], lambda s: gates_out.at[s], (g0, g1))
    message_move = Exchange(p, lambda d: message.at[d], lambda s: message_out.at[s], (m0, m1))
    spread = Spread(p, land, (ys, yr, ps, pr))
    slot_move.start()
    gate_move.start()
    message_move.start()
    for k in range(n_ep):
        slot_move.wait_arrival(k)
        spread.first(p.ep(k))
    for load in loads:
        load.wait()
    multiply(p.t, True)
    for k in range(n_ep):
        spread.p_arrival(0, p.ep(k)).wait_recv()
    multiply(p.partner, False)
    for k in range(n_ep):
        spread.relay(p.ep(k))
    for off in range(1, p.ny):
        multiply(p.chip(-off), False)
        for k in range(n_ep):
            spread.p_arrival(off, p.ep(k)).wait_recv()
        multiply(p.y_at(-off) * 2 + (1 - p.c), False)
    gate = gate_act[...]
    hidden[...] = (gate * lax.logistic(gate) * up_act[...]).astype(hidden.dtype)
    for k in range(n_ep):
        gate_move.wait_arrival(k)
        message_move.wait_arrival(k)
        spread.wait_sent(p.ep(k))
    slot_move.wait_sent()
    gate_move.wait_sent()
    message_move.wait_sent()


def homeward_kernel(
    n_ep, n_tp, hidden, down_weight, heads, ret, heads_all,
    partial, down_held, pair, mine, out_y, in_y, final,
    w, h0, h1, a0, a1, r0, r1, q0, q1, ys, yr, ps, pr,
):
    p = Place(n_ep, n_tp)
    ny = p.ny
    width = ret.shape[2]

    def cols(t):
        return pl.ds(pl.multiple_of(t * width, width), width)

    def land(t, s):
        return heads_all.at[t, s]

    load = pltpu.make_async_copy(down_weight, down_held, w.at[0])
    load.start()
    p.barrier()
    head_move = Exchange(p, lambda d: heads.at[d], lambda s: land(p.t, s), (h0, h1))
    spread = Spread(p, land, (ys, yr, ps, pr))
    head_move.start()

    def pair_copy(s, off):
        src = partial.at[s, :, cols(p.y_at(off) * 2 + (1 - p.c))]
        return remote(src, pair.at[s, off], r0.at[s, off], r1.at[s, off], p.e, p.partner)

    def y_copy(s, off, to):
        return remote(
            out_y.at[s, off - 1], in_y.at[s, off - 1],
            q0.at[s, off - 1], q1.at[s, off - 1], p.e, p.chip(to),
        )

    def final_copy(k):
        d = p.ep(k)
        return remote(final.at[d], ret.at[p.e], a0.at[d], a1.at[p.e], d, p.t)

    order = list(range(1, n_ep)) + [0]
    capacity = ret.shape[1]

    def multiply(t):
        product = jnp.dot(
            hidden[...], down_held[:, cols(t)], preferred_element_type=jnp.float32
        )
        partial[:, :, cols(t)] = product.astype(jnp.bfloat16).reshape(n_ep, capacity, width)

    load.wait()
    turns = [*range(1, ny), 0]
    for off in turns:
        multiply(p.y_at(off) * 2 + (1 - p.c))
        multiply(p.chip(off))
        for k in order:
            pair_copy(p.ep(k), off).start()
        for k in order:
            s = p.ep(k)
            pair_copy(s, off).wait_recv()
            both = partial[s, :, cols(p.chip(off))].astype(jnp.float32) + pair[s, off].astype(
                jnp.float32
            )
            if off == 0:
                mine[s] = both
            else:
                out_y[s, off - 1] = both.astype(jnp.bfloat16)
                y_copy(s, off, off).start()
    for k in range(n_ep):
        head_move.wait_arrival(k)
        spread.first(p.ep(k))
    for k in order:
        s = p.ep(k)
        total = mine[s]
        for off in range(1, ny):
            y_copy(s, off, -off).wait_recv()
            total = total + in_y[s, off - 1].astype(jnp.float32)
        if k == 0:
            ret[s] = total.astype(jnp.bfloat16)
        else:
            final[s] = total.astype(jnp.bfloat16)
            final_copy(k).start()
    for k in range(n_ep):
        spread.relay(p.ep(k))
    for k in range(n_ep):
        spread.finish(p.ep(k))
    for k in range(n_ep):
        s = p.ep(k)
        for off in range(ny):
            pair_copy(s, off).wait_send()
        for off in range(1, ny):
            y_copy(s, off, off).wait_send()
    for k in range(1, n_ep):
        s = p.ep(k)
        remote(final.at[s], ret.at[s], a0.at[s], a1.at[s], s, p.t).wait_recv()
        final_copy(k).wait_send()
    head_move.wait_sent()


def outward(slots, message, gates, gate_weight, up_weight, n_ep, n_tp):
    _, capacity, width = slots.shape
    rows, units = n_ep * capacity, gate_weight.shape[0]
    scratch = [
        pltpu.VMEM((n_ep, capacity, width * n_tp), slots.dtype),
        pltpu.VMEM(gate_weight.shape, gate_weight.dtype),
        pltpu.VMEM(up_weight.shape, up_weight.dtype),
        pltpu.VMEM((rows, units), jnp.float32),
        pltpu.VMEM((rows, units), jnp.float32),
    ]
    sems = [DMA((n_ep,))] * 6 + [DMA((2,))] + spread_sems(n_ep, n_tp)
    return pl.pallas_call(
        functools.partial(outward_kernel, n_ep, n_tp),
        out_shape=[
            jax.ShapeDtypeStruct((rows, units), slots.dtype),
            jax.ShapeDtypeStruct(message.shape, message.dtype),
            jax.ShapeDtypeStruct(gates.shape, gates.dtype),
        ],
        in_specs=[VM] * 3 + [ANY] * 2,
        out_specs=[VM] * 3,
        scratch_shapes=scratch + sems,
        compiler_params=pltpu.CompilerParams(collective_id=0, has_side_effects=True),
        name="outward",
    )(slots, message, gates, gate_weight, up_weight)


def homeward(hidden, down_weight, heads, n_ep, n_tp):
    capacity, features = hidden.shape[0] // n_ep, down_weight.shape[1]
    width, ny = features // n_tp, n_tp // 2
    far = max(ny - 1, 1)
    scratch = [
        pltpu.VMEM((n_ep, capacity, features), jnp.bfloat16),
        pltpu.VMEM(down_weight.shape, down_weight.dtype),
        pltpu.VMEM((n_ep, ny, capacity, width), jnp.bfloat16),
        pltpu.VMEM((n_ep, capacity, width), jnp.float32),
        pltpu.VMEM((n_ep, far, capacity, width), jnp.bfloat16),
        pltpu.VMEM((n_ep, far, capacity, width), jnp.bfloat16),
        pltpu.VMEM((n_ep, capacity, width), jnp.bfloat16),
    ]
    sems = [DMA((1,))] + [DMA((n_ep,))] * 4 + [DMA((n_ep, ny))] * 2 + [DMA((n_ep, far))] * 2
    return pl.pallas_call(
        functools.partial(homeward_kernel, n_ep, n_tp),
        out_shape=[
            jax.ShapeDtypeStruct((n_ep, capacity, width), jnp.bfloat16),
            jax.ShapeDtypeStruct((n_tp,) + heads.shape, jnp.bfloat16),
        ],
        in_specs=[VM, ANY, VM],
        out_specs=[VM] * 2,
        scratch_shapes=scratch + sems + spread_sems(n_ep, n_tp),
        compiler_params=pltpu.CompilerParams(collective_id=1, has_side_effects=True),
        name="homeward",
    )(hidden, down_weight, heads)


def on_device(
    mixer_tokens,
    mixer_gain,
    query_weight,
    key_weight,
    value_weight,
    forget_weight,
    forget_bias,
    output_weight,
    expert_tokens,
    expert_gain,
    routes,
    route_weights,
    gate_weight,
    up_weight,
    down_weight,
):
    n_ep, n_tp = lax.axis_size("ep"), lax.axis_size("tp")
    rows, features = mixer_tokens.shape
    local_heads = forget_weight.shape[1]
    share = n_ep // local_heads
    part = rows // share
    width = features // n_tp
    bf16, f32 = jnp.bfloat16, jnp.float32

    expert_normed = normed_rows(expert_tokens, expert_gain)
    token_count, top_count = routes.shape
    capacity = 2 * top_count * token_count // n_ep
    pairs = token_count * top_count
    flat_routes = routes.reshape(-1)
    onehot = flat_routes[:, None] == jnp.arange(n_ep, dtype=jnp.int32)[None, :]
    before = jnp.tril(jnp.ones((pairs, pairs), bf16), -1)
    ranks = jnp.dot(before, onehot.astype(bf16), preferred_element_type=f32)
    slot_rank = jnp.sum(jnp.where(onehot, ranks, 0.0), axis=1).astype(jnp.int32)
    slot_index = (flat_routes * capacity + slot_rank).reshape(token_count, top_count)
    slot_ids = jnp.arange(n_ep * capacity, dtype=jnp.int32)
    picks = [(slot_index[:, j][:, None] == slot_ids[None, :]).astype(bf16) for j in range(top_count)]
    column = lax.axis_index("tp") * width
    own_columns = lax.dynamic_slice_in_dim(expert_normed, column, width, 1)
    slots = lax.dot_general(
        sum(picks[1:], picks[0]), own_columns, (((0,), (0,)), ((), ())),
        preferred_element_type=f32,
    ).astype(bf16).reshape(n_ep, capacity, width)

    normed = normed_rows(mixer_tokens, mixer_gain)
    queries = by_rows(normed, query_weight).astype(bf16)
    key_rows = by_rows(normed, key_weight).astype(bf16)
    value_rows = by_rows(normed, value_weight).astype(bf16)
    pre_gate = jnp.dot(normed, forget_weight, preferred_element_type=f32) + forget_bias
    block_cum = jnp.dot(
        jnp.tril(jnp.ones((rows, rows), f32)), jax.nn.log_sigmoid(pre_gate),
        precision=lax.Precision.HIGHEST, preferred_element_type=f32,
    )
    key_value = jnp.concatenate(
        [
            key_rows.reshape(rows, local_heads, HD).transpose(1, 0, 2),
            value_rows.reshape(rows, local_heads, HD).transpose(1, 0, 2),
        ],
        axis=2,
    )
    key_value = jnp.broadcast_to(
        key_value[:, None], (local_heads, share, rows, 2 * HD)
    ).reshape(n_ep, rows, 2 * HD)
    half = part // 2
    query_parts = queries.reshape(share, 2, half, local_heads, HD).transpose(3, 0, 2, 1, 4)
    query_parts = query_parts.reshape(n_ep, half, 2 * HD)
    message = jnp.concatenate([key_value, query_parts], axis=1)
    gates = jnp.broadcast_to(block_cum.T[:, None, None, :], (local_heads, share, 1, rows))
    gates = gates.reshape(n_ep, 1, rows)

    hidden, all_messages, all_gates = outward(
        slots, message, gates, gate_weight[0], up_weight[0], n_ep, n_tp
    )

    positions = n_ep * rows
    all_gates = all_gates.reshape(n_ep, rows)
    totals = all_gates[:, rows - 1]
    lower = jnp.arange(n_ep)[None, :] < jnp.arange(n_ep)[:, None]
    base = jnp.sum(jnp.where(lower, totals[None, :], 0.0), axis=1)
    cumulative = all_gates + base[:, None]
    keys = all_messages[:, :rows, :HD].reshape(positions, HD)
    values = all_messages[:, :rows, HD:].reshape(positions, HD)
    head_query = all_messages[:, rows:].reshape(n_ep, half, 2, HD).transpose(0, 2, 1, 3)
    head_query = head_query.reshape(n_ep * part, HD)
    first = (lax.axis_index("ep") % share) * part
    query_cum = lax.dynamic_slice_in_dim(cumulative, first, part, 1).reshape(-1)
    query_pos = (
        jnp.arange(n_ep, dtype=jnp.int32)[:, None] * rows
        + first
        + jnp.arange(part, dtype=jnp.int32)[None, :]
    ).reshape(-1)
    key_pos = jnp.arange(positions, dtype=jnp.int32)
    scores = by_rows(head_query, keys) * HD ** (-0.5)
    scores = scores + query_cum[:, None] - cumulative.reshape(-1)[None, :]
    scores = jnp.where(key_pos[None, :] <= query_pos[:, None], scores, -jnp.inf)
    weights = jnp.exp(scores - jnp.max(scores, axis=-1, keepdims=True)).astype(bf16)
    attended = jnp.dot(weights, values, preferred_element_type=f32)
    rescale = lax.rsqrt(jnp.mean(attended * attended, axis=-1, keepdims=True) + HEAD_FLOOR)
    head_out = (attended * rescale).astype(bf16).reshape(n_ep, part, HD)

    returned, heads_all = homeward(hidden, down_weight[0], head_out, n_ep, n_tp)

    heads_all = heads_all.reshape(n_tp, local_heads, share, part, HD).transpose(2, 3, 0, 1, 4)
    heads_all = heads_all.reshape(rows, n_tp * local_heads * HD)
    mixer_output = jnp.dot(heads_all, output_weight, preferred_element_type=f32).astype(bf16)
    returned = returned.reshape(n_ep * capacity, width)
    expert_output = 0.0
    for j in range(top_count):
        picked = jnp.dot(picks[j], returned, preferred_element_type=f32)
        expert_output = expert_output + picked * route_weights[:, j][:, None]
    return (mixer_output, expert_output.astype(bf16))


def lanes_of(shape, dim):
    return lax.broadcasted_iota(jnp.int32, shape, dim)


class Relay:
    def __init__(self, place, land, sems, batch):
        self.p, self.land, self.batch = place, land, batch
        self.ys, self.yr, self.ps, self.pr = sems

    def y_copy(self, off, s, t, to):
        block = self.land(t, s)
        return remote(block, block, self.ys.at[0], self.yr.at[off - 1, s], self.p.e, to)

    def p_copy(self, off, s, t):
        block, p = self.land(t, s), self.p
        return remote(block, block, self.ps.at[0], self.pr.at[self.batch(s)], p.e, p.partner)

    def first(self, s):
        p = self.p
        for off in range(1, p.ny):
            self.y_copy(off, s, p.t, p.chip(off)).start()
        self.p_copy(0, s, p.t).start()

    def relay(self, s):
        p = self.p
        for off in range(1, p.ny):
            self.y_copy(off, s, p.chip(-off), p.chip(-off)).wait_recv()
            self.p_copy(off, s, p.chip(-off)).start()

    def settle(self, batch, blocks):
        p = self.p
        remote(blocks, blocks, self.ps.at[0], self.pr.at[batch], p.e, p.partner).wait_recv()

    def sent(self, y_blocks, p_blocks):
        p = self.p
        remote(y_blocks, y_blocks, self.ys.at[0], self.yr.at[0, 0], p.e, p.partner).wait_send()
        remote(p_blocks, p_blocks, self.ps.at[0], self.pr.at[0], p.e, p.partner).wait_send()


def flipped(place, bits):
    at, weight = place, 1
    while bits:
        if bits % 2:
            at = at + weight * (1 - 2 * (place // weight % 2))
        bits, weight = bits // 2, weight * 2
    return at


def fused_kernel(
    n_ep, n_tp,
    tokens_a, gain_a, w_q, w_k, w_v, w_f, b_f, w_o, tokens_b, gain_b, routes, route_w,
    w_gate, w_up, w_down,
    out_a, out_b,
    a_held, ga_held, q_held, kv_held, f_held, bf_held, o_held, b_held, gb_held, r_held, rw_held,
    gate_held, up_held, down_held,
    slots, slots_more, land, w_hi, w_lo, kv_send, q_send, g_send, kv_land, q_land, g_land,
    hidden, pair_send, pair_land, own_part, mine, y_send, y_land, final, ret,
    q_all, q_cum, scores, running, row_max, attended, head_send, heads_all, lhs, mixed,
    lsem, s0, s1, m0, m1, ys, yr, ps, pr, k0, k1, x0, x1, q0, q1, g0, g1,
    p0, p1, z0, z1, a0, a1, h0, h1, hy0, hy1, hp0, hp1,
):
    p = Place(n_ep, n_tp)
    ny = p.ny
    bf16, f32 = jnp.bfloat16, jnp.float32
    rows, features = a_held.shape
    tokens = b_held.shape[0]
    _, capacity, width = slots.shape
    local_heads = kv_send.shape[0]
    share = n_ep // local_heads
    part = rows // share
    half = part // 2
    units = gate_held.shape[0]
    eighth = n_ep // 8
    order = [0, 1, 2, 6, 7, 3, 4, 5]

    def places(*eighths):
        return [order.index(k) * eighth + i for k in eighths for i in range(eighth)]

    own, second, third = places(0), places(6, 7), places(4, 5)
    near = [*own[1:], *places(1, 2, 3)]
    groups = [range(eighth), range(eighth, 5 * eighth), range(5 * eighth, n_ep)]
    early_near, late_near = places(1, 2), places(3)
    own_share = p.e % share
    first = own_share * part

    def cols(t):
        return pl.ds(pl.multiple_of(t * width, width), width)

    def peer(j):
        return flipped(p.e, order[j // eighth] * eighth + j % eighth)

    barrier = pltpu.get_barrier_semaphore()
    for k in range(1, n_ep):
        pl.semaphore_signal(
            barrier, inc=1, device_id={"ep": p.ep(k), "tp": p.t}, device_id_type=MESH
        )
    for off in range(1, ny):
        pl.semaphore_signal(
            barrier, inc=1, device_id={"ep": p.e, "tp": p.chip(off)}, device_id_type=MESH
        )
    pl.semaphore_signal(
        barrier, inc=1, device_id={"ep": p.e, "tp": p.partner}, device_id_type=MESH
    )

    early = [(tokens_b, b_held), (routes, r_held), (gain_b, gb_held)]
    middle = [(tokens_a, a_held), (gain_a, ga_held), (w_f, f_held), (b_f, bf_held), (w_q, q_held)]
    late = [
        (w_gate, gate_held), (w_up, up_held), (w_down, down_held), (route_w, rw_held),
        (w_o, o_held),
    ]
    loads, number = [], 0
    for batch in (early, middle, late):
        made = []
        for src, dst in batch:
            made.append(pltpu.make_async_copy(src, dst, lsem.at[number]))
            number += 1
        loads.append(made)
    pieces = []
    for h in range(local_heads):
        mine_rows = pl.ds(h * HD, HD)
        for at, src in ((2 * h, w_k), (2 * h + 1, w_v)):
            there = kv_held.at[pl.ds(at * HD, HD)]
            pieces.append(pltpu.make_async_copy(src.at[mine_rows], there, lsem.at[number]))
    all_pieces = pltpu.make_async_copy(kv_held, kv_held, lsem.at[number])
    early, middle, late = loads
    for load in early + middle + pieces:
        load.start()

    for load in early:
        load.wait()
    values = b_held[...].astype(f32)
    square = jnp.mean(values * values, axis=-1, keepdims=True)
    scale = lax.rsqrt(jnp.maximum(square, MEAN_FLOOR))
    b_held[...] = (values * scale * gb_held[...]).astype(bf16)
    named_by = r_held[...]
    top_count = named_by.shape[0]
    place = lanes_of((n_ep, tokens), 0)
    moved = [jnp.where(place // eighth == k, order[k] - k, 0) for k in range(8)]
    place = place + sum(moved[1:], moved[0]) * eighth
    expert_at, weight = place, 1
    while weight < n_ep:
        flip = (p.e // weight) % 2
        expert_at = expert_at + flip * weight * (1 - 2 * ((place // weight) % 2))
        weight *= 2
    chosen = [named_by[c : c + 1, :] == expert_at for c in range(top_count)]
    named = sum([c.astype(f32) for c in chosen[1:]], chosen[0].astype(f32))
    earlier = (lanes_of((tokens, tokens), 0) < lanes_of((tokens, tokens), 1)).astype(bf16)
    ranks = jnp.dot(named.astype(bf16), earlier, preferred_element_type=f32)
    ranks = jnp.where(named > 0, ranks, -1.0).astype(jnp.int32)
    slot_at = lanes_of((capacity, tokens), 0)
    picks = [ranks[j : j + 1, :] == slot_at for j in range(n_ep)]
    picks = [pick.astype(f32).astype(bf16) for pick in picks]

    def picked(j, lanes):
        return jnp.dot(picks[j], b_held[:, lanes], preferred_element_type=f32).astype(bf16)

    for j in range(1, n_ep):
        slots[j] = picked(j, cols(p.t))
    for j in near:
        for off in range(1, ny):
            slots_more[near.index(j), off - 1] = picked(j, cols(p.chip(-off)))
    pl.semaphore_wait(barrier, n_ep - 1 + ny - 1 + 1)

    def slot_copy(j):
        return remote(
            slots.at[j], land.at[j, :, cols(p.t)], s0.at[0], s1.at[j], peer(j), p.t
        )

    def more_copy(j, off):
        return remote(
            slots_more.at[near.index(j), off - 1], land.at[j, :, cols(p.chip(-off))],
            m0.at[0], m1.at[near.index(j), off - 1], peer(j), p.t,
        )

    def send(j):
        slot_copy(j).start()
        if j in near:
            for off in range(1, ny):
                more_copy(j, off).start()

    spread = Relay(
        p,
        lambda t, j: land.at[j, :, cols(t)],
        (ys, yr, ps, pr),
        lambda j: [j in group for group in groups].index(True),
    )
    for j in [*own[1:], *places(1), *second, *places(2, 3), *third]:
        send(j)
    land[0] = picked(0, slice(None))

    for load in middle + [all_pieces]:
        load.wait()
    for load in late:
        load.start()
    values = a_held[...].astype(f32)
    square = jnp.mean(values * values, axis=-1, keepdims=True)
    scale = lax.rsqrt(jnp.maximum(square, MEAN_FLOOR))
    a_held[...] = (values * scale * ga_held[...]).astype(bf16)
    normed = a_held[...]
    eye = lanes_of((local_heads, local_heads), 0) == lanes_of((local_heads, local_heads), 1)
    bias = jnp.sum(jnp.where(eye, bf_held[...], 0.0), axis=1, keepdims=True)
    gate = by_rows(f_held[...], normed) + bias
    log_gate = jnp.minimum(gate, 0.0) - jnp.log1p(jnp.exp(-jnp.abs(gate)))
    upto = (lanes_of((rows, rows), 0) <= lanes_of((rows, rows), 1)).astype(f32)
    block_cum = jnp.dot(
        log_gate, upto, precision=lax.Precision.HIGHEST, preferred_element_type=f32
    )
    for h in range(local_heads):
        g_send[h] = block_cum[h : h + 1, :]

    def kv_copy(h):
        to = h * share + own_share
        return remote(kv_send.at[h], kv_land.at[p.e], k0.at[0], k1.at[p.e // share], to, p.t)

    def kv_arrival(n):
        s = (p.e // share + n) % local_heads * share + own_share
        return remote(kv_send.at[0], kv_land.at[s], k0.at[0], k1.at[s // share], p.e, p.t), s

    def sibling(off):
        return p.e // share * share + (own_share + off) % share

    def kv_relay(s, off):
        return remote(
            kv_land.at[s], kv_land.at[s], x0.at[0], x1.at[0], sibling(off), p.t
        )

    def q_copy(k):
        d = p.ep(k)
        return remote(q_send.at[d], q_land.at[p.e], q0.at[0], q1.at[0], d, p.t)

    def g_copy(k):
        d = p.ep(k)
        return remote(g_send.at[d // share], g_land.at[p.e], g0.at[0], g1.at[0], d, p.t)

    def others(ref):
        return ref.at[pl.ds(0, n_ep - 1)]

    def batch_of(ref, send, recv):
        return remote(ref, ref, send.at[0], recv.at[0], p.e, p.partner)

    key_value = by_rows(normed, kv_held[...]).astype(bf16)
    for h in range(local_heads):
        kv_send[h] = key_value[:, 2 * h * HD : 2 * (h + 1) * HD]
    for n in range(1, local_heads):
        kv_copy((p.e // share + n) % local_heads).start()
    own_head = p.e // share
    kv_land[p.e] = kv_send[own_head]
    for off in range(1, share):
        kv_relay(p.e, off).start()
    queries = by_rows(normed, q_held[...]) * HD ** (-0.5)
    left = lanes_of((half, 2 * HD), 1) < HD
    for pair in range(local_heads // 2):
        there = queries[:, 2 * pair * HD : 2 * (pair + 1) * HD]
        moved = pltpu.roll(there, HD, 1)
        for x in range(share):
            top, bottom = slice(x * part, x * part + half), slice(x * part + half, (x + 1) * part)
            q_send[2 * pair * share + x] = jnp.where(left, there[top], moved[bottom]).astype(bf16)
            q_send[(2 * pair + 1) * share + x] = jnp.where(
                left, moved[top], there[bottom]
            ).astype(bf16)
    for k in range(1, n_ep):
        q_copy(k).start()
        g_copy(k).start()
    q_land[p.e] = q_send[p.e]
    g_land[p.e] = g_send[own_head]

    def arrive(j):
        slot_copy(j).wait_recv()
        if j in near:
            spread.p_copy(0, j, p.t).start()
            for off in range(1, ny):
                more_copy(j, off).wait_recv()
                spread.p_copy(off, j, p.chip(-off)).start()
        else:
            spread.first(j)

    def complete(j):
        spread.relay(j)

    def settle(g):
        count = len(groups[g]) - (0 in groups[g])
        spread.settle(g, land.at[pl.ds(0, count), :, pl.ds(0, ny * width)])

    cuts = [(at, min(at + 512, units)) for at in range(0, units, 512)]

    def serve(beside, number, count):
        for act, *given in beside[len(beside) * number // count : len(beside) * (number + 1) // count]:
            act(*given)

    def open_up(g, beside):
        low_row, count = groups[g][0], len(groups[g])
        block = land[low_row : low_row + count].reshape(count * capacity, features)
        lines = slice(low_row * capacity, (low_row + count) * capacity)
        for number, (low, high) in enumerate(cuts):
            gated = by_rows(gate_held[low:high], block)
            upped = by_rows(up_held[low:high], block)
            hidden[lines, low:high] = (gated * lax.logistic(gated) * upped).astype(bf16).T
            serve(beside, number, len(cuts))

    def pair_copy(g, off):
        low_row, count = groups[g][0], len(groups[g])
        lines = pl.ds(low_row * capacity, count * capacity)
        return remote(
            pair_send.at[off, lines], pair_land.at[off, lines], p0.at[0], p1.at[g, off],
            p.e, p.partner,
        )

    def y_copy(j, off, to):
        return remote(
            y_send.at[j, off - 1], y_land.at[j, off - 1],
            z0.at[0], z1.at[j, off - 1], p.e, p.chip(to),
        )

    turns = [*range(1, ny), 0]

    def close_down(g, beside, held=()):
        low_row, count = groups[g][0], len(groups[g])
        lines = slice(low_row * capacity, (low_row + count) * capacity)

        def product(t):
            return jnp.dot(hidden[lines], down_held[:, cols(t)], preferred_element_type=f32)

        for number, off in enumerate(turns):
            pair_send[off, lines] = product(p.y_at(off) * 2 + (1 - p.c)).astype(bf16)
            pair_copy(g, off).start()
            serve(beside, number, 2 * ny)
        for number, off in enumerate(turns):
            own_part[lines] = product(p.chip(off))
            serve(beside, ny + number, 2 * ny)
            pair_copy(g, off).wait_recv()
            both = own_part[lines] + pair_land[off, lines].astype(f32)
            both = both.reshape(count, capacity, width)
            for m in range(count):
                j = low_row + m
                if off == 0:
                    mine[j] = both[m]
                else:
                    y_send[j, off - 1] = both[m].astype(bf16)
                    if j not in held:
                        y_copy(j, off, off).start()

    def final_copy(j):
        return remote(final.at[j], ret.at[j], a0.at[0], a1.at[0], peer(j), p.t)

    def finish(j):
        total = mine[j]
        for off in range(1, ny):
            y_copy(j, off, -off).wait_recv()
            total = total + y_land[j, off - 1].astype(f32)
        if j == 0:
            ret[0] = total.astype(bf16)
        else:
            final[j] = total.astype(bf16)
            final_copy(j).start()

    def kv_forward(n):
        copy, s = kv_arrival(n)
        copy.wait_recv()
        for off in range(1, share):
            kv_relay(s, off).start()

    for j in own[1:]:
        arrive(j)
    if own[1:]:
        settle(0)
    late[0].wait()
    late[1].wait()
    open_up(0, [(arrive, j) for j in places(1)])
    late[2].wait()
    close_down(0, [(arrive, j) for j in second], own)
    for j in places(2):
        arrive(j)
    for j in second:
        complete(j)
    settle(1)
    open_up(1, [(arrive, j) for j in [*third, *late_near]])
    close_down(1, [], near)
    for j in early_near:
        for off in range(1, ny):
            y_copy(j, off, off).start()
    complete(third[0])
    for n in range(1, local_heads):
        kv_forward(n)
    for j in third[1:]:
        complete(j)
    settle(2)
    open_up(2, [(finish, j) for j in second])
    close_down(2, [], near)
    behind = [*late_near, *own]
    for j in behind:
        for off in range(1, ny):
            y_copy(j, off, off).start()

    late[3].wait()
    for j in range(n_ep):
        weight = 0.0
        for c in range(top_count):
            weight = weight + jnp.where(
                named_by[c : c + 1, :] == peer(j), rw_held[c : c + 1, :], 0.0
            )
        weight = jnp.where(ranks[j : j + 1, :] == slot_at, weight, 0.0)
        high = weight.astype(bf16)
        w_hi[j * capacity : (j + 1) * capacity] = high
        w_lo[j * capacity : (j + 1) * capacity] = (weight - high.astype(f32)).astype(bf16)

    batch_of(others(g_land), g0, g1).wait_recv()
    batch_of(others(q_land), q0, q1).wait_recv()
    relayed = kv_land.at[pl.ds(0, local_heads * (share - 1))]
    batch_of(relayed, x0, x1).wait_recv()
    positions = lanes_of((part, rows), 1)
    asked = first + lanes_of((part, rows), 0)
    base = jnp.zeros((1, 1), f32)
    key_cum = []
    last = lanes_of((1, rows), 1) == rows - 1
    for b in range(n_ep):
        block = g_land[b]
        key_cum.append(block + base)
        base = base + jnp.sum(jnp.where(last, block, 0.0), axis=1, keepdims=True)
        at = b * part
        q_cum[at : at + part] = jnp.sum(
            jnp.where(positions == asked, key_cum[b], 0.0), axis=1, keepdims=True
        )
        packed = q_land[b].astype(f32)
        q_all[at : at + half] = jnp.where(left, packed, 0.0).astype(bf16)
        q_all[at + half : at + part] = jnp.where(
            left, pltpu.roll(packed, HD, 1), 0.0
        ).astype(bf16)
    for b in range(n_ep):
        at = b * part
        block = by_rows(q_all[at:], kv_land[b]) + q_cum[at:] - key_cum[b]
        seen = jnp.where(positions <= asked, block[:part], -jnp.inf)
        scores[b, at : at + part] = seen
        if b == 0:
            running[:part] = seen
            running[part:] = block[part:]
        else:
            running[at : at + part] = jnp.maximum(running[at : at + part], seen)
        if b + 1 < n_ep:
            scores[b, at + part :] = block[part:]
            if b > 0:
                running[at + part :] = jnp.maximum(running[at + part :], block[part:])
    row_max[...] = jnp.max(running[...], axis=1, keepdims=True)
    for b in range(n_ep):
        at = b * part
        weights = jnp.exp(scores[b, at:] - row_max[at:]).astype(bf16)
        product = jnp.dot(weights, kv_land[b], preferred_element_type=f32)
        if b == 0:
            attended[...] = product
        else:
            attended[at:] = attended[at:] + product
    right = lanes_of((part, 2 * HD), 1) >= HD
    for b in range(n_ep):
        block = jnp.where(right, attended[b * part : (b + 1) * part], 0.0)
        block = block * lax.rsqrt(
            jnp.sum(block * block, axis=1, keepdims=True) * (1.0 / HD) + HEAD_FLOOR
        )
        moved = pltpu.roll(block, HD, 1)
        head_send[b] = jnp.where(left, moved[:half], block[half:]).astype(bf16)

    def head_copy(k):
        d = peer(k)
        return remote(head_send.at[d], heads_all.at[p.t, p.e], h0.at[0], h1.at[p.e], d, p.t)

    def head_arrival(k):
        s = peer(k)
        return remote(head_send.at[s], heads_all.at[p.t, s], h0.at[0], h1.at[s], s, p.t)

    for k in [*second, *third, *near]:
        head_copy(k).start()
    heads_all[p.t, p.e] = head_send[p.e]

    for j in early_near:
        finish(j)
    for j in third:
        finish(j)

    gather = Relay(p, lambda t, s: heads_all.at[t, s], (hy0, hy1, hp0, hp1), lambda s: 0)
    gather.first(p.e)
    for k in near:
        head_arrival(k).wait_recv()
        gather.first(peer(k))
    for j in behind:
        finish(j)
    for k in [*second, *third]:
        head_arrival(k).wait_recv()
        gather.first(peer(k))
    for k in range(n_ep):
        gather.relay(peer(k))
    late[4].wait()

    def project(t):
        for pair in range(local_heads // 2):
            lanes = slice(2 * pair * HD, 2 * (pair + 1) * HD)
            for x in range(share):
                one = heads_all[t, 2 * pair * share + x].astype(f32)
                two = heads_all[t, (2 * pair + 1) * share + x].astype(f32)
                at = x * part
                lhs[at : at + half, lanes] = jnp.where(
                    left, one, pltpu.roll(two, HD, 1)
                ).astype(bf16)
                lhs[at + half : at + part, lanes] = jnp.where(
                    left, pltpu.roll(one, HD, 1), two
                ).astype(bf16)
        deep = local_heads * HD
        here = o_held[pl.ds(pl.multiple_of(t * deep, deep), deep), :]
        return jnp.dot(lhs[...], here, preferred_element_type=f32)

    mixed[...] = project(p.t)
    for off in range(1, ny):
        mixed[...] = mixed[...] + project(p.chip(-off))
    gather.settle(0, heads_all.at[pl.ds(0, ny)])
    for off in range(ny - 1):
        mixed[...] = mixed[...] + project(p.y_at(-off) * 2 + (1 - p.c))
    last_part = project(p.y_at(-(ny - 1)) * 2 + (1 - p.c))
    out_a[...] = (mixed[...] + last_part).astype(bf16)

    batch_of(others(ret), a0, a1).wait_recv()
    returned = ret[...].reshape(n_ep * capacity, width)
    over_slots = (((0,), (0,)), ((), ()))
    total = lax.dot_general(w_hi[...], returned, over_slots, preferred_element_type=f32)
    total = total + lax.dot_general(w_lo[...], returned, over_slots, preferred_element_type=f32)
    out_b[...] = total.astype(bf16)

    spread.sent(
        land.at[pl.ds(0, len(second) + len(third)), :, pl.ds(0, (ny - 1) * width)],
        land.at[pl.ds(0, n_ep - 1), :, pl.ds(0, ny * width)],
    )
    gather.sent(heads_all.at[pl.ds(0, ny - 1)], heads_all.at[pl.ds(0, ny)])
    for ref, send, recv in (
        (others(slots), s0, s1), (slots_more, m0, s1), (others(q_send), q0, q1), (others(final), a0, a1),
        (others(head_send), h0, h1), (pair_send, p0, a1), (y_send, z0, a1),
        (others(g_land), g0, g1), (kv_send.at[pl.ds(0, local_heads - 1)], k0, k1),
        (relayed, x0, x1),
    ):
        batch_of(ref, send, recv).wait_send()


def fused_on_device(
    mixer_tokens, mixer_gain, query_weight, key_weight, value_weight, forget_weight,
    forget_bias, output_weight, expert_tokens, expert_gain, routes, route_weights,
    gate_weight, up_weight, down_weight,
):
    n_ep, n_tp = lax.axis_size("ep"), lax.axis_size("tp")
    ny = n_tp // 2
    far = max(ny - 1, 1)
    rows, features = mixer_tokens.shape
    tokens, top_count = routes.shape
    local_heads = forget_weight.shape[1]
    share = n_ep // local_heads
    part = rows // share
    half = part // 2
    width = features // n_tp
    capacity = 2 * top_count * tokens // n_ep
    units = gate_weight.shape[1]
    groups = 3
    asked = n_ep * part
    bf16, f32 = jnp.bfloat16, jnp.float32
    operands = [
        mixer_tokens, mixer_gain.reshape(1, features), query_weight, key_weight, value_weight,
        forget_weight.T, forget_bias, output_weight, expert_tokens,
        expert_gain.reshape(1, features), routes.T, route_weights.T,
        gate_weight[0], up_weight[0], down_weight[0],
    ]
    operands = [pltpu.with_memory_space_constraint(x, pltpu.HBM) for x in operands]
    vmem = pltpu.VMEM
    scratch = [
        vmem((rows, features), bf16), vmem((1, features), f32),
        vmem(query_weight.shape, bf16), vmem((2 * local_heads * HD, features), bf16),
        vmem((local_heads, features), bf16), vmem((1, local_heads), f32),
        vmem(output_weight.shape, bf16), vmem((tokens, features), bf16),
        vmem((1, features), f32), vmem((top_count, tokens), jnp.int32),
        vmem((top_count, tokens), f32),
        vmem((units, features), bf16), vmem((units, features), bf16),
        vmem((units, features), bf16),
        vmem((n_ep, capacity, width), bf16), vmem((n_ep // 2 - 1, far, capacity, width), bf16),
        vmem((n_ep, capacity, features), bf16),
        vmem((n_ep * capacity, tokens), bf16), vmem((n_ep * capacity, tokens), bf16),
        vmem((local_heads, rows, 2 * HD), bf16), vmem((n_ep, half, 2 * HD), bf16),
        vmem((local_heads, 1, rows), f32),
        vmem((n_ep, rows, 2 * HD), bf16), vmem((n_ep, half, 2 * HD), bf16),
        vmem((n_ep, 1, rows), f32),
        vmem((n_ep * capacity, units), bf16),
        vmem((ny, n_ep * capacity, width), bf16),
        vmem((ny, n_ep * capacity, width), bf16),
        vmem((n_ep * capacity, width), f32),
        vmem((n_ep, capacity, width), f32),
        vmem((n_ep, far, capacity, width), bf16), vmem((n_ep, far, capacity, width), bf16),
        vmem((n_ep, capacity, width), bf16), vmem((n_ep, capacity, width), bf16),
        vmem((asked, 2 * HD), bf16), vmem((asked, 1), f32),
        vmem((n_ep, asked, rows), f32), vmem((asked, rows), f32), vmem((asked, 1), f32),
        vmem((asked, 2 * HD), f32), vmem((n_ep, half, 2 * HD), bf16),
        vmem((n_tp, n_ep, half, 2 * HD), bf16), vmem((rows, local_heads * HD), bf16), vmem((rows, width), f32),
    ]
    one = DMA((1,))
    sems = [DMA((14,)), one, DMA((n_ep,)), one, DMA((n_ep // 2 - 1, far)), one, DMA((far, n_ep)), one, DMA((groups,))]
    sems += [one, DMA((local_heads,))] + [one] * 6
    sems += [one, DMA((groups, ny)), one, DMA((n_ep, far)), one, one, one, DMA((n_ep,))]
    sems += [one, DMA((far, n_ep)), one, one]
    return pl.pallas_call(
        functools.partial(fused_kernel, n_ep, n_tp),
        out_shape=[
            jax.ShapeDtypeStruct((rows, width), bf16),
            jax.ShapeDtypeStruct((tokens, width), bf16),
        ],
        in_specs=[ANY] * len(operands),
        out_specs=[VM] * 2,
        scratch_shapes=scratch + sems,
        compiler_params=pltpu.CompilerParams(
            collective_id=2, has_side_effects=True, vmem_limit_bytes=LIMIT
        ),
        name="fused",
    )(*operands)


def deliver_kernel(one, two, one_out, two_out, sem):
    copies = [
        pltpu.make_async_copy(one, one_out, sem.at[0]),
        pltpu.make_async_copy(two, two_out, sem.at[1]),
    ]
    for copy in copies:
        copy.start()
    for copy in copies:
        copy.wait()


def deliver(one, two):
    return pl.pallas_call(
        deliver_kernel,
        out_shape=[
            jax.ShapeDtypeStruct(one.shape, one.dtype),
            jax.ShapeDtypeStruct(two.shape, two.dtype),
        ],
        in_specs=[ANY] * 2,
        out_specs=[ANY] * 2,
        scratch_shapes=[DMA((2,))],
        compiler_params=pltpu.CompilerParams(vmem_limit_bytes=1 << 20),
        name="deliver",
    )(one, two)


def choose(*arguments):
    n_ep = lax.axis_size("ep")
    rows, local_heads = arguments[0].shape[0], arguments[5].shape[1]
    share = n_ep // local_heads
    packed = local_heads % 2 == 0 and n_ep % local_heads == 0
    packed = packed and n_ep >= 8 and n_ep & (n_ep - 1) == 0 and lax.axis_size("tp") >= 4
    if packed and rows % (32 * share) == 0:
        return tuple(deliver(*fused_on_device(*arguments)))
    return on_device(*arguments)


def solution(mesh):
    in_specs = (
        P("ep", None),
        P(),
        P("tp", None),
        P("tp", None),
        P("tp", None),
        P(None, "tp"),
        P("ep", "tp"),
        P(None, "tp"),
        P("ep", None),
        P(),
        P("ep", None),
        P("ep", None),
        P("ep", "tp", None),
        P("ep", "tp", None),
        P("ep", "tp", None),
    )
    out_specs = (P("ep", "tp"), P("ep", "tp"))
    return jax.shard_map(
        choose, mesh=mesh, in_specs=in_specs, out_specs=out_specs, check_vma=False
    )
```

```python
import functools

import jax
import jax.numpy as jnp
from jax import lax
from jax.experimental import pallas as pl
from jax.experimental.pallas import tpu as pltpu
from jax.sharding import PartitionSpec as P

HD = 64
MEAN_FLOOR = 0.1
HEAD_FLOOR = 1.0
MESH = pl.DeviceIdType.MESH
VM = pl.BlockSpec(memory_space=pltpu.VMEM)
ANY = pl.BlockSpec(memory_space=pl.ANY)
DMA = pltpu.SemaphoreType.DMA
LIMIT = 48 << 20


def normed_rows(inputs, gain):
    values = inputs.astype(jnp.float32)
    square = jnp.mean(values * values, axis=-1, keepdims=True)
    return (values * lax.rsqrt(jnp.maximum(square, MEAN_FLOOR)) * gain).astype(jnp.bfloat16)


def by_rows(left, weight):
    return lax.dot_general(
        left, weight, (((1,), (1,)), ((), ())), preferred_element_type=jnp.float32
    )


class Place:
    def __init__(self, n_ep, n_tp):
        self.n_ep, self.n_tp, self.ny = n_ep, n_tp, n_tp // 2
        self.e = lax.axis_index("ep")
        self.t = lax.axis_index("tp")
        self.y, self.c = self.t // 2, self.t % 2
        self.partner = self.y * 2 + (1 - self.c)

    def ep(self, k):
        return (self.e + k) % self.n_ep

    def y_at(self, off):
        return (self.y + self.ny + off) % self.ny

    def chip(self, off):
        return self.y_at(off) * 2 + self.c

    def barrier(self):
        sem = pltpu.get_barrier_semaphore()
        for k in range(1, self.n_ep):
            pl.semaphore_signal(
                sem, inc=1, device_id={"ep": self.ep(k), "tp": self.t}, device_id_type=MESH
            )
        for off in range(1, self.ny):
            pl.semaphore_signal(
                sem, inc=1, device_id={"ep": self.e, "tp": self.chip(off)}, device_id_type=MESH
            )
        pl.semaphore_signal(
            sem, inc=1, device_id={"ep": self.e, "tp": self.partner}, device_id_type=MESH
        )
        pl.semaphore_wait(sem, self.n_ep - 1 + self.ny - 1 + 1)


def remote(src, dst, send, recv, e, t):
    return pltpu.make_async_remote_copy(
        src_ref=src,
        dst_ref=dst,
        send_sem=send,
        recv_sem=recv,
        device_id={"ep": e, "tp": t},
        device_id_type=MESH,
    )


class Exchange:
    def __init__(self, place, send, land, sems):
        self.p, self.send, self.land = place, send, land
        self.ssem, self.rsem = sems

    def copy(self, k):
        p = self.p
        d = p.ep(k)
        return remote(
            self.send(d), self.land(p.e), self.ssem.at[d], self.rsem.at[p.e], d, p.t
        )

    def arrival(self, k):
        p = self.p
        s = p.ep(k)
        return remote(self.send(s), self.land(s), self.ssem.at[s], self.rsem.at[s], s, p.t)

    def own(self):
        p = self.p
        return pltpu.make_async_copy(self.send(p.e), self.land(p.e), self.rsem.at[p.e])

    def start(self):
        for k in range(1, self.p.n_ep):
            self.copy(k).start()
        self.own().start()

    def wait_arrival(self, k):
        if k == 0:
            self.own().wait()
        else:
            self.arrival(k).wait_recv()

    def wait_sent(self):
        for k in range(1, self.p.n_ep):
            self.copy(k).wait_send()


class Spread:
    def __init__(self, place, land, sems):
        self.p, self.land = place, land
        self.ys, self.yr, self.ps, self.pr = sems

    def y_copy(self, off, s):
        p = self.p
        block = self.land(p.t, s)
        return remote(
            block, block, self.ys.at[off - 1, s], self.yr.at[off - 1, s], p.e, p.chip(off)
        )

    def y_arrival(self, off, s):
        p = self.p
        block = self.land(p.chip(-off), s)
        return remote(
            block, block, self.ys.at[off - 1, s], self.yr.at[off - 1, s], p.e, p.chip(-off)
        )

    def p_copy(self, off, s):
        p = self.p
        block = self.land(p.chip(-off), s)
        return remote(block, block, self.ps.at[off, s], self.pr.at[off, s], p.e, p.partner)

    def p_arrival(self, off, s):
        p = self.p
        block = self.land(p.y_at(-off) * 2 + (1 - p.c), s)
        return remote(block, block, self.ps.at[off, s], self.pr.at[off, s], p.e, p.partner)

    def first(self, s):
        for off in range(1, self.p.ny):
            self.y_copy(off, s).start()
        self.p_copy(0, s).start()

    def relay(self, s):
        for off in range(1, self.p.ny):
            self.y_arrival(off, s).wait_recv()
            self.p_copy(off, s).start()

    def finish(self, s):
        for off in range(self.p.ny):
            self.p_arrival(off, s).wait_recv()
        self.wait_sent(s)

    def wait_sent(self, s):
        for off in range(self.p.ny):
            self.p_copy(off, s).wait_send()
        for off in range(1, self.p.ny):
            self.y_copy(off, s).wait_send()


def spread_sems(n_ep, n_tp):
    ny = n_tp // 2
    far = max(ny - 1, 1)
    return [DMA((far, n_ep)), DMA((far, n_ep)), DMA((ny, n_ep)), DMA((ny, n_ep))]


def outward_kernel(
    n_ep, n_tp, slots, message, gates, gate_weight, up_weight,
    hidden, message_out, gates_out,
    out, gate_held, up_held, gate_act, up_act,
    s0, s1, m0, m1, g0, g1, w, ys, yr, ps, pr,
):
    p = Place(n_ep, n_tp)
    width = slots.shape[2]

    def cols(t):
        return pl.ds(pl.multiple_of(t * width, width), width)

    def land(t, s):
        return out.at[s, :, cols(t)]

    def multiply(t, opening):
        rows = out[:, :, cols(t)].reshape(hidden.shape[0], width)
        for held, total in ((gate_held, gate_act), (up_held, up_act)):
            product = by_rows(rows, held[:, cols(t)])
            total[...] = product if opening else total[...] + product

    loads = [
        pltpu.make_async_copy(gate_weight, gate_held, w.at[0]),
        pltpu.make_async_copy(up_weight, up_held, w.at[1]),
    ]
    for load in loads:
        load.start()
    p.barrier()
    slot_move = Exchange(p, lambda d: slots.at[d], lambda s: land(p.t, s), (s0, s1))
    gate_move = Exchange(p, lambda d: gates.at[d], lambda s: gates_out.at[s], (g0, g1))
    message_move = Exchange(p, lambda d: message.at[d], lambda s: message_out.at[s], (m0, m1))
    spread = Spread(p, land, (ys, yr, ps, pr))
    slot_move.start()
    gate_move.start()
    message_move.start()
    for k in range(n_ep):
        slot_move.wait_arrival(k)
        spread.first(p.ep(k))
    for load in loads:
        load.wait()
    multiply(p.t, True)
    for k in range(n_ep):
        spread.p_arrival(0, p.ep(k)).wait_recv()
    multiply(p.partner, False)
    for k in range(n_ep):
        spread.relay(p.ep(k))
    for off in range(1, p.ny):
        multiply(p.chip(-off), False)
        for k in range(n_ep):
            spread.p_arrival(off, p.ep(k)).wait_recv()
        multiply(p.y_at(-off) * 2 + (1 - p.c), False)
    gate = gate_act[...]
    hidden[...] = (gate * lax.logistic(gate) * up_act[...]).astype(hidden.dtype)
    for k in range(n_ep):
        gate_move.wait_arrival(k)
        message_move.wait_arrival(k)
        spread.wait_sent(p.ep(k))
    slot_move.wait_sent()
    gate_move.wait_sent()
    message_move.wait_sent()


def homeward_kernel(
    n_ep, n_tp, hidden, down_weight, heads, ret, heads_all,
    partial, down_held, pair, mine, out_y, in_y, final,
    w, h0, h1, a0, a1, r0, r1, q0, q1, ys, yr, ps, pr,
):
    p = Place(n_ep, n_tp)
    ny = p.ny
    width = ret.shape[2]

    def cols(t):
        return pl.ds(pl.multiple_of(t * width, width), width)

    def land(t, s):
        return heads_all.at[t, s]

    load = pltpu.make_async_copy(down_weight, down_held, w.at[0])
    load.start()
    p.barrier()
    head_move = Exchange(p, lambda d: heads.at[d], lambda s: land(p.t, s), (h0, h1))
    spread = Spread(p, land, (ys, yr, ps, pr))
    head_move.start()

    def pair_copy(s, off):
        src = partial.at[s, :, cols(p.y_at(off) * 2 + (1 - p.c))]
        return remote(src, pair.at[s, off], r0.at[s, off], r1.at[s, off], p.e, p.partner)

    def y_copy(s, off, to):
        return remote(
            out_y.at[s, off - 1], in_y.at[s, off - 1],
            q0.at[s, off - 1], q1.at[s, off - 1], p.e, p.chip(to),
        )

    def final_copy(k):
        d = p.ep(k)
        return remote(final.at[d], ret.at[p.e], a0.at[d], a1.at[p.e], d, p.t)

    order = list(range(1, n_ep)) + [0]
    capacity = ret.shape[1]

    def multiply(t):
        product = jnp.dot(
            hidden[...], down_held[:, cols(t)], preferred_element_type=jnp.float32
        )
        partial[:, :, cols(t)] = product.astype(jnp.bfloat16).reshape(n_ep, capacity, width)

    load.wait()
    turns = [*range(1, ny), 0]
    for off in turns:
        multiply(p.y_at(off) * 2 + (1 - p.c))
        multiply(p.chip(off))
        for k in order:
            pair_copy(p.ep(k), off).start()
        for k in order:
            s = p.ep(k)
            pair_copy(s, off).wait_recv()
            both = partial[s, :, cols(p.chip(off))].astype(jnp.float32) + pair[s, off].astype(
                jnp.float32
            )
            if off == 0:
                mine[s] = both
            else:
                out_y[s, off - 1] = both.astype(jnp.bfloat16)
                y_copy(s, off, off).start()
    for k in range(n_ep):
        head_move.wait_arrival(k)
        spread.first(p.ep(k))
    for k in order:
        s = p.ep(k)
        total = mine[s]
        for off in range(1, ny):
            y_copy(s, off, -off).wait_recv()
            total = total + in_y[s, off - 1].astype(jnp.float32)
        if k == 0:
            ret[s] = total.astype(jnp.bfloat16)
        else:
            final[s] = total.astype(jnp.bfloat16)
            final_copy(k).start()
    for k in range(n_ep):
        spread.relay(p.ep(k))
    for k in range(n_ep):
        spread.finish(p.ep(k))
    for k in range(n_ep):
        s = p.ep(k)
        for off in range(ny):
            pair_copy(s, off).wait_send()
        for off in range(1, ny):
            y_copy(s, off, off).wait_send()
    for k in range(1, n_ep):
        s = p.ep(k)
        remote(final.at[s], ret.at[s], a0.at[s], a1.at[s], s, p.t).wait_recv()
        final_copy(k).wait_send()
    head_move.wait_sent()


def outward(slots, message, gates, gate_weight, up_weight, n_ep, n_tp):
    _, capacity, width = slots.shape
    rows, units = n_ep * capacity, gate_weight.shape[0]
    scratch = [
        pltpu.VMEM((n_ep, capacity, width * n_tp), slots.dtype),
        pltpu.VMEM(gate_weight.shape, gate_weight.dtype),
        pltpu.VMEM(up_weight.shape, up_weight.dtype),
        pltpu.VMEM((rows, units), jnp.float32),
        pltpu.VMEM((rows, units), jnp.float32),
    ]
    sems = [DMA((n_ep,))] * 6 + [DMA((2,))] + spread_sems(n_ep, n_tp)
    return pl.pallas_call(
        functools.partial(outward_kernel, n_ep, n_tp),
        out_shape=[
            jax.ShapeDtypeStruct((rows, units), slots.dtype),
            jax.ShapeDtypeStruct(message.shape, message.dtype),
            jax.ShapeDtypeStruct(gates.shape, gates.dtype),
        ],
        in_specs=[VM] * 3 + [ANY] * 2,
        out_specs=[VM] * 3,
        scratch_shapes=scratch + sems,
        compiler_params=pltpu.CompilerParams(collective_id=0, has_side_effects=True),
        name="outward",
    )(slots, message, gates, gate_weight, up_weight)


def homeward(hidden, down_weight, heads, n_ep, n_tp):
    capacity, features = hidden.shape[0] // n_ep, down_weight.shape[1]
    width, ny = features // n_tp, n_tp // 2
    far = max(ny - 1, 1)
    scratch = [
        pltpu.VMEM((n_ep, capacity, features), jnp.bfloat16),
        pltpu.VMEM(down_weight.shape, down_weight.dtype),
        pltpu.VMEM((n_ep, ny, capacity, width), jnp.bfloat16),
        pltpu.VMEM((n_ep, capacity, width), jnp.float32),
        pltpu.VMEM((n_ep, far, capacity, width), jnp.bfloat16),
        pltpu.VMEM((n_ep, far, capacity, width), jnp.bfloat16),
        pltpu.VMEM((n_ep, capacity, width), jnp.bfloat16),
    ]
    sems = [DMA((1,))] + [DMA((n_ep,))] * 4 + [DMA((n_ep, ny))] * 2 + [DMA((n_ep, far))] * 2
    return pl.pallas_call(
        functools.partial(homeward_kernel, n_ep, n_tp),
        out_shape=[
            jax.ShapeDtypeStruct((n_ep, capacity, width), jnp.bfloat16),
            jax.ShapeDtypeStruct((n_tp,) + heads.shape, jnp.bfloat16),
        ],
        in_specs=[VM, ANY, VM],
        out_specs=[VM] * 2,
        scratch_shapes=scratch + sems + spread_sems(n_ep, n_tp),
        compiler_params=pltpu.CompilerParams(collective_id=1, has_side_effects=True),
        name="homeward",
    )(hidden, down_weight, heads)


def on_device(
    mixer_tokens,
    mixer_gain,
    query_weight,
    key_weight,
    value_weight,
    forget_weight,
    forget_bias,
    output_weight,
    expert_tokens,
    expert_gain,
    routes,
    route_weights,
    gate_weight,
    up_weight,
    down_weight,
):
    n_ep, n_tp = lax.axis_size("ep"), lax.axis_size("tp")
    rows, features = mixer_tokens.shape
    local_heads = forget_weight.shape[1]
    share = n_ep // local_heads
    part = rows // share
    width = features // n_tp
    bf16, f32 = jnp.bfloat16, jnp.float32

    expert_normed = normed_rows(expert_tokens, expert_gain)
    token_count, top_count = routes.shape
    capacity = 2 * top_count * token_count // n_ep
    pairs = token_count * top_count
    flat_routes = routes.reshape(-1)
    onehot = flat_routes[:, None] == jnp.arange(n_ep, dtype=jnp.int32)[None, :]
    before = jnp.tril(jnp.ones((pairs, pairs), bf16), -1)
    ranks = jnp.dot(before, onehot.astype(bf16), preferred_element_type=f32)
    slot_rank = jnp.sum(jnp.where(onehot, ranks, 0.0), axis=1).astype(jnp.int32)
    slot_index = (flat_routes * capacity + slot_rank).reshape(token_count, top_count)
    slot_ids = jnp.arange(n_ep * capacity, dtype=jnp.int32)
    picks = [(slot_index[:, j][:, None] == slot_ids[None, :]).astype(bf16) for j in range(top_count)]
    column = lax.axis_index("tp") * width
    own_columns = lax.dynamic_slice_in_dim(expert_normed, column, width, 1)
    slots = lax.dot_general(
        sum(picks[1:], picks[0]), own_columns, (((0,), (0,)), ((), ())),
        preferred_element_type=f32,
    ).astype(bf16).reshape(n_ep, capacity, width)

    normed = normed_rows(mixer_tokens, mixer_gain)
    queries = by_rows(normed, query_weight).astype(bf16)
    key_rows = by_rows(normed, key_weight).astype(bf16)
    value_rows = by_rows(normed, value_weight).astype(bf16)
    pre_gate = jnp.dot(normed, forget_weight, preferred_element_type=f32) + forget_bias
    block_cum = jnp.dot(
        jnp.tril(jnp.ones((rows, rows), f32)), jax.nn.log_sigmoid(pre_gate),
        precision=lax.Precision.HIGHEST, preferred_element_type=f32,
    )
    key_value = jnp.concatenate(
        [
            key_rows.reshape(rows, local_heads, HD).transpose(1, 0, 2),
            value_rows.reshape(rows, local_heads, HD).transpose(1, 0, 2),
        ],
        axis=2,
    )
    key_value = jnp.broadcast_to(
        key_value[:, None], (local_heads, share, rows, 2 * HD)
    ).reshape(n_ep, rows, 2 * HD)
    half = part // 2
    query_parts = queries.reshape(share, 2, half, local_heads, HD).transpose(3, 0, 2, 1, 4)
    query_parts = query_parts.reshape(n_ep, half, 2 * HD)
    message = jnp.concatenate([key_value, query_parts], axis=1)
    gates = jnp.broadcast_to(block_cum.T[:, None, None, :], (local_heads, share, 1, rows))
    gates = gates.reshape(n_ep, 1, rows)

    hidden, all_messages, all_gates = outward(
        slots, message, gates, gate_weight[0], up_weight[0], n_ep, n_tp
    )

    positions = n_ep * rows
    all_gates = all_gates.reshape(n_ep, rows)
    totals = all_gates[:, rows - 1]
    lower = jnp.arange(n_ep)[None, :] < jnp.arange(n_ep)[:, None]
    base = jnp.sum(jnp.where(lower, totals[None, :], 0.0), axis=1)
    cumulative = all_gates + base[:, None]
    keys = all_messages[:, :rows, :HD].reshape(positions, HD)
    values = all_messages[:, :rows, HD:].reshape(positions, HD)
    head_query = all_messages[:, rows:].reshape(n_ep, half, 2, HD).transpose(0, 2, 1, 3)
    head_query = head_query.reshape(n_ep * part, HD)
    first = (lax.axis_index("ep") % share) * part
    query_cum = lax.dynamic_slice_in_dim(cumulative, first, part, 1).reshape(-1)
    query_pos = (
        jnp.arange(n_ep, dtype=jnp.int32)[:, None] * rows
        + first
        + jnp.arange(part, dtype=jnp.int32)[None, :]
    ).reshape(-1)
    key_pos = jnp.arange(positions, dtype=jnp.int32)
    scores = by_rows(head_query, keys) * HD ** (-0.5)
    scores = scores + query_cum[:, None] - cumulative.reshape(-1)[None, :]
    scores = jnp.where(key_pos[None, :] <= query_pos[:, None], scores, -jnp.inf)
    weights = jnp.exp(scores - jnp.max(scores, axis=-1, keepdims=True)).astype(bf16)
    attended = jnp.dot(weights, values, preferred_element_type=f32)
    rescale = lax.rsqrt(jnp.mean(attended * attended, axis=-1, keepdims=True) + HEAD_FLOOR)
    head_out = (attended * rescale).astype(bf16).reshape(n_ep, part, HD)

    returned, heads_all = homeward(hidden, down_weight[0], head_out, n_ep, n_tp)

    heads_all = heads_all.reshape(n_tp, local_heads, share, part, HD).transpose(2, 3, 0, 1, 4)
    heads_all = heads_all.reshape(rows, n_tp * local_heads * HD)
    mixer_output = jnp.dot(heads_all, output_weight, preferred_element_type=f32).astype(bf16)
    returned = returned.reshape(n_ep * capacity, width)
    expert_output = 0.0
    for j in range(top_count):
        picked = jnp.dot(picks[j], returned, preferred_element_type=f32)
        expert_output = expert_output + picked * route_weights[:, j][:, None]
    return (mixer_output, expert_output.astype(bf16))


def lanes_of(shape, dim):
    return lax.broadcasted_iota(jnp.int32, shape, dim)


class Relay:
    def __init__(self, place, land, sems, batch):
        self.p, self.land, self.batch = place, land, batch
        self.ys, self.yr, self.ps, self.pr = sems

    def y_copy(self, off, s, t, to):
        block = self.land(t, s)
        return remote(block, block, self.ys.at[0], self.yr.at[off - 1, s], self.p.e, to)

    def p_copy(self, off, s, t):
        block, p = self.land(t, s), self.p
        return remote(block, block, self.ps.at[0], self.pr.at[self.batch(s)], p.e, p.partner)

    def first(self, s):
        p = self.p
        for off in range(1, p.ny):
            self.y_copy(off, s, p.t, p.chip(off)).start()
        self.p_copy(0, s, p.t).start()

    def relay(self, s):
        p = self.p
        for off in range(1, p.ny):
            self.y_copy(off, s, p.chip(-off), p.chip(-off)).wait_recv()
            self.p_copy(off, s, p.chip(-off)).start()

    def settle(self, batch, blocks):
        p = self.p
        remote(blocks, blocks, self.ps.at[0], self.pr.at[batch], p.e, p.partner).wait_recv()

    def sent(self, y_blocks, p_blocks):
        p = self.p
        remote(y_blocks, y_blocks, self.ys.at[0], self.yr.at[0, 0], p.e, p.partner).wait_send()
        remote(p_blocks, p_blocks, self.ps.at[0], self.pr.at[0], p.e, p.partner).wait_send()


def flipped(place, bits):
    at, weight = place, 1
    while bits:
        if bits % 2:
            at = at + weight * (1 - 2 * (place // weight % 2))
        bits, weight = bits // 2, weight * 2
    return at


def fused_kernel(
    n_ep, n_tp,
    tokens_a, gain_a, w_q, w_k, w_v, w_f, b_f, w_o, tokens_b, gain_b, routes, route_w,
    w_gate, w_up, w_down,
    out_a, out_b,
    a_held, ga_held, q_held, kv_held, f_held, bf_held, o_held, b_held, gb_held, r_held, rw_held,
    gate_held, up_held, down_held,
    slots, slots_more, land, w_hi, w_lo, kv_send, q_send, g_send, kv_land, q_land, g_land,
    hidden, pair_send, pair_land, own_part, mine, y_send, y_land, final, ret,
    q_all, q_cum, scores, running, row_max, attended, head_send, heads_all, lhs, mixed,
    lsem, s0, s1, m0, m1, ys, yr, ps, pr, k0, k1, x0, x1, q0, q1, g0, g1,
    p0, p1, z0, z1, a0, a1, h0, h1, hy0, hy1, hp0, hp1,
):
    p = Place(n_ep, n_tp)
    ny = p.ny
    bf16, f32 = jnp.bfloat16, jnp.float32
    rows, features = a_held.shape
    tokens = b_held.shape[0]
    _, capacity, width = slots.shape
    local_heads = kv_send.shape[0]
    share = n_ep // local_heads
    part = rows // share
    half = part // 2
    units = gate_held.shape[0]
    eighth = n_ep // 8
    order = [0, 1, 2, 6, 7, 3, 4, 5]

    def places(*eighths):
        return [order.index(k) * eighth + i for k in eighths for i in range(eighth)]

    own, second, third = places(0), places(6, 7), places(4, 5)
    near = [*own[1:], *places(1, 2, 3)]
    groups = [range(eighth), range(eighth, 5 * eighth), range(5 * eighth, n_ep)]
    early_near, late_near = places(1, 2), places(3)
    own_share = p.e % share
    first = own_share * part

    def cols(t):
        return pl.ds(pl.multiple_of(t * width, width), width)

    def peer(j):
        return flipped(p.e, order[j // eighth] * eighth + j % eighth)

    barrier = pltpu.get_barrier_semaphore()
    for k in range(1, n_ep):
        pl.semaphore_signal(
            barrier, inc=1, device_id={"ep": p.ep(k), "tp": p.t}, device_id_type=MESH
        )
    for off in range(1, ny):
        pl.semaphore_signal(
            barrier, inc=1, device_id={"ep": p.e, "tp": p.chip(off)}, device_id_type=MESH
        )
    pl.semaphore_signal(
        barrier, inc=1, device_id={"ep": p.e, "tp": p.partner}, device_id_type=MESH
    )

    early = [(tokens_b, b_held), (routes, r_held), (gain_b, gb_held)]
    middle = [(tokens_a, a_held), (gain_a, ga_held), (w_f, f_held), (b_f, bf_held), (w_q, q_held)]
    late = [
        (w_gate, gate_held), (w_up, up_held), (w_down, down_held), (route_w, rw_held),
        (w_o, o_held),
    ]
    loads, number = [], 0
    for batch in (early, middle, late):
        made = []
        for src, dst in batch:
            made.append(pltpu.make_async_copy(src, dst, lsem.at[number]))
            number += 1
        loads.append(made)
    pieces = []
    for h in range(local_heads):
        mine_rows = pl.ds(h * HD, HD)
        for at, src in ((2 * h, w_k), (2 * h + 1, w_v)):
            there = kv_held.at[pl.ds(at * HD, HD)]
            pieces.append(pltpu.make_async_copy(src.at[mine_rows], there, lsem.at[number]))
    all_pieces = pltpu.make_async_copy(kv_held, kv_held, lsem.at[number])
    early, middle, late = loads
    for load in early + middle + pieces:
        load.start()

    for load in early:
        load.wait()
    values = b_held[...].astype(f32)
    square = jnp.mean(values * values, axis=-1, keepdims=True)
    scale = lax.rsqrt(jnp.maximum(square, MEAN_FLOOR))
    b_held[...] = (values * scale * gb_held[...]).astype(bf16)
    named_by = r_held[...]
    top_count = named_by.shape[0]
    place = lanes_of((n_ep, tokens), 0)
    moved = [jnp.where(place // eighth == k, order[k] - k, 0) for k in range(8)]
    place = place + sum(moved[1:], moved[0]) * eighth
    expert_at, weight = place, 1
    while weight < n_ep:
        flip = (p.e // weight) % 2
        expert_at = expert_at + flip * weight * (1 - 2 * ((place // weight) % 2))
        weight *= 2
    chosen = [named_by[c : c + 1, :] == expert_at for c in range(top_count)]
    named = sum([c.astype(f32) for c in chosen[1:]], chosen[0].astype(f32))
    earlier = (lanes_of((tokens, tokens), 0) < lanes_of((tokens, tokens), 1)).astype(bf16)
    ranks = jnp.dot(named.astype(bf16), earlier, preferred_element_type=f32)
    ranks = jnp.where(named > 0, ranks, -1.0).astype(jnp.int32)
    slot_at = lanes_of((capacity, tokens), 0)
    picks = [ranks[j : j + 1, :] == slot_at for j in range(n_ep)]
    picks = [pick.astype(f32).astype(bf16) for pick in picks]

    def picked(j, lanes):
        return jnp.dot(picks[j], b_held[:, lanes], preferred_element_type=f32).astype(bf16)

    for j in range(1, n_ep):
        slots[j] = picked(j, cols(p.t))
    for j in near:
        for off in range(1, ny):
            slots_more[near.index(j), off - 1] = picked(j, cols(p.chip(-off)))
    pl.semaphore_wait(barrier, n_ep - 1 + ny - 1 + 1)

    def slot_copy(j):
        return remote(
            slots.at[j], land.at[j, :, cols(p.t)], s0.at[0], s1.at[j], peer(j), p.t
        )

    def more_copy(j, off):
        return remote(
            slots_more.at[near.index(j), off - 1], land.at[j, :, cols(p.chip(-off))],
            m0.at[0], m1.at[near.index(j), off - 1], peer(j), p.t,
        )

    def send(j):
        slot_copy(j).start()
        if j in near:
            for off in range(1, ny):
                more_copy(j, off).start()

    spread = Relay(
        p,
        lambda t, j: land.at[j, :, cols(t)],
        (ys, yr, ps, pr),
        lambda j: [j in group for group in groups].index(True),
    )
    for j in [*own[1:], *places(1), *second, *places(2, 3), *third]:
        send(j)
    land[0] = picked(0, slice(None))

    for load in middle + [all_pieces]:
        load.wait()
    for load in late:
        load.start()
    values = a_held[...].astype(f32)
    square = jnp.mean(values * values, axis=-1, keepdims=True)
    scale = lax.rsqrt(jnp.maximum(square, MEAN_FLOOR))
    a_held[...] = (values * scale * ga_held[...]).astype(bf16)
    normed = a_held[...]
    eye = lanes_of((local_heads, local_heads), 0) == lanes_of((local_heads, local_heads), 1)
    bias = jnp.sum(jnp.where(eye, bf_held[...], 0.0), axis=1, keepdims=True)
    gate = by_rows(f_held[...], normed) + bias
    log_gate = jnp.minimum(gate, 0.0) - jnp.log1p(jnp.exp(-jnp.abs(gate)))
    upto = (lanes_of((rows, rows), 0) <= lanes_of((rows, rows), 1)).astype(f32)
    block_cum = jnp.dot(
        log_gate, upto, precision=lax.Precision.HIGHEST, preferred_element_type=f32
    )
    for h in range(local_heads):
        g_send[h] = block_cum[h : h + 1, :]

    def kv_copy(h):
        to = h * share + own_share
        return remote(kv_send.at[h], kv_land.at[p.e], k0.at[0], k1.at[p.e // share], to, p.t)

    def kv_arrival(n):
        s = (p.e // share + n) % local_heads * share + own_share
        return remote(kv_send.at[0], kv_land.at[s], k0.at[0], k1.at[s // share], p.e, p.t), s

    def sibling(off):
        return p.e // share * share + (own_share + off) % share

    def kv_relay(s, off):
        return remote(
            kv_land.at[s], kv_land.at[s], x0.at[0], x1.at[0], sibling(off), p.t
        )

    def q_copy(k):
        d = p.ep(k)
        return remote(q_send.at[d], q_land.at[p.e], q0.at[0], q1.at[0], d, p.t)

    def g_copy(k):
        d = p.ep(k)
        return remote(g_send.at[d // share], g_land.at[p.e], g0.at[0], g1.at[0], d, p.t)

    def others(ref):
        return ref.at[pl.ds(0, n_ep - 1)]

    def batch_of(ref, send, recv):
        return remote(ref, ref, send.at[0], recv.at[0], p.e, p.partner)

    key_value = by_rows(normed, kv_held[...]).astype(bf16)
    for h in range(local_heads):
        kv_send[h] = key_value[:, 2 * h * HD : 2 * (h + 1) * HD]
    for n in range(1, local_heads):
        kv_copy((p.e // share + n) % local_heads).start()
    own_head = p.e // share
    kv_land[p.e] = kv_send[own_head]
    for off in range(1, share):
        kv_relay(p.e, off).start()
    queries = by_rows(normed, q_held[...]) * HD ** (-0.5)
    left = lanes_of((half, 2 * HD), 1) < HD
    for pair in range(local_heads // 2):
        there = queries[:, 2 * pair * HD : 2 * (pair + 1) * HD]
        moved = pltpu.roll(there, HD, 1)
        for x in range(share):
            top, bottom = slice(x * part, x * part + half), slice(x * part + half, (x + 1) * part)
            q_send[2 * pair * share + x] = jnp.where(left, there[top], moved[bottom]).astype(bf16)
            q_send[(2 * pair + 1) * share + x] = jnp.where(
                left, moved[top], there[bottom]
            ).astype(bf16)
    for k in range(1, n_ep):
        q_copy(k).start()
        g_copy(k).start()
    q_land[p.e] = q_send[p.e]
    g_land[p.e] = g_send[own_head]

    def arrive(j):
        slot_copy(j).wait_recv()
        if j in near:
            spread.p_copy(0, j, p.t).start()
            for off in range(1, ny):
                more_copy(j, off).wait_recv()
                spread.p_copy(off, j, p.chip(-off)).start()
        else:
            spread.first(j)

    def complete(j):
        spread.relay(j)

    def settle(g):
        count = len(groups[g]) - (0 in groups[g])
        spread.settle(g, land.at[pl.ds(0, count), :, pl.ds(0, ny * width)])

    cuts = [(at, min(at + 512, units)) for at in range(0, units, 512)]

    def serve(beside, number, count):
        for act, *given in beside[len(beside) * number // count : len(beside) * (number + 1) // count]:
            act(*given)

    def open_up(g, beside):
        low_row, count = groups[g][0], len(groups[g])
        block = land[low_row : low_row + count].reshape(count * capacity, features)
        lines = slice(low_row * capacity, (low_row + count) * capacity)
        for number, (low, high) in enumerate(cuts):
            gated = by_rows(gate_held[low:high], block)
            upped = by_rows(up_held[low:high], block)
            hidden[lines, low:high] = (gated * lax.logistic(gated) * upped).astype(bf16).T
            serve(beside, number, len(cuts))

    def pair_copy(g, off):
        low_row, count = groups[g][0], len(groups[g])
        lines = pl.ds(low_row * capacity, count * capacity)
        return remote(
            pair_send.at[off, lines], pair_land.at[off, lines], p0.at[0], p1.at[g, off],
            p.e, p.partner,
        )

    def y_copy(j, off, to):
        return remote(
            y_send.at[j, off - 1], y_land.at[j, off - 1],
            z0.at[0], z1.at[j, off - 1], p.e, p.chip(to),
        )

    turns = [*range(1, ny), 0]

    def close_down(g, beside, held=()):
        low_row, count = groups[g][0], len(groups[g])
        lines = slice(low_row * capacity, (low_row + count) * capacity)

        def product(t):
            return jnp.dot(hidden[lines], down_held[:, cols(t)], preferred_element_type=f32)

        for number, off in enumerate(turns):
            pair_send[off, lines] = product(p.y_at(off) * 2 + (1 - p.c)).astype(bf16)
            pair_copy(g, off).start()
            serve(beside, number, 2 * ny)
        for number, off in enumerate(turns):
            own_part[lines] = product(p.chip(off))
            serve(beside, ny + number, 2 * ny)
            pair_copy(g, off).wait_recv()
            both = own_part[lines] + pair_land[off, lines].astype(f32)
            both = both.reshape(count, capacity, width)
            for m in range(count):
                j = low_row + m
                if off == 0:
                    mine[j] = both[m]
                else:
                    y_send[j, off - 1] = both[m].astype(bf16)
                    if j not in held:
                        y_copy(j, off, off).start()

    def final_copy(j):
        return remote(final.at[j], ret.at[j], a0.at[0], a1.at[0], peer(j), p.t)

    def finish(j):
        total = mine[j]
        for off in range(1, ny):
            y_copy(j, off, -off).wait_recv()
            total = total + y_land[j, off - 1].astype(f32)
        if j == 0:
            ret[0] = total.astype(bf16)
        else:
            final[j] = total.astype(bf16)
            final_copy(j).start()

    def kv_forward(n):
        copy, s = kv_arrival(n)
        copy.wait_recv()
        for off in range(1, share):
            kv_relay(s, off).start()

    for j in own[1:]:
        arrive(j)
    if own[1:]:
        settle(0)
    late[0].wait()
    late[1].wait()
    open_up(0, [(arrive, j) for j in places(1)])
    late[2].wait()
    close_down(0, [(arrive, j) for j in second], own)
    for j in places(2):
        arrive(j)
    for j in second:
        complete(j)
    settle(1)
    open_up(1, [(arrive, j) for j in [*third, *late_near]])
    close_down(1, [], near)
    for j in early_near:
        for off in range(1, ny):
            y_copy(j, off, off).start()
    complete(third[0])
    for n in range(1, local_heads):
        kv_forward(n)
    for j in third[1:]:
        complete(j)
    settle(2)
    open_up(2, [(finish, j) for j in second])
    close_down(2, [], near)

    late[3].wait()
    for j in range(n_ep):
        weight = 0.0
        for c in range(top_count):
            weight = weight + jnp.where(
                named_by[c : c + 1, :] == peer(j), rw_held[c : c + 1, :], 0.0
            )
        weight = jnp.where(ranks[j : j + 1, :] == slot_at, weight, 0.0)
        high = weight.astype(bf16)
        w_hi[j * capacity : (j + 1) * capacity] = high
        w_lo[j * capacity : (j + 1) * capacity] = (weight - high.astype(f32)).astype(bf16)

    batch_of(others(g_land), g0, g1).wait_recv()
    batch_of(others(q_land), q0, q1).wait_recv()
    relayed = kv_land.at[pl.ds(0, local_heads * (share - 1))]
    batch_of(relayed, x0, x1).wait_recv()
    positions = lanes_of((part, rows), 1)
    asked = first + lanes_of((part, rows), 0)
    base = jnp.zeros((1, 1), f32)
    key_cum = []
    last = lanes_of((1, rows), 1) == rows - 1
    for b in range(n_ep):
        block = g_land[b]
        key_cum.append(block + base)
        base = base + jnp.sum(jnp.where(last, block, 0.0), axis=1, keepdims=True)
        at = b * part
        q_cum[at : at + part] = jnp.sum(
            jnp.where(positions == asked, key_cum[b], 0.0), axis=1, keepdims=True
        )
        packed = q_land[b].astype(f32)
        q_all[at : at + half] = jnp.where(left, packed, 0.0).astype(bf16)
        q_all[at + half : at + part] = jnp.where(
            left, pltpu.roll(packed, HD, 1), 0.0
        ).astype(bf16)
    for b in range(n_ep):
        at = b * part
        block = by_rows(q_all[at:], kv_land[b]) + q_cum[at:] - key_cum[b]
        seen = jnp.where(positions <= asked, block[:part], -jnp.inf)
        scores[b, at : at + part] = seen
        if b == 0:
            running[:part] = seen
            running[part:] = block[part:]
        else:
            running[at : at + part] = jnp.maximum(running[at : at + part], seen)
        if b + 1 < n_ep:
            scores[b, at + part :] = block[part:]
            if b > 0:
                running[at + part :] = jnp.maximum(running[at + part :], block[part:])
    row_max[...] = jnp.max(running[...], axis=1, keepdims=True)
    for b in range(n_ep):
        at = b * part
        weights = jnp.exp(scores[b, at:] - row_max[at:]).astype(bf16)
        product = jnp.dot(weights, kv_land[b], preferred_element_type=f32)
        if b == 0:
            attended[...] = product
        else:
            attended[at:] = attended[at:] + product
    behind = [*late_near, *own]
    for j in behind:
        for off in range(1, ny):
            y_copy(j, off, off).start()
    right = lanes_of((part, 2 * HD), 1) >= HD
    for b in range(n_ep):
        block = jnp.where(right, attended[b * part : (b + 1) * part], 0.0)
        block = block * lax.rsqrt(
            jnp.sum(block * block, axis=1, keepdims=True) * (1.0 / HD) + HEAD_FLOOR
        )
        moved = pltpu.roll(block, HD, 1)
        head_send[b] = jnp.where(left, moved[:half], block[half:]).astype(bf16)

    def head_copy(k):
        d = peer(k)
        return remote(head_send.at[d], heads_all.at[p.t, p.e], h0.at[0], h1.at[p.e], d, p.t)

    def head_arrival(k):
        s = peer(k)
        return remote(head_send.at[s], heads_all.at[p.t, s], h0.at[0], h1.at[s], s, p.t)

    for k in [*second, *third, *near]:
        head_copy(k).start()
    heads_all[p.t, p.e] = head_send[p.e]

    for j in early_near:
        finish(j)
    for j in third:
        finish(j)

    gather = Relay(p, lambda t, s: heads_all.at[t, s], (hy0, hy1, hp0, hp1), lambda s: 0)
    gather.first(p.e)
    for k in near:
        head_arrival(k).wait_recv()
        gather.first(peer(k))
    for j in behind:
        finish(j)
    for k in [*second, *third]:
        head_arrival(k).wait_recv()
        gather.first(peer(k))
    for k in range(n_ep):
        gather.relay(peer(k))
    late[4].wait()

    def project(t):
        for pair in range(local_heads // 2):
            lanes = slice(2 * pair * HD, 2 * (pair + 1) * HD)
            for x in range(share):
                one = heads_all[t, 2 * pair * share + x].astype(f32)
                two = heads_all[t, (2 * pair + 1) * share + x].astype(f32)
                at = x * part
                lhs[at : at + half, lanes] = jnp.where(
                    left, one, pltpu.roll(two, HD, 1)
                ).astype(bf16)
                lhs[at + half : at + part, lanes] = jnp.where(
                    left, pltpu.roll(one, HD, 1), two
                ).astype(bf16)
        deep = local_heads * HD
        here = o_held[pl.ds(pl.multiple_of(t * deep, deep), deep), :]
        return jnp.dot(lhs[...], here, preferred_element_type=f32)

    mixed[...] = project(p.t)
    for off in range(1, ny):
        mixed[...] = mixed[...] + project(p.chip(-off))
    gather.settle(0, heads_all.at[pl.ds(0, ny)])
    for off in range(ny - 1):
        mixed[...] = mixed[...] + project(p.y_at(-off) * 2 + (1 - p.c))
    last_part = project(p.y_at(-(ny - 1)) * 2 + (1 - p.c))
    out_a[...] = (mixed[...] + last_part).astype(bf16)

    batch_of(others(ret), a0, a1).wait_recv()
    returned = ret[...].reshape(n_ep * capacity, width)
    over_slots = (((0,), (0,)), ((), ()))
    total = lax.dot_general(w_hi[...], returned, over_slots, preferred_element_type=f32)
    total = total + lax.dot_general(w_lo[...], returned, over_slots, preferred_element_type=f32)
    out_b[...] = total.astype(bf16)

    spread.sent(
        land.at[pl.ds(0, len(second) + len(third)), :, pl.ds(0, (ny - 1) * width)],
        land.at[pl.ds(0, n_ep - 1), :, pl.ds(0, ny * width)],
    )
    gather.sent(heads_all.at[pl.ds(0, ny - 1)], heads_all.at[pl.ds(0, ny)])
    for ref, send, recv in (
        (others(slots), s0, s1), (slots_more, m0, s1), (others(q_send), q0, q1), (others(final), a0, a1),
        (others(head_send), h0, h1), (pair_send, p0, a1), (y_send, z0, a1),
        (others(g_land), g0, g1), (kv_send.at[pl.ds(0, local_heads - 1)], k0, k1),
        (relayed, x0, x1),
    ):
        batch_of(ref, send, recv).wait_send()


def fused_on_device(
    mixer_tokens, mixer_gain, query_weight, key_weight, value_weight, forget_weight,
    forget_bias, output_weight, expert_tokens, expert_gain, routes, route_weights,
    gate_weight, up_weight, down_weight,
):
    n_ep, n_tp = lax.axis_size("ep"), lax.axis_size("tp")
    ny = n_tp // 2
    far = max(ny - 1, 1)
    rows, features = mixer_tokens.shape
    tokens, top_count = routes.shape
    local_heads = forget_weight.shape[1]
    share = n_ep // local_heads
    part = rows // share
    half = part // 2
    width = features // n_tp
    capacity = 2 * top_count * tokens // n_ep
    units = gate_weight.shape[1]
    groups = 3
    asked = n_ep * part
    bf16, f32 = jnp.bfloat16, jnp.float32
    operands = [
        mixer_tokens, mixer_gain.reshape(1, features), query_weight, key_weight, value_weight,
        forget_weight.T, forget_bias, output_weight, expert_tokens,
        expert_gain.reshape(1, features), routes.T, route_weights.T,
        gate_weight[0], up_weight[0], down_weight[0],
    ]
    operands = [pltpu.with_memory_space_constraint(x, pltpu.HBM) for x in operands]
    vmem = pltpu.VMEM
    scratch = [
        vmem((rows, features), bf16), vmem((1, features), f32),
        vmem(query_weight.shape, bf16), vmem((2 * local_heads * HD, features), bf16),
        vmem((local_heads, features), bf16), vmem((1, local_heads), f32),
        vmem(output_weight.shape, bf16), vmem((tokens, features), bf16),
        vmem((1, features), f32), vmem((top_count, tokens), jnp.int32),
        vmem((top_count, tokens), f32),
        vmem((units, features), bf16), vmem((units, features), bf16),
        vmem((units, features), bf16),
        vmem((n_ep, capacity, width), bf16), vmem((n_ep // 2 - 1, far, capacity, width), bf16),
        vmem((n_ep, capacity, features), bf16),
        vmem((n_ep * capacity, tokens), bf16), vmem((n_ep * capacity, tokens), bf16),
        vmem((local_heads, rows, 2 * HD), bf16), vmem((n_ep, half, 2 * HD), bf16),
        vmem((local_heads, 1, rows), f32),
        vmem((n_ep, rows, 2 * HD), bf16), vmem((n_ep, half, 2 * HD), bf16),
        vmem((n_ep, 1, rows), f32),
        vmem((n_ep * capacity, units), bf16),
        vmem((ny, n_ep * capacity, width), bf16),
        vmem((ny, n_ep * capacity, width), bf16),
        vmem((n_ep * capacity, width), f32),
        vmem((n_ep, capacity, width), f32),
        vmem((n_ep, far, capacity, width), bf16), vmem((n_ep, far, capacity, width), bf16),
        vmem((n_ep, capacity, width), bf16), vmem((n_ep, capacity, width), bf16),
        vmem((asked, 2 * HD), bf16), vmem((asked, 1), f32),
        vmem((n_ep, asked, rows), f32), vmem((asked, rows), f32), vmem((asked, 1), f32),
        vmem((asked, 2 * HD), f32), vmem((n_ep, half, 2 * HD), bf16),
        vmem((n_tp, n_ep, half, 2 * HD), bf16), vmem((rows, local_heads * HD), bf16), vmem((rows, width), f32),
    ]
    one = DMA((1,))
    sems = [DMA((14,)), one, DMA((n_ep,)), one, DMA((n_ep // 2 - 1, far)), one, DMA((far, n_ep)), one, DMA((groups,))]
    sems += [one, DMA((local_heads,))] + [one] * 6
    sems += [one, DMA((groups, ny)), one, DMA((n_ep, far)), one, one, one, DMA((n_ep,))]
    sems += [one, DMA((far, n_ep)), one, one]
    return pl.pallas_call(
        functools.partial(fused_kernel, n_ep, n_tp),
        out_shape=[
            jax.ShapeDtypeStruct((rows, width), bf16),
            jax.ShapeDtypeStruct((tokens, width), bf16),
        ],
        in_specs=[ANY] * len(operands),
        out_specs=[VM] * 2,
        scratch_shapes=scratch + sems,
        compiler_params=pltpu.CompilerParams(
            collective_id=2, has_side_effects=True, vmem_limit_bytes=LIMIT
        ),
        name="fused",
    )(*operands)


def deliver_kernel(one, two, one_out, two_out, sem):
    copies = [
        pltpu.make_async_copy(one, one_out, sem.at[0]),
        pltpu.make_async_copy(two, two_out, sem.at[1]),
    ]
    for copy in copies:
        copy.start()
    for copy in copies:
        copy.wait()


def deliver(one, two):
    return pl.pallas_call(
        deliver_kernel,
        out_shape=[
            jax.ShapeDtypeStruct(one.shape, one.dtype),
            jax.ShapeDtypeStruct(two.shape, two.dtype),
        ],
        in_specs=[ANY] * 2,
        out_specs=[ANY] * 2,
        scratch_shapes=[DMA((2,))],
        compiler_params=pltpu.CompilerParams(vmem_limit_bytes=1 << 20),
        name="deliver",
    )(one, two)


def choose(*arguments):
    n_ep = lax.axis_size("ep")
    rows, local_heads = arguments[0].shape[0], arguments[5].shape[1]
    share = n_ep // local_heads
    packed = local_heads % 2 == 0 and n_ep % local_heads == 0
    packed = packed and n_ep >= 8 and n_ep & (n_ep - 1) == 0 and lax.axis_size("tp") >= 4
    if packed and rows % (32 * share) == 0:
        return tuple(deliver(*fused_on_device(*arguments)))
    return on_device(*arguments)


def solution(mesh):
    in_specs = (
        P("ep", None),
        P(),
        P("tp", None),
        P("tp", None),
        P("tp", None),
        P(None, "tp"),
        P("ep", "tp"),
        P(None, "tp"),
        P("ep", None),
        P(),
        P("ep", None),
        P("ep", None),
        P("ep", "tp", None),
        P("ep", "tp", None),
        P("ep", "tp", None),
    )
    out_specs = (P("ep", "tp"), P("ep", "tp"))
    return jax.shard_map(
        choose, mesh=mesh, in_specs=in_specs, out_specs=out_specs, check_vma=False
    )
```
